32 devices in a mesh: sp: 8 (over z, x), tp: 4 (over y, core).
Axes of the slice: x: 2, y: 2, z: 4, core: 2. Of those that a mesh axis runs over, the one named last changes fastest.
Arguments:
- inputs: bfloat16 [3072, 2048], P('sp', 'tp'), may hold values from -6 to 6
- norm_gain: float32 [2048], replicated, may hold values from 0.1 to 1.9
- query_weight: bfloat16 [2048, 1024], P(None, 'tp')
- key_weight: bfloat16 [2048, 1024], P(None, 'tp'), may hold values from -0.15625 to 0.15625
- value_weight: bfloat16 [2048, 1024], P(None, 'tp'), may hold values from -0.125 to 0.125
- memory_query_weight: bfloat16 [2048, 1024], P(None, 'tp'), may hold values from -0.125 to 0.125
- memory_key_weight: bfloat16 [2048, 1024], P(None, 'tp'), may hold values from -0.125 to 0.125
- memory_value_weight: bfloat16 [2048, 1024], P(None, 'tp'), may hold values from -0.125 to 0.125
- input_gate_weight: bfloat16 [2048, 16], P(None, 'tp')
- forget_gate_weight: bfloat16 [2048, 16], P(None, 'tp'), may hold values from -0.3125 to 0.3125
- forget_bias: float32 [16], P('tp'), may hold values from 3 to 13
- decay_shift: float32 [3072, 16], P('sp', 'tp'), may hold values from -2 to 0, as said below
- lambdas: float32 [16], P('tp'), may hold values from 0.3 to 0.8
- head_gain: float32 [64], replicated, may hold values from 0.1 to 1.9
- out_weight_attention: bfloat16 [1024, 2048], P('tp'), may hold values from -0.125 to 0.125
- out_weight_memory: bfloat16 [1024, 2048], P('tp'), may hold values from -0.125 to 0.125
Outputs:
- combined: bfloat16 [3072, 2048], P('sp', 'tp')
The draws below stay inside these ranges and needn't reach their ends.
Inputs may be any that keep to these rules, and one draw needn't show every extreme that they name: `decay_shift`: never positive.
All inputs are finite; a program needn't handle non-finite values.
Results may differ from the reference program's by a relative error of at most 0.018.
The reference program's roundings to bfloat16 on the way count: a program that leaves them out, or rounds other values in their place, can miss the bound.
Values may be sent and summed in bfloat16 or wider, within the bound.
A program may use at most 192 MiB of HBM per device.

```python
import math
import jax
import jax.numpy as jnp
from jax import lax

D = 2048
HEAD = 64
DD = 32
HD = 16
MATRIX_HEADS = 16
BLOCK = 64
SEQUENCE_TOKENS = 3072
N_TP = 4


def draw_query_weight(key, part):
    entries = jnp.clip(jax.random.normal(jax.random.fold_in(key, 11), (D, HD * HEAD), jnp.float32), -6.0, 6.0)
    entries = entries * (1.3 / D ** 0.5)
    return entries.astype(jnp.bfloat16)


def draw_input_gate_weight(key, part):
    entries = jnp.clip(jax.random.normal(jax.random.fold_in(key, 13), (D, MATRIX_HEADS), jnp.float32), -6.0, 6.0)
    entries = entries / D ** 0.5
    return entries.astype(jnp.bfloat16)


def draw_forget_bias(key, part):
    fast_share = 0.5
    fast_heads = jax.random.uniform(jax.random.fold_in(key, 21), (MATRIX_HEADS,), jnp.float32) < fast_share
    jitter = jax.random.uniform(jax.random.fold_in(key, 22), (MATRIX_HEADS,), jnp.float32)
    quick_bias = math.log(40.0) + jitter - 0.5
    slow_bias = math.log(float(SEQUENCE_TOKENS)) + 2.0 + jitter
    return jnp.where(fast_heads, quick_bias, slow_bias).astype(jnp.float32)


def draw_decay_shift(key, part):
    block_count = SEQUENCE_TOKENS // BLOCK
    factor = jnp.exp(jax.random.uniform(jax.random.fold_in(key, 31), (block_count, 1, MATRIX_HEADS), jnp.float32, math.log(0.3), math.log(5.0)))
    constant_level = -jnp.broadcast_to(factor, (block_count, BLOCK, MATRIX_HEADS)).reshape(SEQUENCE_TOKENS, MATRIX_HEADS) / SEQUENCE_TOKENS
    spike_row_list = jax.random.randint(jax.random.fold_in(key, 32), (4, MATRIX_HEADS), 0, SEQUENCE_TOKENS)
    spike_dropouts = jnp.log(jax.random.uniform(jax.random.fold_in(key, 33), (4, MATRIX_HEADS), jnp.float32, 0.4, 0.75))
    row_indices = jnp.arange(SEQUENCE_TOKENS, dtype=jnp.int32)[:, None, None]
    spike_events = jnp.sum(jnp.where(row_indices == spike_row_list[None], spike_dropouts[None], 0.0), axis=1)
    return jnp.maximum(constant_level + spike_events, -2.0).astype(jnp.float32)


def levels(own_key, extent, cuts, low, top_value):
    def one(position, parts):
        draws = jax.random.uniform(jax.random.fold_in(jax.random.fold_in(own_key, 6), position), (parts,), jnp.float32, low / len(cuts), top_value / len(cuts))
        return jnp.repeat(jnp.exp(draws), extent[position] // parts).reshape((-1,) + (1,) * (len(extent) - position - 1))

    gain = one(*cuts[0])
    for cut in cuts[1:]:
        gain = gain * one(*cut)
    return gain


def centred(own_key, extent, deviation, bound, shards=(), kind=jnp.bfloat16):
    drawn = deviation * jax.random.normal(own_key, extent, jnp.float32)
    if shards:
        drawn = drawn * levels(own_key, extent, shards, -0.22, 0.18)
    return jnp.clip(drawn, -bound, bound).astype(kind)


def setup_inputs(seed: int = 0) -> dict:
    key_of = jax.random.split(jax.random.key(seed), 17)
    return {
        "inputs": centred(key_of[0], (SEQUENCE_TOKENS, D), 1.0, 6.0, ((0, 8), (1, 4))),
        "norm_gain": jnp.clip(1.0 + 0.18 * jax.random.normal(key_of[1], (D,), jnp.float32), 0.1, 1.9),
        "query_weight": draw_query_weight(jax.random.fold_in(key_of[16], 71), 0),
        "key_weight": centred(key_of[3], (D, HD * HEAD), (D * 10 // 17) ** -0.5, 0.15625, ((1, 4),)),
        "value_weight": centred(key_of[4], (D, HD * HEAD), D ** -0.5, 0.125, ((1, 4),)),
        "memory_query_weight": centred(key_of[5], (D, MATRIX_HEADS * HEAD), D ** -0.5, 0.125, ((1, 4),)),
        "memory_key_weight": centred(key_of[6], (D, MATRIX_HEADS * HEAD), D ** -0.5, 0.125, ((1, 4),)),
        "memory_value_weight": centred(key_of[7], (D, MATRIX_HEADS * HEAD), D ** -0.5, 0.125, ((1, 4),)),
        "input_gate_weight": draw_input_gate_weight(jax.random.fold_in(key_of[16], 71), 0),
        "forget_gate_weight": centred(key_of[9], (D, MATRIX_HEADS), (D // 6) ** -0.5, 0.3125, ((1, 4),)),
        "forget_bias": draw_forget_bias(jax.random.fold_in(key_of[16], 71), 0),
        "decay_shift": draw_decay_shift(jax.random.fold_in(key_of[16], 71), 0),
        "lambdas": jnp.clip(0.3 + 0.5 * jax.random.uniform(key_of[12], (HD,), jnp.float32) ** levels(key_of[12], (HD,), ((0, 4),), -0.2, 0.2), 0.3, 0.8),
        "head_gain": jnp.clip(1.0 + 0.18 * jax.random.normal(key_of[13], (HEAD,), jnp.float32), 0.1, 1.9),
        "out_weight_attention": centred(key_of[14], (HD * HEAD, D), ((HD + MATRIX_HEADS) * HEAD) ** -0.5, 0.125, ((0, 4),)),
        "out_weight_memory": centred(key_of[15], (MATRIX_HEADS * HEAD, D), ((HD + MATRIX_HEADS) * HEAD) ** -0.5, 0.125, ((0, 4),)),
    }


EPSILON = 1e-06
ROTARY_BASE = 10000.0
NEGATIVE = -1e+30

def rotate(halves, positions):
    middle = halves.shape[-1] // 2
    inverse = 1.0 / ROTARY_BASE ** (jnp.arange(middle, dtype=jnp.float32) / middle)
    angles = positions.astype(jnp.float32)[:, None] * inverse[None, :]
    cosine = jnp.cos(angles)[:, None, :]
    sine_part = jnp.sin(angles)[:, None, :]
    floats = halves.astype(jnp.float32)
    former = floats[..., :middle]
    latter = floats[..., middle:]
    turned = jnp.concatenate([former * cosine - latter * sine_part, latter * cosine + former * sine_part], axis=-1)
    return turned.astype(jnp.bfloat16)

def advance_state(carried, block_entry):
    memory, normal, stable = carried
    block_memory, block_normal, block_max, block_decay = block_entry
    new_stable = jnp.maximum(block_decay + stable, block_max)
    former = jnp.exp(block_decay + stable - new_stable)
    latter = jnp.exp(block_max - new_stable)
    return (former[:, None, None] * memory + latter[:, None, None] * block_memory, former[:, None] * normal + latter[:, None] * block_normal, new_stable)

def memory_blocks(queries, key_heads, values, gate_in, log_forget, entering):
    token_count, head_count, head_width = queries.shape
    block_count = token_count // BLOCK
    highest = lax.Precision.HIGHEST

    def blocked(flat_array):
        return flat_array.astype(jnp.float32).reshape(block_count, BLOCK, head_count, head_width).transpose(2, 0, 1, 3)
    query_blocks = blocked(queries)
    key_blocks = blocked(key_heads) * head_width ** (-0.5)
    value_blocks = blocked(values)
    gate_blocks = gate_in.reshape(block_count, BLOCK, head_count).transpose(2, 0, 1)
    cumulative = jnp.cumsum(log_forget.reshape(block_count, BLOCK, head_count).transpose(2, 0, 1), axis=-1)
    block_ends = cumulative[..., -1]
    toward_end = block_ends[..., None] - cumulative + gate_blocks
    local_max = lax.optimization_barrier(jnp.max(toward_end, axis=-1))
    end_weights = jnp.exp(toward_end - local_max[..., None])
    local_memory = jnp.einsum('hcl,hclv,hclk->chvk', end_weights, value_blocks, key_blocks, precision=highest)
    local_normal = jnp.einsum('hcl,hclk->chk', end_weights, key_blocks, precision=highest)

    def scan_step(carried, block_entry):
        return (advance_state(carried, block_entry), carried)
    entries = (local_memory, local_normal, local_max.T, block_ends.T)
    unused, (memory_in, normal_in, stable_in) = lax.scan(scan_step, entering, entries)
    lower_mask = jnp.tril(jnp.ones((BLOCK, BLOCK), dtype=bool))
    decays = jnp.where(lower_mask, cumulative[..., :, None] - cumulative[..., None, :] + gate_blocks[..., None, :], NEGATIVE)
    carried_log = cumulative + stable_in.T[..., None]
    row_max = jnp.maximum(carried_log, lax.optimization_barrier(jnp.max(decays, axis=-1)))
    within = jnp.where(lower_mask, jnp.exp(decays - row_max[..., None]), 0.0)
    outside = jnp.exp(carried_log - row_max)
    scores = within * jnp.einsum('hctd,hcsd->hcts', query_blocks, key_blocks, precision=highest)
    numerator = outside[..., None] * jnp.einsum('chvk,hctk->hctv', memory_in, query_blocks, precision=highest)
    numerator = numerator + jnp.einsum('hcts,hcsv->hctv', scores, value_blocks, precision=highest)
    denominator = outside * jnp.einsum('chk,hctk->hct', normal_in, query_blocks, precision=highest) + lax.optimization_barrier(jnp.sum(scores, axis=-1))
    result = numerator / jnp.maximum(jnp.abs(denominator), 1.0)[..., None]
    return result.transpose(1, 2, 0, 3).reshape(token_count, head_count * head_width).astype(jnp.bfloat16)

def differential(query_first, query_second, key_first, key_second, values, lambdas, head_gain):
    token_count = query_first.shape[0]
    query_span = min(512, token_count)
    score_scale = DD ** (-0.5)
    key_positions = jnp.arange(token_count, dtype=jnp.int32)

    def per_head(head_entry):
        head_query_first, head_query_second, head_key_first, head_key_second, value_head, factor = head_entry

        def per_block(block_index):
            first_row = block_index * query_span
            query_positions = first_row + jnp.arange(query_span, dtype=jnp.int32)
            visible = key_positions[None, :] <= query_positions[:, None]
            results = []
            for query_side, key_side in ((head_query_first, head_key_first), (head_query_second, head_key_second)):
                query_block = lax.dynamic_slice_in_dim(query_side, first_row, query_span, 0)
                scores = jnp.dot(query_block, key_side.T, preferred_element_type=jnp.float32) * score_scale
                scores = jnp.where(visible, scores, NEGATIVE)
                row_max = lax.optimization_barrier(jnp.max(scores, axis=1, keepdims=True))
                weights = jnp.where(visible, jnp.exp(scores - row_max), 0.0)
                totals = lax.optimization_barrier(jnp.sum(weights, axis=1, keepdims=True))
                results.append(jnp.dot(weights.astype(jnp.bfloat16), value_head, preferred_element_type=jnp.float32) / totals)
            return results[0] - factor * results[1]
        return lax.map(per_block, jnp.arange(token_count // query_span, dtype=jnp.int32))
    entries = (query_first.transpose(1, 0, 2), query_second.transpose(1, 0, 2), key_first.transpose(1, 0, 2), key_second.transpose(1, 0, 2), values.transpose(1, 0, 2), lambdas)
    stacked = lax.map(per_head, entries)
    head_count = stacked.shape[0]
    stacked = stacked.reshape(head_count, token_count, -1).transpose(1, 0, 2)
    norm_scale = lax.rsqrt(lax.optimization_barrier(jnp.mean(stacked * stacked, axis=-1, keepdims=True)) + EPSILON)
    return (stacked * norm_scale * head_gain).astype(jnp.bfloat16).reshape(token_count, -1)

def reference(inputs, norm_gain, query_weight, key_weight, value_weight, memory_query_weight, memory_key_weight, memory_value_weight, input_gate_weight, forget_gate_weight, forget_bias, decay_shift, lambdas, head_gain, out_weight_attention, out_weight_memory):
    token_count = inputs.shape[0]
    floats = inputs.astype(jnp.float32)
    inverse_rms = lax.rsqrt(lax.optimization_barrier(jnp.mean(floats * floats, axis=1, keepdims=True)) + EPSILON)
    scaled = (floats * norm_gain[None, :]).astype(jnp.bfloat16)

    def project(weight):
        return jnp.dot(scaled, weight, preferred_element_type=jnp.float32) * inverse_rms

    def split_heads(weight):
        return project(weight).astype(jnp.bfloat16).reshape(token_count, -1, HEAD)
    positions = jnp.arange(token_count, dtype=jnp.int32)
    queries = split_heads(query_weight)
    key_heads = split_heads(key_weight)
    values = split_heads(value_weight)
    attended = differential(rotate(queries[..., :DD], positions), rotate(queries[..., DD:], positions), rotate(key_heads[..., :DD], positions), rotate(key_heads[..., DD:], positions), values, lambdas, head_gain)
    gate_in = project(input_gate_weight)
    log_forget = jax.nn.log_sigmoid(project(forget_gate_weight) + forget_bias[None, :]) + decay_shift
    head_count = gate_in.shape[1]
    entering = (jnp.zeros((head_count, HEAD, HEAD), jnp.float32), jnp.zeros((head_count, HEAD), jnp.float32), jnp.zeros((head_count,), jnp.float32))
    memory = memory_blocks(split_heads(memory_query_weight), split_heads(memory_key_weight), split_heads(memory_value_weight), gate_in, log_forget, entering)
    attended_width = attended.shape[1] // N_TP
    memory_width = memory.shape[1] // N_TP
    combined = jnp.zeros((token_count, out_weight_attention.shape[1]), jnp.float32)
    for group_index in range(N_TP):
        low_a = group_index * attended_width
        low_m = group_index * memory_width
        partial_sum = jnp.dot(attended[:, low_a:low_a + attended_width], out_weight_attention[low_a:low_a + attended_width], preferred_element_type=jnp.float32)
        partial_sum = partial_sum + jnp.dot(memory[:, low_m:low_m + memory_width], out_weight_memory[low_m:low_m + memory_width], preferred_element_type=jnp.float32)
        combined = combined + lax.optimization_barrier(partial_sum.astype(jnp.bfloat16)).astype(jnp.float32)
    return combined.astype(jnp.bfloat16)
```

```python
import functools

import jax
import jax.numpy as jnp
from jax import lax
from jax.experimental import pallas as pl
from jax.experimental.pallas import tpu as pltpu
from jax.sharding import PartitionSpec as P

HEAD = 64
DD = 32
EPSILON = 1e-06
ROTARY_BASE = 10000.0
NEGATIVE = -1e30
LOG2E = 1.4426950408889634
CORES = 2
STATE_ROWS = HEAD + 8
VALUE_ROWS = HEAD + 16
VMEM = pl.BlockSpec(memory_space=pltpu.VMEM)
MESH = pl.DeviceIdType.MESH
VMEM_LIMIT = 60 * 1024 * 1024
TILE = 256


def signal(semaphore, axis, place):
    pl.semaphore_signal(semaphore, inc=1, device_id={axis: place}, device_id_type=MESH)


def remote(source, target, send_sem, recv_sem, axis, place):
    return pltpu.make_async_remote_copy(
        src_ref=source,
        dst_ref=target,
        send_sem=send_sem,
        recv_sem=recv_sem,
        device_id={axis: place},
        device_id_type=MESH,
    )


def head_mask(width, head):
    lanes = lax.broadcasted_iota(jnp.int32, (1, width), 1)
    return (lanes // HEAD) == head


def spread(columns, width):
    spreaded = columns[:, 0:1]
    for head in range(1, columns.shape[1]):
        lanes = lax.broadcasted_iota(jnp.int32, (1, width), 1)
        spreaded = jnp.where(lanes >= head * HEAD, columns[:, head : head + 1], spreaded)
    return jnp.broadcast_to(spreaded, (columns.shape[0], width))


def two_parts(floats):
    high = floats.astype(jnp.bfloat16)
    return high, (floats - high.astype(jnp.float32)).astype(jnp.bfloat16)


def dot(a, b, dims=((1,), (0,))):
    return lax.dot_general(a, b, (dims, ((), ())), preferred_element_type=jnp.float32)


def near_first(place, count, rank):
    both = jnp.minimum(place, count - 1 - place)
    half = (rank + 1) // 2
    alternating = jnp.where(rank % 2 == 1, place - half, place + half)
    one_sided = jnp.where(place < count - 1 - place, rank, count - 1 - rank)
    return jnp.where(rank <= 2 * both, alternating, one_sided)


def layer_kernel(
    size, depth, across, chunks, out_chunks,
    shard_ref, gain_ref, cos_ref, sin_ref, wq, wk, wv, wmq, wmk, wmv, wi, wf, bias_ref, shift_ref,
    lambda_ref, head_gain_ref, woa, wom,
    out_ref,
    sq, sk, sv, smq, smk, smv, soa, som, x_ref, scaled_ref, square_ref, sum_ref, cosine_ref, sine_ref,
    kv_out, q_out, kv_all, q_all, vt_ref, qb_ref, top_ref, acc_ref, att_out, attended_ref,
    mq_ref, mk_ref, mv_ref, pre_ref, states_ref, prefix_in, prefix_out, enter_ref,
    inner_ref, inner_den, inner_top, cumulative_ref, offset_ref, memory_ref,
    part_ref, pair_in, line_out, line_in,
    load_sems, line_send, line_recv, pair_send, pair_recv,
    kv_send, fwd_send, kv_recv, q_send, q_recv, att_send, att_recv,
    st_send, st_recv, px_send, px_recv,
    sp_send, sp_recv, sl_send, sl_recv,
):
    rows, columns = shard_ref.shape
    features = x_ref.shape[1]
    width = mq_ref.shape[1]
    heads = width // HEAD
    groups = width // 128
    lines = size // CORES
    spans = depth * across
    parts = spans // heads
    span = rows // chunks
    packed = span // 2

    tp = lax.axis_index("tp")
    core = lax.rem(tp, CORES)
    line = tp // CORES
    pair = line * CORES + (1 - core)
    me = lax.axis_index("sp")
    z = me // across
    x = lax.rem(me, across)
    my_head = me // parts
    my_part = lax.rem(me, parts)

    def owner_of(place):
        place_part = lax.rem(place, parts)
        return jnp.where((place // parts) % 2 == 0, place_part, parts - 1 - place_part)

    loads = []
    for place, (source, target) in enumerate(
        ((wk, sk), (wv, sv), (wq, sq), (wmk, smk), (wmv, smv), (wmq, smq), (woa, soa), (wom, som))
    ):
        copy = pltpu.make_async_copy(source, target, load_sems.at[place])
        copy.start()
        loads.append(copy)

    barrier = pltpu.get_barrier_semaphore()
    signal(barrier, "tp", pair)
    for step in range(1, lines):
        signal(barrier, "tp", lax.rem(line + step, lines) * CORES + core)
    for step in range(1, spans):
        signal(barrier, "sp", lax.rem(me + step, spans))

    cosine_ref[...] = jnp.concatenate([cos_ref[...]] * (128 * 2 // DD), axis=0).T
    sine_ref[...] = jnp.concatenate([-sin_ref[...], sin_ref[...]] * (128 // DD), axis=0).T
    lanes = lax.broadcasted_iota(jnp.int32, (1, 128), 1)
    former = lax.rem(lanes, DD) < DD // 2
    low_lanes = lanes < HEAD

    def columns_of(owner):
        return pl.ds(pl.multiple_of(owner * columns, 128), columns)

    def rows_of(chunk):
        return pl.ds(chunk * span, span)

    def place(owner, chunk):
        return x_ref.at[rows_of(chunk), columns_of(owner)]

    pl.semaphore_wait(barrier, lines + spans - 1)

    sends = []
    pairs = {}
    for chunk in range(chunks):
        for step in range(1, lines):
            copy = remote(
                shard_ref.at[rows_of(chunk)], place(tp, chunk), line_send.at[step, chunk],
                line_recv.at[step, chunk], "tp", lax.rem(line + step, lines) * CORES + core,
            )
            copy.start()
            sends.append(copy)
    for chunk in range(chunks):
        copy = remote(
            shard_ref.at[rows_of(chunk)], place(tp, chunk), pair_send.at[0, chunk],
            pair_recv.at[0, chunk], "tp", pair,
        )
        copy.start()
        pairs[0, chunk] = copy

    def take(values, at_rows, owner):
        floats = values.astype(jnp.float32)
        scaled_ref[at_rows, columns_of(owner)] = (floats * gain_ref[:, columns_of(owner)]).astype(
            jnp.bfloat16
        )
        return jnp.sum(floats * floats, axis=1, keepdims=True)

    everywhere = pl.ds(0, rows)
    squares = take(shard_ref[...], everywhere, tp)
    for chunk in range(chunks):
        pairs[0, chunk].wait_recv()
    square_ref[...] = squares + take(x_ref[:, columns_of(pair)], everywhere, pair)

    def line_columns(owner_line):
        return pl.ds(pl.multiple_of(owner_line * CORES * columns, 128), CORES * columns)

    weights = (sk, sv, sq, smk, smv, smq)
    for index, weight in enumerate(weights):
        loads[index].wait()
        sum_ref[:, index * width : (index + 1) * width] = dot(
            scaled_ref[:, line_columns(line)], weight[line_columns(line), :]
        )

    gate_weights = jnp.concatenate([wi[...], wf[...]], axis=0)
    factor = (DD**-0.5) * LOG2E

    def rotated(wide, cosine, sine):
        partner = jnp.where(former, pltpu.roll(wide, 128 - DD // 2, 1), pltpu.roll(wide, DD // 2, 1))
        return wide * cosine + partner * sine

    def kv_sends(chunk):
        for rank in range(heads - 1, 0, -1):
            head = near_first(my_head, heads, rank)
            yield remote(
                kv_out.at[head, rows_of(chunk)], kv_all.at[me, rows_of(chunk)],
                kv_send.at[rank, chunk], kv_recv.at[me, chunk], "sp", head * parts + my_part,
            )

    def forwards(source, origin, index, chunk):
        for step in range(1, parts):
            yield remote(
                source, kv_all.at[origin, rows_of(chunk)], fwd_send.at[index, step, chunk],
                kv_recv.at[origin, chunk], "sp",
                my_head * parts + lax.rem(my_part + step, parts),
            )

    packed_of = lambda chunk: pl.ds(chunk * packed, packed)
    my_slot = me // parts
    my_owner = owner_of(me)

    def q_sends(chunk):
        for rank in range(heads - 1, 0, -1):
            head = near_first(my_head, heads, rank)
            yield remote(
                q_out.at[head, packed_of(chunk)], q_all.at[my_slot, packed_of(chunk)],
                q_send.at[rank, chunk], q_recv.at[my_slot, chunk], "sp", head * parts + my_owner,
            )

    def q_aside(chunk):
        return remote(
            q_out.at[my_head, packed_of(chunk)], q_all.at[my_slot, packed_of(chunk)],
            q_send.at[0, chunk], q_recv.at[my_slot, chunk], "sp", my_head * parts + my_owner,
        )

    for chunk in range(chunks):
        at = rows_of(chunk)
        for step in range(1, lines):
            source = lax.rem(line + lines - step, lines) * CORES + core
            remote(
                place(source, chunk), place(source, chunk), line_send.at[step, chunk],
                line_recv.at[step, chunk], "tp", pair,
            ).wait_recv()
            copy = remote(
                place(source, chunk), place(source, chunk), pair_send.at[step, chunk],
                pair_recv.at[step, chunk], "tp", pair,
            )
            copy.start()
            pairs[step, chunk] = copy
        squares = square_ref[at]
        for step in range(1, lines):
            source = lax.rem(line + lines - step, lines) * CORES + core
            squares = squares + take(x_ref[at, columns_of(source)], at, source)
        for step in range(1, lines):
            source = lax.rem(line + lines - step, lines) * CORES + 1 - core
            pairs[step, chunk].wait_recv()
            squares = squares + take(x_ref[at, columns_of(source)], at, source)
        inverse = lax.rsqrt(squares / features + EPSILON)

        def product(index):
            total = sum_ref[at, index * width : (index + 1) * width]
            for step in range(1, lines):
                other = line_columns(lax.rem(line + step, lines))
                total = total + dot(scaled_ref[at, other], weights[index][other, :])
            return (total * inverse).astype(jnp.bfloat16).astype(jnp.float32)

        cosine = cosine_ref[at]
        sine = sine_ref[at]
        keys = product(0)
        values = product(1)
        for group in range(groups):
            lane_group = slice(group * 128, group * 128 + 128)
            key = rotated(keys[:, lane_group], cosine, sine)
            value = values[:, lane_group]
            kv_out[2 * group, at] = jnp.where(low_lanes, key, pltpu.roll(value, HEAD, 1)).astype(
                jnp.bfloat16
            )
            kv_out[2 * group + 1, at] = jnp.where(
                low_lanes, pltpu.roll(key, HEAD, 1), value
            ).astype(jnp.bfloat16)
        for copy in kv_sends(chunk):
            copy.start()
        for copy in forwards(kv_out.at[my_head, at], me, my_head, chunk):
            copy.start()
        kv_all[me, at] = kv_out[my_head, at]

        queries = product(2)
        for group in range(groups):
            query = rotated(queries[:, group * 128 : group * 128 + 128], cosine, sine) * factor
            top, bottom = query[:packed], query[packed:]
            q_out[2 * group, packed_of(chunk)] = jnp.where(
                low_lanes, top, pltpu.roll(bottom, HEAD, 1)
            ).astype(jnp.bfloat16)
            q_out[2 * group + 1, packed_of(chunk)] = jnp.where(
                low_lanes, pltpu.roll(top, HEAD, 1), bottom
            ).astype(jnp.bfloat16)
        for copy in q_sends(chunk):
            copy.start()

        @pl.when(my_owner == my_part)
        def _():
            q_all[my_slot, packed_of(chunk)] = q_out[my_head, packed_of(chunk)]

        @pl.when(my_owner != my_part)
        def _():
            q_aside(chunk).start()

        mk_ref[at] = product(3).astype(jnp.bfloat16)
        mv_ref[at] = product(4).astype(jnp.bfloat16)
        mq_ref[at] = product(5).astype(jnp.bfloat16)
        pre_ref[at, : 2 * heads] = dot(scaled_ref[at, :], gate_weights, ((1,), (1,))) * inverse

    gate = pre_ref[:, :heads]
    pre = pre_ref[:, heads : 2 * heads] + bias_ref[...]
    shift = shift_ref[...]
    shift = jnp.concatenate(
        [shift, jnp.zeros((128 - shift.shape[0], rows), jnp.float32)], axis=0
    ).T[:, : shift.shape[0]]
    forget = jnp.minimum(pre, 0.0) - jnp.log1p(jnp.exp(-jnp.abs(pre))) + shift
    row_index = lax.broadcasted_iota(jnp.int32, (rows, rows), 0)
    column_index = lax.broadcasted_iota(jnp.int32, (rows, rows), 1)
    lower = column_index <= row_index
    lower_ones = lower.astype(jnp.bfloat16)
    first, rest = two_parts(forget)
    second = (forget - first.astype(jnp.float32) - rest.astype(jnp.float32)).astype(jnp.bfloat16)
    cumulative = dot(lower_ones, first) + (dot(lower_ones, rest) + dot(lower_ones, second))
    cumulative_ref[:, :heads] = cumulative
    offsets = jnp.concatenate(
        [gate - cumulative, jnp.zeros((rows, 128 - heads), jnp.float32)], axis=1
    )
    offset_ref[...] = offsets.T[:8, :]
    end = cumulative[rows - 1 : rows, :]
    toward = end - cumulative + gate
    top = jnp.max(toward, axis=0, keepdims=True)
    end_weights = spread(jnp.exp(toward - top), width)
    keyed = mk_ref[...].astype(jnp.float32) * (HEAD**-0.5) * end_weights
    high, low = two_parts(keyed)
    whole = dot(high, mv_ref[...], ((0,), (0,))) + dot(low, mv_ref[...], ((0,), (0,)))
    memory = jnp.zeros((HEAD, width), jnp.float32)
    for head in range(heads):
        memory = jnp.where(
            head_mask(width, head), whole[head * HEAD : (head + 1) * HEAD, :], memory
        )
    states_ref[x, :HEAD, :] = memory
    states_ref[x, HEAD : HEAD + 1, :] = jnp.sum(keyed, axis=0, keepdims=True)
    states_ref[x, HEAD + 1 : HEAD + 2, :] = spread(top, width)
    states_ref[x, HEAD + 2 : HEAD + 3, :] = spread(end, width)
    states_ref[x, HEAD + 3 :, :] = jnp.zeros((STATE_ROWS - HEAD - 3, width), jnp.float32)

    def state_sends():
        for step in range(1, across):
            yield remote(
                states_ref.at[x], states_ref.at[x], st_send.at[step], st_recv.at[x], "sp",
                z * across + lax.rem(x + step, across),
            )

    for copy in state_sends():
        copy.start()

    for group in range(groups):
        lane_group = slice(group * 128, (group + 1) * 128)
        keys = mk_ref[:, lane_group]
        values = mv_ref[:, lane_group]
        group_queries = mq_ref[:, lane_group]
        result = None
        for side in range(2):
            head = group * 2 + side
            chosen = (lanes // HEAD) == side
            column = cumulative[:, head : head + 1]
            gaps = jnp.where(lower, column + offset_ref[head : head + 1, :], NEGATIVE)
            row_top = jnp.max(gaps, axis=1, keepdims=True)
            within = jnp.exp(gaps - row_top)
            scores = dot(jnp.where(chosen, group_queries, 0), keys, ((1,), (1,)))
            scores = jnp.where(lower, within * (scores * (HEAD**-0.5)), 0.0)
            inner_den[:, head : head + 1] = jnp.sum(scores, axis=1, keepdims=True)
            inner_top[:, head : head + 1] = row_top
            score_high, score_low = two_parts(scores)
            numerator = dot(score_high, values) + dot(score_low, values)
            result = numerator if result is None else jnp.where(chosen, numerator, result)
        inner_ref[:, lane_group] = result

    def advance(body, stable, later):
        later_top = later[HEAD + 1 : HEAD + 2, :]
        decay = later[HEAD + 2 : HEAD + 3, :]
        new = jnp.maximum(decay + stable, later_top)
        return jnp.exp(decay + stable - new) * body + jnp.exp(later_top - new) * later, new

    def prefix_send():
        return remote(
            prefix_out, prefix_in, px_send, px_recv, "sp", jnp.minimum(me + across, spans - 1)
        )

    def level(body, stable):
        for other in range(across):

            @pl.when(x == other)
            def _():
                enter_ref[...] = body
                enter_ref[HEAD + 1 : HEAD + 2, :] = stable

            if other < across - 1:
                body, stable = advance(body, stable, states_ref[other])
        body, stable = advance(body, stable, states_ref[across - 1])

        @pl.when(z < depth - 1)
        def _():
            prefix_out[...] = body
            prefix_out[HEAD + 1 : HEAD + 2, :] = stable
            prefix_send().start()

    for step in range(1, across):
        other = lax.rem(x + step, across)
        remote(
            states_ref.at[other], states_ref.at[other], st_send.at[step], st_recv.at[other], "sp", me
        ).wait_recv()

    @pl.when(z == 0)
    def _():
        level(jnp.zeros((STATE_ROWS, width), jnp.float32), jnp.zeros((1, width), jnp.float32))

    def chain():
        prefix_send().wait_recv()
        body = prefix_in[...]
        level(body, body[HEAD + 1 : HEAD + 2, :])

    top_ref[...] = jnp.full(top_ref.shape, NEGATIVE, jnp.float32)
    acc_ref[...] = jnp.zeros(acc_ref.shape, jnp.float32)
    query_width = 2 * rows
    tiles = [slice(start, min(start + TILE, query_width)) for start in range(0, query_width, TILE)]

    def block(slot, place, diagonal):
        def score(tile):
            scores = dot(kv_all[place], qb_ref[slot, tile], ((1,), (1,)))
            if diagonal:
                shape = scores.shape
                key_index = lax.broadcasted_iota(jnp.int32, shape, 0)
                query_index = lax.broadcasted_iota(jnp.int32, shape, 1) + tile.start
                query_index = jnp.where(query_index >= rows, query_index - rows, query_index)
                scores = jnp.where(key_index <= query_index, scores, NEGATIVE)
            return scores

        def soften(tile, scores):
            old_top = top_ref[slot, :, tile]
            top = jnp.maximum(jnp.max(scores, axis=0, keepdims=True), old_top)
            return top, jnp.exp2(old_top - top), jnp.exp2(scores - top).astype(jnp.bfloat16)

        def gather_up(tile, top, shrink, weights):
            sums = dot(vt_ref[place], weights)
            acc_ref[slot, :, tile] = acc_ref[slot, :, tile] * shrink + sums
            top_ref[slot, :, tile] = top

        scores = score(tiles[0])
        held = None
        for index, tile in enumerate(tiles):
            following = score(tiles[index + 1]) if index + 1 < len(tiles) else None
            if held is not None:
                gather_up(tiles[index - 1], *held)
            held = soften(tile, scores)
            scores = following
        gather_up(tiles[-1], *held)

    def visit_place(rank):
        level_rank = rank // across
        return near_first(z, depth, level_rank) * across + lax.rem(
            x + lax.rem(rank, across), across
        )

    def arrive(origin):
        for chunk in range(chunks):
            remote(
                kv_all.at[origin, rows_of(chunk)], kv_all.at[origin, rows_of(chunk)],
                kv_send.at[0, chunk], kv_recv.at[origin, chunk], "sp", me,
            ).wait_recv()

            @pl.when(lax.rem(origin, parts) == my_part)
            def _():
                for copy in forwards(
                    kv_all.at[origin, rows_of(chunk)], origin, origin // parts, chunk
                ):
                    copy.start()

    def visit(rank, unused):
        origin = visit_place(rank)
        slot = origin // parts
        owned = owner_of(origin) == my_part
        pl.when(origin != me)(lambda: arrive(origin))
        turned = kv_all[origin].T
        vt_ref[origin, :HEAD, :] = turned[HEAD:, :]
        vt_ref[origin, HEAD:, :] = jnp.ones((VALUE_ROWS - HEAD, rows), jnp.bfloat16)

        @pl.when(owned)
        def _():
            @pl.when(origin != me)
            def _():
                for chunk in range(chunks):
                    at = q_all.at[slot, packed_of(chunk)]
                    remote(
                        at, at, q_send.at[0, chunk], q_recv.at[slot, chunk], "sp", me
                    ).wait_recv()

            for chunk in range(chunks):
                low_rows = q_all[slot, packed_of(chunk)].astype(jnp.float32)
                high_rows = pltpu.roll(low_rows, HEAD, 1)
                for half in range(2):
                    chosen = (lanes // DD) == half
                    for side, values in enumerate((low_rows, high_rows)):
                        qb_ref[
                            slot, pl.ds(half * rows + chunk * span + side * packed, packed)
                        ] = jnp.where(chosen, values, 0.0).astype(jnp.bfloat16)

            block(slot, origin, True)

        def earlier(other_rank, unused):
            other = visit_place(other_rank)
            query = jnp.maximum(origin, other)
            key = jnp.minimum(origin, other)

            @pl.when(owner_of(query) == my_part)
            def _():
                block(query // parts, key, False)

            return unused

        lax.fori_loop(0, rank, earlier, 0)
        pl.when((z > 0) & (rank == 2 * z - 1))(chain)
        return unused

    lax.fori_loop(0, spans, visit, 0)

    eye = lax.broadcasted_iota(jnp.int32, (HEAD, HEAD), 0) == lax.broadcasted_iota(
        jnp.int32, (HEAD, HEAD), 1
    )
    head_gain = jnp.sum(jnp.where(eye, head_gain_ref[...], 0.0), axis=1, keepdims=True)
    head_lanes = lax.broadcasted_iota(jnp.int32, lambda_ref.shape, 1)
    factor_second = jnp.sum(
        jnp.where(head_lanes == my_head, lambda_ref[...], 0.0), axis=1, keepdims=True
    )

    def span_of(slot):
        return slot * parts + (my_part if slot % 2 == 0 else parts - 1 - my_part)

    def att_copy(slot):
        return remote(
            att_out.at[slot], attended_ref.at[pl.ds(pl.multiple_of(my_head * HEAD, HEAD), HEAD)],
            att_send.at[slot], att_recv.at[my_head], "sp", span_of(slot),
        )

    for slot in range(heads):
        first, second = (
            acc_ref[slot, :HEAD, half * rows : (half + 1) * rows]
            / acc_ref[slot, HEAD : HEAD + 1, half * rows : (half + 1) * rows]
            for half in range(2)
        )
        difference = first - factor_second * second
        mean = jnp.mean(difference * difference, axis=0, keepdims=True)
        att_out[slot] = (difference * lax.rsqrt(mean + EPSILON) * head_gain).astype(jnp.bfloat16)

        @pl.when(span_of(slot) == me)
        def _():
            attended_ref[pl.ds(pl.multiple_of(my_head * HEAD, HEAD), HEAD), :] = att_out[slot]

        @pl.when(span_of(slot) != me)
        def _():
            att_copy(slot).start()

    stable = enter_ref[HEAD + 1 : HEAD + 2, :]
    memory_in = enter_ref[:HEAD, :]
    normal_in = enter_ref[HEAD : HEAD + 1, :]
    blocks = jnp.concatenate(
        [jnp.where(head_mask(width, head), memory_in, 0.0) for head in range(heads)], axis=0
    )
    high, low = two_parts(blocks)
    memory_queries = mq_ref[...]
    carried_part = dot(memory_queries, high) + dot(memory_queries, low)
    weighted = memory_queries.astype(jnp.float32) * normal_in
    for group in range(groups):
        lane_group = slice(group * 128, (group + 1) * 128)
        result = None
        for side in range(2):
            head = group * 2 + side
            chosen = (lanes // HEAD) == side
            column = slice(head, head + 1)
            carried_log = cumulative_ref[:, column] + stable[:, head * HEAD : head * HEAD + 1]
            own_top = inner_top[:, column]
            row_top = jnp.maximum(carried_log, own_top)
            inside = jnp.exp(own_top - row_top)
            outside = jnp.exp(carried_log - row_top)
            denominator = inside * inner_den[:, column] + outside * jnp.sum(
                jnp.where(chosen, weighted[:, lane_group], 0.0), axis=1, keepdims=True
            )
            numerator = inside * inner_ref[:, lane_group] + outside * carried_part[:, lane_group]
            quotient = numerator / jnp.maximum(jnp.abs(denominator), 1.0)
            result = quotient if result is None else jnp.where(chosen, quotient, result)
        memory_ref[:, lane_group] = result.astype(jnp.bfloat16)

    loads[6].wait()
    loads[7].wait()
    for step in range(heads):
        here = (my_owner != my_part) | (my_head != step)

        @pl.when(here)
        def _():
            at = attended_ref.at[pl.ds(step * HEAD, HEAD)]
            remote(at, at, att_send.at[0], att_recv.at[step], "sp", me).wait_recv()

    out_span = rows // out_chunks

    def out_rows(chunk):
        return pl.ds(chunk * out_span, out_span)

    order = list(range(1, lines)) + [0]
    swaps = {}
    lined = {}

    def pair_sum(step, chunk):
        swaps[step, chunk].wait_recv()
        mine = part_ref[
            out_rows(chunk), columns_of(lax.rem(line + step, lines) * CORES + core)
        ]
        return mine.astype(jnp.float32) + pair_in[step, out_rows(chunk), :].astype(jnp.float32)

    def pass_on(chunk):
        for step in range(1, lines):
            line_out[step, out_rows(chunk), :] = pair_sum(step, chunk).astype(jnp.bfloat16)
            copy = remote(
                line_out.at[step, out_rows(chunk)], line_in.at[step, out_rows(chunk)],
                sl_send.at[step, chunk], sl_recv.at[step, chunk], "tp",
                lax.rem(line + step, lines) * CORES + core,
            )
            copy.start()
            lined[step, chunk] = copy

    for chunk in range(out_chunks):
        at = slice(chunk * out_span, (chunk + 1) * out_span)
        part_ref[at, :] = (
            dot(attended_ref[:, at], soa[...], ((0,), (0,))) + dot(memory_ref[at, :], som[...])
        ).astype(jnp.bfloat16)
        for step in order:
            target = lax.rem(line + step, lines) * CORES + (1 - core)
            copy = remote(
                part_ref.at[out_rows(chunk), columns_of(target)],
                pair_in.at[step, out_rows(chunk)], sp_send.at[step, chunk],
                sp_recv.at[step, chunk], "tp", pair,
            )
            copy.start()
            swaps[step, chunk] = copy
        if chunk > 0:
            pass_on(chunk - 1)
    pass_on(out_chunks - 1)

    for copy in sends:
        copy.wait_send()
    for copy in pairs.values():
        copy.wait_send()
    for chunk in range(chunks):
        for copy in kv_sends(chunk):
            copy.wait_send()
        for copy in q_sends(chunk):
            copy.wait_send()
        for index in range(heads):
            for copy in forwards(kv_all.at[0, rows_of(chunk)], 0, index, chunk):
                copy.wait_send()

        @pl.when(my_owner != my_part)
        def _():
            q_aside(chunk).wait_send()

    for copy in state_sends():
        copy.wait_send()
    pl.when(z < depth - 1)(lambda: prefix_send().wait_send())
    for slot in range(heads):

        @pl.when(span_of(slot) != me)
        def _():
            att_copy(slot).wait_send()

    for chunk in range(out_chunks):
        total = pair_sum(0, chunk)
        for step in range(1, lines):
            lined[step, chunk].wait_recv()
            total = total + line_in[step, out_rows(chunk), :].astype(jnp.float32)
        out_ref[out_rows(chunk), :] = total.astype(jnp.bfloat16)
    for copy in swaps.values():
        copy.wait_send()
    for copy in lined.values():
        copy.wait_send()


def per_device(tp_size, depth, across, inputs, norm_gain, query_weight, key_weight, value_weight,
               memory_query_weight, memory_key_weight, memory_value_weight, input_gate_weight,
               forget_gate_weight, forget_bias, decay_shift, lambdas, head_gain,
               out_weight_attention, out_weight_memory):
    rows, columns = inputs.shape
    features = norm_gain.shape[0]
    width = query_weight.shape[1]
    heads = width // HEAD
    lines = tp_size // CORES
    spans = depth * across
    parts = spans // heads
    chunks = 4
    out_chunks = 3
    dma = pltpu.SemaphoreType.DMA

    middle = DD // 2
    inverse = 1.0 / ROTARY_BASE ** (jnp.arange(middle, dtype=jnp.float32) / middle)
    positions = lax.axis_index("sp") * rows + jnp.arange(rows, dtype=jnp.int32)
    angles = inverse[:, None] * positions.astype(jnp.float32)[None, :]
    cosine = jnp.cos(angles)
    sine = jnp.sin(angles)

    hbm = pl.BlockSpec(memory_space=pl.ANY)
    bf16 = lambda *shape: pltpu.VMEM(shape, jnp.bfloat16)
    f32 = lambda *shape: pltpu.VMEM(shape, jnp.float32)
    return pl.pallas_call(
        functools.partial(layer_kernel, tp_size, depth, across, chunks, out_chunks),
        out_shape=jax.ShapeDtypeStruct((rows, columns), jnp.bfloat16),
        in_specs=[VMEM] * 4 + [hbm] * 6 + [VMEM] * 6 + [hbm] * 2,
        out_specs=VMEM,
        scratch_shapes=[bf16(features, width)] * 6
        + [bf16(width, features)] * 2
        + [
            bf16(rows, features), bf16(rows, features), f32(rows, 1), f32(rows, 6 * width),
            f32(rows, 128), f32(rows, 128),
            bf16(heads, rows, 128), bf16(heads, rows // 2, 128), bf16(spans, rows, 128),
            bf16(heads, rows // 2, 128), bf16(spans, VALUE_ROWS, rows),
            bf16(heads, 2 * rows, 128), f32(heads, 1, 2 * rows), f32(heads, VALUE_ROWS, 2 * rows),
            bf16(heads, HEAD, rows), bf16(width, rows),
            bf16(rows, width), bf16(rows, width), bf16(rows, width), f32(rows, 128),
            f32(across, STATE_ROWS, width), f32(STATE_ROWS, width), f32(STATE_ROWS, width),
            f32(STATE_ROWS, width),
            f32(rows, width), f32(rows, 128), f32(rows, 128), f32(rows, 128), f32(8, rows),
            bf16(rows, width),
            bf16(rows, features), bf16(lines, rows, columns), bf16(lines, rows, columns),
            bf16(lines, rows, columns),
            dma((8,)), dma((lines, chunks)), dma((lines, chunks)), dma((lines, chunks)),
            dma((lines, chunks)),
            dma((heads, chunks)), dma((heads, parts, chunks)), dma((spans, chunks)),
            dma((heads, chunks)), dma((heads, chunks)), dma((heads,)), dma((heads,)),
            dma((across,)), dma((across,)), dma(()), dma(()),
            dma((lines, out_chunks)), dma((lines, out_chunks)), dma((lines, out_chunks)),
            dma((lines, out_chunks)),
        ],
        compiler_params=pltpu.CompilerParams(
            vmem_limit_bytes=VMEM_LIMIT, collective_id=0, has_side_effects=True
        ),
        name="layer",
    )(
        inputs, norm_gain[None, :], cosine, sine, query_weight, key_weight, value_weight,
        memory_query_weight, memory_key_weight, memory_value_weight, input_gate_weight.T,
        forget_gate_weight.T, forget_bias[None, :], decay_shift.T, lambdas[None, :],
        head_gain[None, :], out_weight_attention, out_weight_memory,
    )


def columns_across(mesh):
    spans = mesh.shape["sp"]
    try:
        places = {device.coords[0] for device in mesh.devices.flat}
        across = len(places)
    except AttributeError:
        across = 2
    return across if spans % across == 0 else 1


def solution(mesh):
    across = columns_across(mesh)
    in_specs = (
        P("sp", "tp"),
        P(),
        P(None, "tp"),
        P(None, "tp"),
        P(None, "tp"),
        P(None, "tp"),
        P(None, "tp"),
        P(None, "tp"),
        P(None, "tp"),
        P(None, "tp"),
        P("tp"),
        P("sp", "tp"),
        P("tp"),
        P(),
        P("tp", None),
        P("tp", None),
    )
    return jax.shard_map(
        functools.partial(
            per_device, mesh.shape["tp"], mesh.shape["sp"] // across, across
        ),
        mesh=mesh,
        in_specs=in_specs,
        out_specs=P("sp", "tp"),
        check_vma=False,
    )
```

```python
import functools

import jax
import jax.numpy as jnp
from jax import lax
from jax.experimental import pallas as pl
from jax.experimental.pallas import tpu as pltpu
from jax.sharding import PartitionSpec as P

HEAD = 64
DD = 32
EPSILON = 1e-06
ROTARY_BASE = 10000.0
NEGATIVE = -1e30
LOG2E = 1.4426950408889634
CORES = 2
STATE_ROWS = HEAD + 8
VALUE_ROWS = HEAD + 16
VMEM = pl.BlockSpec(memory_space=pltpu.VMEM)
MESH = pl.DeviceIdType.MESH
VMEM_LIMIT = 60 * 1024 * 1024


def signal(semaphore, axis, place):
    pl.semaphore_signal(semaphore, inc=1, device_id={axis: place}, device_id_type=MESH)


def remote(source, target, send_sem, recv_sem, axis, place):
    return pltpu.make_async_remote_copy(
        src_ref=source,
        dst_ref=target,
        send_sem=send_sem,
        recv_sem=recv_sem,
        device_id={axis: place},
        device_id_type=MESH,
    )


def head_mask(width, head):
    lanes = lax.broadcasted_iota(jnp.int32, (1, width), 1)
    return (lanes // HEAD) == head


def spread(columns, width):
    spreaded = columns[:, 0:1]
    for head in range(1, columns.shape[1]):
        lanes = lax.broadcasted_iota(jnp.int32, (1, width), 1)
        spreaded = jnp.where(lanes >= head * HEAD, columns[:, head : head + 1], spreaded)
    return jnp.broadcast_to(spreaded, (columns.shape[0], width))


def two_parts(floats):
    high = floats.astype(jnp.bfloat16)
    return high, (floats - high.astype(jnp.float32)).astype(jnp.bfloat16)


def dot(a, b, dims=((1,), (0,))):
    return lax.dot_general(a, b, (dims, ((), ())), preferred_element_type=jnp.float32)


def near_first(place, count, rank):
    both = jnp.minimum(place, count - 1 - place)
    half = (rank + 1) // 2
    alternating = jnp.where(rank % 2 == 1, place - half, place + half)
    one_sided = jnp.where(place < count - 1 - place, rank, count - 1 - rank)
    return jnp.where(rank <= 2 * both, alternating, one_sided)


def layer_kernel(
    size, depth, across, chunks, out_chunks,
    shard_ref, gain_ref, cos_ref, sin_ref, wq, wk, wv, wmq, wmk, wmv, wi, wf, bias_ref, shift_ref,
    lambda_ref, head_gain_ref, woa, wom,
    out_ref,
    weight_ref, soa, som, x_ref, scaled_ref, square_ref, sum_ref, cosine_ref, sine_ref,
    kv_out, q_out, kv_all, q_all, vt_ref, qn_ref, qt_ref, top_ref, acc_ref, att_out, attended_ref,
    mq_ref, mk_ref, mv_ref, pre_ref, states_ref, prefix_in, prefix_out, enter_ref,
    inner_ref, inner_den, inner_top, cumulative_ref, offset_ref, memory_ref,
    partial_ref, part_ref, pair_in, line_out, line_in,
    load_sems, line_send, line_recv, pair_send, pair_recv,
    kv_send, fwd_send, kv_recv, q_send, q_recv, att_send, att_recv,
    st_send, st_recv, px_send, px_recv,
    sp_send, sp_recv, sl_send, sl_recv,
):
    rows, columns = shard_ref.shape
    features = x_ref.shape[1]
    width = mq_ref.shape[1]
    heads = width // HEAD
    groups = width // 128
    lines = size // CORES
    spans = depth * across
    parts = spans // heads
    span = rows // chunks
    packed = span // 2

    tp = lax.axis_index("tp")
    core = lax.rem(tp, CORES)
    line = tp // CORES
    pair = line * CORES + (1 - core)
    me = lax.axis_index("sp")
    z = me // across
    x = lax.rem(me, across)
    my_head = me // parts
    my_part = lax.rem(me, parts)

    def owner_of(place):
        place_part = lax.rem(place, parts)
        return jnp.where((place // parts) % 2 == 0, place_part, parts - 1 - place_part)

    loads = []
    for index, source in enumerate((wk, wv, wq, wmk, wmv, wmq)):
        loads.append(
            pltpu.make_async_copy(
                source, weight_ref.at[:, pl.ds(index * width, width)], load_sems.at[index]
            )
        )
    loads.append(pltpu.make_async_copy(woa, soa, load_sems.at[6]))
    loads.append(pltpu.make_async_copy(wom, som, load_sems.at[7]))
    for copy in loads:
        copy.start()

    barrier = pltpu.get_barrier_semaphore()
    signal(barrier, "tp", pair)
    for step in range(1, lines):
        signal(barrier, "tp", lax.rem(line + step, lines) * CORES + core)
    for step in range(1, spans):
        signal(barrier, "sp", lax.rem(me + step, spans))

    cosine_ref[...] = jnp.concatenate([cos_ref[...]] * (128 * 2 // DD), axis=0).T
    sine_ref[...] = jnp.concatenate([-sin_ref[...], sin_ref[...]] * (128 // DD), axis=0).T
    lanes = lax.broadcasted_iota(jnp.int32, (1, 128), 1)
    former = lax.rem(lanes, DD) < DD // 2
    low_lanes = lanes < HEAD

    def columns_of(owner):
        return pl.ds(pl.multiple_of(owner * columns, 128), columns)

    def rows_of(chunk):
        return pl.ds(chunk * span, span)

    def place(owner, chunk):
        return x_ref.at[rows_of(chunk), columns_of(owner)]

    pl.semaphore_wait(barrier, lines + spans - 1)

    sends = []
    pairs = {}
    for chunk in range(chunks):
        for step in range(1, lines):
            copy = remote(
                shard_ref.at[rows_of(chunk)], place(tp, chunk), line_send.at[step, chunk],
                line_recv.at[step, chunk], "tp", lax.rem(line + step, lines) * CORES + core,
            )
            copy.start()
            sends.append(copy)
    for chunk in range(chunks):
        copy = remote(
            shard_ref.at[rows_of(chunk)], place(tp, chunk), pair_send.at[0, chunk],
            pair_recv.at[0, chunk], "tp", pair,
        )
        copy.start()
        pairs[0, chunk] = copy

    def take(values, at_rows, owner):
        floats = values.astype(jnp.float32)
        scaled_ref[at_rows, columns_of(owner)] = (floats * gain_ref[:, columns_of(owner)]).astype(
            jnp.bfloat16
        )
        return jnp.sum(floats * floats, axis=1, keepdims=True)

    everywhere = pl.ds(0, rows)
    squares = take(shard_ref[...], everywhere, tp)
    for chunk in range(chunks):
        pairs[0, chunk].wait_recv()
    square_ref[...] = squares + take(x_ref[:, columns_of(pair)], everywhere, pair)

    def line_columns(owner_line):
        return pl.ds(pl.multiple_of(owner_line * CORES * columns, 128), CORES * columns)

    couples = [slice(index * width, (index + 2) * width) for index in (0, 2, 4)]
    for index, couple in enumerate(couples):
        loads[2 * index].wait()
        loads[2 * index + 1].wait()
        sum_ref[:, couple] = dot(
            scaled_ref[:, line_columns(line)], weight_ref[line_columns(line), couple]
        )

    gate_weights = jnp.concatenate([wi[...], wf[...]], axis=0)
    factor = (DD**-0.5) * LOG2E

    def rotated(wide, cosine, sine):
        partner = jnp.where(former, pltpu.roll(wide, 128 - DD // 2, 1), pltpu.roll(wide, DD // 2, 1))
        return wide * cosine + partner * sine

    def kv_sends(chunk):
        for rank in range(heads - 1, 0, -1):
            head = near_first(my_head, heads, rank)
            yield remote(
                kv_out.at[head, rows_of(chunk)], kv_all.at[me, rows_of(chunk)],
                kv_send.at[rank, chunk], kv_recv.at[me, chunk], "sp", head * parts + my_part,
            )

    def forwards(source, origin, index, chunk):
        for step in range(1, parts):
            yield remote(
                source, kv_all.at[origin, rows_of(chunk)], fwd_send.at[index, step, chunk],
                kv_recv.at[origin, chunk], "sp",
                my_head * parts + lax.rem(my_part + step, parts),
            )

    points = {
        (1, 0): "chunk2", (2, 0): "projected", (3, 0): "projected", (1, 1): "projected",
        (2, 1): "state", (1, 2): "state", (3, 1): "inner", (2, 2): "inner", (1, 3): "inner",
        (3, 2): "first", (2, 3): "second", (3, 3): "seconded",
    }

    def landed(rank):
        return near_first(my_head, heads, rank) * parts + my_part

    def forward(point, index=""):
        for chunk in range(chunks):
            for rank in range(1, heads):
                if points.get((rank, chunk), "inner") == f"{point}{index}":
                    origin = landed(rank)
                    at = kv_all.at[origin, rows_of(chunk)]
                    remote(
                        at, at, kv_send.at[0, chunk], kv_recv.at[origin, chunk], "sp", me
                    ).wait_recv()
                    for copy in forwards(at, origin, origin // parts, chunk):
                        copy.start()

    packed_of = lambda chunk: pl.ds(chunk * packed, packed)
    my_slot = me // parts
    my_owner = owner_of(me)

    def q_sends(chunk):
        for rank in range(heads - 1, 0, -1):
            head = near_first(my_head, heads, rank)
            yield remote(
                q_out.at[head, packed_of(chunk)], q_all.at[my_slot, packed_of(chunk)],
                q_send.at[rank, chunk], q_recv.at[my_slot, chunk], "sp", head * parts + my_owner,
            )

    def q_aside(chunk):
        return remote(
            q_out.at[my_head, packed_of(chunk)], q_all.at[my_slot, packed_of(chunk)],
            q_send.at[0, chunk], q_recv.at[my_slot, chunk], "sp", my_head * parts + my_owner,
        )

    for chunk in range(chunks):
        at = rows_of(chunk)
        for step in range(1, lines):
            source = lax.rem(line + lines - step, lines) * CORES + core
            remote(
                place(source, chunk), place(source, chunk), line_send.at[step, chunk],
                line_recv.at[step, chunk], "tp", pair,
            ).wait_recv()
            copy = remote(
                place(source, chunk), place(source, chunk), pair_send.at[step, chunk],
                pair_recv.at[step, chunk], "tp", pair,
            )
            copy.start()
            pairs[step, chunk] = copy
        squares = square_ref[at]
        for step in range(1, lines):
            source = lax.rem(line + lines - step, lines) * CORES + core
            squares = squares + take(x_ref[at, columns_of(source)], at, source)
        for step in range(1, lines):
            source = lax.rem(line + lines - step, lines) * CORES + 1 - core
            pairs[step, chunk].wait_recv()
            squares = squares + take(x_ref[at, columns_of(source)], at, source)
        inverse = lax.rsqrt(squares / features + EPSILON)

        def products(index):
            total = sum_ref[at, couples[index]]
            for step in range(1, lines):
                other = line_columns(lax.rem(line + step, lines))
                total = total + dot(scaled_ref[at, other], weight_ref[other, couples[index]])
            total = (total * inverse).astype(jnp.bfloat16).astype(jnp.float32)
            return total[:, :width], total[:, width:]

        cosine = cosine_ref[at]
        sine = sine_ref[at]
        keys, values = products(0)
        for group in range(groups):
            lane_group = slice(group * 128, group * 128 + 128)
            key = rotated(keys[:, lane_group], cosine, sine)
            value = values[:, lane_group]
            kv_out[2 * group, at] = jnp.where(low_lanes, key, pltpu.roll(value, HEAD, 1)).astype(
                jnp.bfloat16
            )
            kv_out[2 * group + 1, at] = jnp.where(
                low_lanes, pltpu.roll(key, HEAD, 1), value
            ).astype(jnp.bfloat16)
        for copy in kv_sends(chunk):
            copy.start()
        for copy in forwards(kv_out.at[my_head, at], me, my_head, chunk):
            copy.start()
        kv_all[me, at] = kv_out[my_head, at]

        queries, memory_keys = products(1)
        for group in range(groups):
            query = rotated(queries[:, group * 128 : group * 128 + 128], cosine, sine) * factor
            top, bottom = query[:packed], query[packed:]
            q_out[2 * group, packed_of(chunk)] = jnp.where(
                low_lanes, top, pltpu.roll(bottom, HEAD, 1)
            ).astype(jnp.bfloat16)
            q_out[2 * group + 1, packed_of(chunk)] = jnp.where(
                low_lanes, pltpu.roll(top, HEAD, 1), bottom
            ).astype(jnp.bfloat16)
        for copy in q_sends(chunk):
            copy.start()

        @pl.when(my_owner == my_part)
        def _():
            q_all[my_slot, packed_of(chunk)] = q_out[my_head, packed_of(chunk)]

        @pl.when(my_owner != my_part)
        def _():
            q_aside(chunk).start()

        mk_ref[at] = memory_keys.astype(jnp.bfloat16)
        memory_values, memory_queries = products(2)
        mv_ref[at] = memory_values.astype(jnp.bfloat16)
        mq_ref[at] = memory_queries.astype(jnp.bfloat16)
        pre_ref[at, : 2 * heads] = dot(scaled_ref[at, :], gate_weights, ((1,), (1,))) * inverse
        if chunk < chunks - 1:
            forward("chunk", chunk)

    forward("projected")

    gate = pre_ref[:, :heads]
    pre = pre_ref[:, heads : 2 * heads] + bias_ref[...]
    shift = shift_ref[...]
    shift = jnp.concatenate(
        [shift, jnp.zeros((128 - shift.shape[0], rows), jnp.float32)], axis=0
    ).T[:, : shift.shape[0]]
    forget = jnp.minimum(pre, 0.0) - jnp.log1p(jnp.exp(-jnp.abs(pre))) + shift
    row_index = lax.broadcasted_iota(jnp.int32, (rows, rows), 0)
    column_index = lax.broadcasted_iota(jnp.int32, (rows, rows), 1)
    lower = column_index <= row_index
    lower_ones = lower.astype(jnp.bfloat16)
    first, rest = two_parts(forget)
    second = (forget - first.astype(jnp.float32) - rest.astype(jnp.float32)).astype(jnp.bfloat16)
    cumulative = dot(lower_ones, first) + (dot(lower_ones, rest) + dot(lower_ones, second))
    cumulative_ref[:, :heads] = cumulative
    offsets = jnp.concatenate(
        [gate - cumulative, jnp.zeros((rows, 128 - heads), jnp.float32)], axis=1
    )
    offset_ref[...] = offsets.T[:8, :]
    end = cumulative[rows - 1 : rows, :]
    toward = end - cumulative + gate
    top = jnp.max(toward, axis=0, keepdims=True)
    end_weights = spread(jnp.exp(toward - top), width)
    keyed = mk_ref[...].astype(jnp.float32) * (HEAD**-0.5) * end_weights
    high, low = two_parts(keyed)
    whole = dot(high, mv_ref[...], ((0,), (0,))) + dot(low, mv_ref[...], ((0,), (0,)))
    memory = jnp.zeros((HEAD, width), jnp.float32)
    for head in range(heads):
        memory = jnp.where(
            head_mask(width, head), whole[head * HEAD : (head + 1) * HEAD, :], memory
        )
    states_ref[x, :HEAD, :] = memory
    states_ref[x, HEAD : HEAD + 1, :] = jnp.sum(keyed, axis=0, keepdims=True)
    states_ref[x, HEAD + 1 : HEAD + 2, :] = spread(top, width)
    states_ref[x, HEAD + 2 : HEAD + 3, :] = spread(end, width)
    states_ref[x, HEAD + 3 :, :] = jnp.zeros((STATE_ROWS - HEAD - 3, width), jnp.float32)

    def state_sends():
        for step in range(1, across):
            yield remote(
                states_ref.at[x], states_ref.at[x], st_send.at[step], st_recv.at[x], "sp",
                z * across + lax.rem(x + step, across),
            )

    for copy in state_sends():
        copy.start()

    forward("state")
    for group in range(groups):
        lane_group = slice(group * 128, (group + 1) * 128)
        keys = mk_ref[:, lane_group]
        values = mv_ref[:, lane_group]
        group_queries = mq_ref[:, lane_group]
        result = None
        for side in range(2):
            head = group * 2 + side
            chosen = (lanes // HEAD) == side
            column = cumulative[:, head : head + 1]
            gaps = jnp.where(lower, column + offset_ref[head : head + 1, :], NEGATIVE)
            row_top = jnp.max(gaps, axis=1, keepdims=True)
            within = jnp.exp(gaps - row_top)
            scores = dot(jnp.where(chosen, group_queries, 0), keys, ((1,), (1,)))
            scores = jnp.where(lower, within * (scores * (HEAD**-0.5)), 0.0)
            inner_den[:, head : head + 1] = jnp.sum(scores, axis=1, keepdims=True)
            inner_top[:, head : head + 1] = row_top
            score_high, score_low = two_parts(scores)
            numerator = dot(score_high, values) + dot(score_low, values)
            result = numerator if result is None else jnp.where(chosen, numerator, result)
        inner_ref[:, lane_group] = result

    forward("inner")
    def advance(body, stable, later):
        later_top = later[HEAD + 1 : HEAD + 2, :]
        decay = later[HEAD + 2 : HEAD + 3, :]
        new = jnp.maximum(decay + stable, later_top)
        return jnp.exp(decay + stable - new) * body + jnp.exp(later_top - new) * later, new

    def prefix_send():
        return remote(
            prefix_out, prefix_in, px_send, px_recv, "sp", jnp.minimum(me + across, spans - 1)
        )

    def level(body, stable):
        for other in range(across):

            @pl.when(x == other)
            def _():
                enter_ref[...] = body
                enter_ref[HEAD + 1 : HEAD + 2, :] = stable

            if other < across - 1:
                body, stable = advance(body, stable, states_ref[other])
        body, stable = advance(body, stable, states_ref[across - 1])

        @pl.when(z < depth - 1)
        def _():
            prefix_out[...] = body
            prefix_out[HEAD + 1 : HEAD + 2, :] = stable
            prefix_send().start()

    def chain():
        for step in range(1, across):
            other = lax.rem(x + step, across)
            at = states_ref.at[other]
            remote(at, at, st_send.at[step], st_recv.at[other], "sp", me).wait_recv()

        @pl.when(z == 0)
        def _():
            prefix_in[...] = jnp.zeros((STATE_ROWS, width), jnp.float32)

        pl.when(z > 0)(lambda: prefix_send().wait_recv())
        body = prefix_in[...]
        level(body, body[HEAD + 1 : HEAD + 2, :])

    top_ref[...] = jnp.full(top_ref.shape, NEGATIVE, jnp.float32)
    acc_ref[...] = jnp.zeros(acc_ref.shape, jnp.float32)
    units = spans // 2
    half_rows = rows // 2

    def run(steps):
        def score(step):
            slot, wave, place, diagonal = step
            if not diagonal:
                return dot(kv_all[place], qt_ref[slot, wave])
            visible = (wave + 1) * half_rows
            scores = dot(kv_all[place, :visible], qt_ref[slot, wave])
            key_index = lax.broadcasted_iota(jnp.int32, scores.shape, 0)
            query_index = lax.broadcasted_iota(jnp.int32, scores.shape, 1)
            query_index = jnp.where(query_index >= half_rows, query_index - half_rows, query_index)
            return jnp.where(key_index <= query_index + wave * half_rows, scores, NEGATIVE)

        def soften(step, scores):
            slot, wave, place, diagonal = step
            old_top = top_ref[slot, wave]
            top = jnp.maximum(jnp.max(scores, axis=0, keepdims=True), old_top)
            top_ref[slot, wave] = top
            return jnp.exp2(old_top - top), jnp.exp2(scores - top).astype(jnp.bfloat16)

        def gather_up(step, shrink, weights):
            slot, wave, place, diagonal = step
            sums = dot(vt_ref[place, :, : weights.shape[0]], weights)
            acc_ref[slot, wave] = acc_ref[slot, wave] * shrink + sums

        count = len(steps)
        scores = [score(step) for step in steps[:2]]
        held = None
        for index, step in enumerate(steps):
            if index + 2 < count:
                scores.append(score(steps[index + 2]))
            if held is not None:
                gather_up(steps[index - 1], *held)
            held = soften(step, scores[index])
        gather_up(steps[-1], *held)

    def visit_unit(rank):
        return near_first(me // 2, units, rank)

    def arrive(origin):
        @pl.when((origin != me) & (lax.rem(origin, parts) != my_part))
        def _():
            for chunk in range(chunks):
                at = kv_all.at[origin, rows_of(chunk)]
                remote(at, at, kv_send.at[0, chunk], kv_recv.at[origin, chunk], "sp", me).wait_recv()

        turned = kv_all[origin].T
        vt_ref[origin, :HEAD, :] = turned[HEAD:, :]
        vt_ref[origin, HEAD:, :] = jnp.ones((VALUE_ROWS - HEAD, rows), jnp.bfloat16)

        @pl.when(owner_of(origin) == my_part)
        def _():
            slot = origin // parts

            @pl.when(origin != me)
            def _():
                for chunk in range(chunks):
                    at = q_all.at[slot, packed_of(chunk)]
                    remote(
                        at, at, q_send.at[0, chunk], q_recv.at[slot, chunk], "sp", me
                    ).wait_recv()

            for chunk in range(chunks):
                wave = chunk * span // half_rows
                start = chunk * span - wave * half_rows
                low_rows = q_all[slot, packed_of(chunk)].astype(jnp.float32)
                high_rows = pltpu.roll(low_rows, HEAD, 1)
                for half in range(2):
                    chosen = (lanes // DD) == half
                    for side, values in enumerate((low_rows, high_rows)):
                        qn_ref[
                            wave, pl.ds(half * half_rows + start + side * packed, packed)
                        ] = jnp.where(chosen, values, 0.0).astype(jnp.bfloat16)
            for wave in range(2):
                qt_ref[slot, wave] = qn_ref[wave].T

    def mine(unit):
        return [owner_of(2 * unit + side) == my_part for side in range(2)]

    def within(unit, waves):
        chosen = mine(unit)

        @pl.when(chosen[0])
        def _():
            slot = 2 * unit // parts
            run([(slot, wave, 2 * unit, True) for wave in waves])

        @pl.when(chosen[1])
        def _():
            slot = (2 * unit + 1) // parts
            run(
                [(slot, wave, 2 * unit, False) for wave in waves]
                + [(slot, wave, 2 * unit + 1, True) for wave in waves]
            )

    def across_units(unit, other, waves):
        query = jnp.maximum(unit, other)
        key = jnp.minimum(unit, other)

        def both(slot):
            run([(slot, wave, 2 * key + side, False) for side in range(2) for wave in waves])

        if parts == 2:
            both(query)
        else:
            chosen = mine(query)
            for side in range(2):
                pl.when(chosen[side])(functools.partial(both, (2 * query + side) // parts))

    def settle(unit):
        for side in range(2):
            arrive(2 * unit + side)

    def visit(rank, unused):
        unit = visit_unit(rank)
        settle(unit)
        pl.when(rank == 1)(lambda: forward("second"))
        within(unit, (0, 1))

        def earlier(other_rank, unused):
            across_units(unit, visit_unit(other_rank), (0, 1))
            return unused

        lax.fori_loop(0, rank, earlier, 0)
        pl.when(rank == 0)(lambda: forward("first"))
        pl.when(rank == 1)(lambda: forward("seconded"))
        pl.when(rank == z)(chain)
        return unused

    eye = lax.broadcasted_iota(jnp.int32, (HEAD, HEAD), 0) == lax.broadcasted_iota(
        jnp.int32, (HEAD, HEAD), 1
    )
    head_gain = jnp.sum(jnp.where(eye, head_gain_ref[...], 0.0), axis=1, keepdims=True)
    head_lanes = lax.broadcasted_iota(jnp.int32, lambda_ref.shape, 1)
    factor_second = jnp.sum(
        jnp.where(head_lanes == my_head, lambda_ref[...], 0.0), axis=1, keepdims=True
    )

    def span_of(slot):
        return slot * parts + (my_part if slot % 2 == 0 else parts - 1 - my_part)

    def att_place(wave):
        return attended_ref.at[wave, pl.ds(pl.multiple_of(my_head * HEAD, HEAD), HEAD)]

    def att_copy(slot, wave):
        return remote(
            att_out.at[slot, wave], att_place(wave), att_send.at[slot, wave],
            att_recv.at[my_head, wave], "sp", span_of(slot),
        )

    def finish(wave):
        for slot in range(heads):
            sums = acc_ref[slot, wave]
            maps = sums[:HEAD] / sums[HEAD : HEAD + 1]
            second = pltpu.roll(maps, half_rows, 1)[:, :half_rows]
            difference = maps[:, :half_rows] - factor_second * second
            mean = jnp.mean(difference * difference, axis=0, keepdims=True)
            att_out[slot, wave] = (
                difference * lax.rsqrt(mean + EPSILON) * head_gain
            ).astype(jnp.bfloat16)

            @pl.when(span_of(slot) == me)
            def _():
                att_place(wave)[...] = att_out[slot, wave]

            @pl.when(span_of(slot) != me)
            def _():
                att_copy(slot, wave).start()

    lax.fori_loop(0, units - 1, visit, 0)
    last = visit_unit(units - 1)
    settle(last)
    for wave in range(2):
        within(last, (wave,))
        if parts == 2:
            steps = []
            for rank in range(units - 1):
                other = visit_unit(rank)
                query = jnp.maximum(last, other)
                key = jnp.minimum(last, other)
                steps.append([(query, wave, 2 * key + side, False) for side in range(2)])
            run([step for side in zip(*steps) for step in side])
        else:

            def earlier(rank, unused):
                across_units(last, visit_unit(rank), (wave,))
                return unused

            lax.fori_loop(0, units - 1, earlier, 0)
        finish(wave)
    pl.when(z == units - 1)(chain)

    stable = enter_ref[HEAD + 1 : HEAD + 2, :]
    memory_in = enter_ref[:HEAD, :]
    normal_in = enter_ref[HEAD : HEAD + 1, :]
    blocks = jnp.concatenate(
        [jnp.where(head_mask(width, head), memory_in, 0.0) for head in range(heads)], axis=0
    )
    high, low = two_parts(blocks)
    memory_queries = mq_ref[...]
    carried_part = dot(memory_queries, high) + dot(memory_queries, low)
    weighted = memory_queries.astype(jnp.float32) * normal_in
    for group in range(groups):
        lane_group = slice(group * 128, (group + 1) * 128)
        result = None
        for side in range(2):
            head = group * 2 + side
            chosen = (lanes // HEAD) == side
            column = slice(head, head + 1)
            carried_log = cumulative_ref[:, column] + stable[:, head * HEAD : head * HEAD + 1]
            own_top = inner_top[:, column]
            row_top = jnp.maximum(carried_log, own_top)
            inside = jnp.exp(own_top - row_top)
            outside = jnp.exp(carried_log - row_top)
            denominator = inside * inner_den[:, column] + outside * jnp.sum(
                jnp.where(chosen, weighted[:, lane_group], 0.0), axis=1, keepdims=True
            )
            numerator = inside * inner_ref[:, lane_group] + outside * carried_part[:, lane_group]
            quotient = numerator / jnp.maximum(jnp.abs(denominator), 1.0)
            result = quotient if result is None else jnp.where(chosen, quotient, result)
        memory_ref[:, lane_group] = result.astype(jnp.bfloat16)

    loads[6].wait()
    loads[7].wait()
    partial_ref[...] = dot(memory_ref[...], som[...])

    out_span = rows // out_chunks
    per_wave = out_chunks // 2

    def out_rows(chunk):
        return pl.ds(chunk * out_span, out_span)

    order = list(range(1, lines)) + [0]
    swaps = {}
    lined = {}

    def pair_sum(step, chunk):
        swaps[step, chunk].wait_recv()
        mine = part_ref[
            out_rows(chunk), columns_of(lax.rem(line + step, lines) * CORES + core)
        ]
        return mine.astype(jnp.float32) + pair_in[step, out_rows(chunk), :].astype(jnp.float32)

    def pass_on(chunk):
        for step in range(1, lines):
            line_out[step, out_rows(chunk), :] = pair_sum(step, chunk).astype(jnp.bfloat16)
            copy = remote(
                line_out.at[step, out_rows(chunk)], line_in.at[step, out_rows(chunk)],
                sl_send.at[step, chunk], sl_recv.at[step, chunk], "tp",
                lax.rem(line + step, lines) * CORES + core,
            )
            copy.start()
            lined[step, chunk] = copy

    for wave in range(2):
        for step in range(heads):

            @pl.when((my_owner != my_part) | (my_head != step))
            def _():
                at = attended_ref.at[wave, pl.ds(step * HEAD, HEAD)]
                remote(at, at, att_send.at[0, wave], att_recv.at[step, wave], "sp", me).wait_recv()

        at = slice(wave * half_rows, (wave + 1) * half_rows)
        part_ref[at, :] = (
            dot(attended_ref[wave], soa[...], ((0,), (0,))) + partial_ref[at, :]
        ).astype(jnp.bfloat16)
        for chunk in range(wave * per_wave, (wave + 1) * per_wave):
            for step in order:
                target = lax.rem(line + step, lines) * CORES + (1 - core)
                copy = remote(
                    part_ref.at[out_rows(chunk), columns_of(target)],
                    pair_in.at[step, out_rows(chunk)], sp_send.at[step, chunk],
                    sp_recv.at[step, chunk], "tp", pair,
                )
                copy.start()
                swaps[step, chunk] = copy
        for chunk in range(wave * per_wave, (wave + 1) * per_wave):
            pass_on(chunk)

    for copy in sends:
        copy.wait_send()
    for copy in pairs.values():
        copy.wait_send()
    for chunk in range(chunks):
        for copy in kv_sends(chunk):
            copy.wait_send()
        for copy in q_sends(chunk):
            copy.wait_send()
        for index in range(heads):
            for copy in forwards(kv_all.at[0, rows_of(chunk)], 0, index, chunk):
                copy.wait_send()

        @pl.when(my_owner != my_part)
        def _():
            q_aside(chunk).wait_send()

    for copy in state_sends():
        copy.wait_send()
    pl.when(z < depth - 1)(lambda: prefix_send().wait_send())
    for slot in range(heads):

        @pl.when(span_of(slot) != me)
        def _():
            for wave in range(2):
                att_copy(slot, wave).wait_send()

    for chunk in range(out_chunks):
        total = pair_sum(0, chunk)
        for step in range(1, lines):
            lined[step, chunk].wait_recv()
            total = total + line_in[step, out_rows(chunk), :].astype(jnp.float32)
        out_ref[out_rows(chunk), :] = total.astype(jnp.bfloat16)
    for copy in swaps.values():
        copy.wait_send()
    for copy in lined.values():
        copy.wait_send()


def per_device(tp_size, depth, across, inputs, norm_gain, query_weight, key_weight, value_weight,
               memory_query_weight, memory_key_weight, memory_value_weight, input_gate_weight,
               forget_gate_weight, forget_bias, decay_shift, lambdas, head_gain,
               out_weight_attention, out_weight_memory):
    rows, columns = inputs.shape
    features = norm_gain.shape[0]
    width = query_weight.shape[1]
    heads = width // HEAD
    lines = tp_size // CORES
    spans = depth * across
    parts = spans // heads
    chunks = 4
    out_chunks = 4
    dma = pltpu.SemaphoreType.DMA

    middle = DD // 2
    inverse = 1.0 / ROTARY_BASE ** (jnp.arange(middle, dtype=jnp.float32) / middle)
    positions = lax.axis_index("sp") * rows + jnp.arange(rows, dtype=jnp.int32)
    angles = inverse[:, None] * positions.astype(jnp.float32)[None, :]
    cosine = jnp.cos(angles)
    sine = jnp.sin(angles)

    hbm = pl.BlockSpec(memory_space=pl.ANY)
    bf16 = lambda *shape: pltpu.VMEM(shape, jnp.bfloat16)
    f32 = lambda *shape: pltpu.VMEM(shape, jnp.float32)
    return pl.pallas_call(
        functools.partial(layer_kernel, tp_size, depth, across, chunks, out_chunks),
        out_shape=jax.ShapeDtypeStruct((rows, columns), jnp.bfloat16),
        in_specs=[VMEM] * 4 + [hbm] * 6 + [VMEM] * 6 + [hbm] * 2,
        out_specs=VMEM,
        scratch_shapes=[bf16(features, 6 * width)]
        + [bf16(width, features)] * 2
        + [
            bf16(rows, features), bf16(rows, features), f32(rows, 1), f32(rows, 6 * width),
            f32(rows, 128), f32(rows, 128),
            bf16(heads, rows, 128), bf16(heads, rows // 2, 128), bf16(spans, rows, 128),
            bf16(heads, rows // 2, 128), bf16(spans, VALUE_ROWS, rows),
            bf16(2, rows, 128), bf16(heads, 2, 128, rows), f32(heads, 2, 1, rows),
            f32(heads, 2, VALUE_ROWS, rows), bf16(heads, 2, HEAD, rows // 2),
            bf16(2, width, rows // 2),
            bf16(rows, width), bf16(rows, width), bf16(rows, width), f32(rows, 128),
            f32(across, STATE_ROWS, width), f32(STATE_ROWS, width), f32(STATE_ROWS, width),
            f32(STATE_ROWS, width),
            f32(rows, width), f32(rows, 128), f32(rows, 128), f32(rows, 128), f32(8, rows),
            bf16(rows, width),
            f32(rows, features), bf16(rows, features), bf16(lines, rows, columns),
            bf16(lines, rows, columns),
            bf16(lines, rows, columns),
            dma((8,)), dma((lines, chunks)), dma((lines, chunks)), dma((lines, chunks)),
            dma((lines, chunks)),
            dma((heads, chunks)), dma((heads, parts, chunks)), dma((spans, chunks)),
            dma((heads, chunks)), dma((heads, chunks)), dma((heads, 2)), dma((heads, 2)),
            dma((across,)), dma((across,)), dma(()), dma(()),
            dma((lines, out_chunks)), dma((lines, out_chunks)), dma((lines, out_chunks)),
            dma((lines, out_chunks)),
        ],
        compiler_params=pltpu.CompilerParams(
            vmem_limit_bytes=VMEM_LIMIT, collective_id=0, has_side_effects=True
        ),
        name="layer",
    )(
        inputs, norm_gain[None, :], cosine, sine, query_weight, key_weight, value_weight,
        memory_query_weight, memory_key_weight, memory_value_weight, input_gate_weight.T,
        forget_gate_weight.T, forget_bias[None, :], decay_shift.T, lambdas[None, :],
        head_gain[None, :], out_weight_attention, out_weight_memory,
    )


def columns_across(mesh):
    spans = mesh.shape["sp"]
    try:
        places = {device.coords[0] for device in mesh.devices.flat}
        across = len(places)
    except AttributeError:
        across = 2
    return across if spans % across == 0 else 1


def solution(mesh):
    across = columns_across(mesh)
    in_specs = (
        P("sp", "tp"),
        P(),
        P(None, "tp"),
        P(None, "tp"),
        P(None, "tp"),
        P(None, "tp"),
        P(None, "tp"),
        P(None, "tp"),
        P(None, "tp"),
        P(None, "tp"),
        P("tp"),
        P("sp", "tp"),
        P("tp"),
        P(),
        P("tp", None),
        P("tp", None),
    )
    return jax.shard_map(
        functools.partial(
            per_device, mesh.shape["tp"], mesh.shape["sp"] // across, across
        ),
        mesh=mesh,
        in_specs=in_specs,
        out_specs=P("sp", "tp"),
        check_vma=False,
    )
```

```python
import functools

import jax
import jax.numpy as jnp
from jax import lax
from jax.experimental import pallas as pl
from jax.experimental.pallas import tpu as pltpu
from jax.sharding import PartitionSpec as P

HEAD = 64
DD = 32
EPSILON = 1e-06
ROTARY_BASE = 10000.0
NEGATIVE = -1e30
LOG2E = 1.4426950408889634
CORES = 2
STATE_ROWS = HEAD + 8
VALUE_ROWS = HEAD + 16
VMEM = pl.BlockSpec(memory_space=pltpu.VMEM)
MESH = pl.DeviceIdType.MESH
VMEM_LIMIT = 60 * 1024 * 1024


def signal(semaphore, axis, place):
    pl.semaphore_signal(semaphore, inc=1, device_id={axis: place}, device_id_type=MESH)


def remote(source, target, send_sem, recv_sem, axis, place):
    return pltpu.make_async_remote_copy(
        src_ref=source,
        dst_ref=target,
        send_sem=send_sem,
        recv_sem=recv_sem,
        device_id={axis: place},
        device_id_type=MESH,
    )


def head_mask(width, head):
    lanes = lax.broadcasted_iota(jnp.int32, (1, width), 1)
    return (lanes // HEAD) == head


def spread(columns, width):
    spreaded = columns[:, 0:1]
    for head in range(1, columns.shape[1]):
        lanes = lax.broadcasted_iota(jnp.int32, (1, width), 1)
        spreaded = jnp.where(lanes >= head * HEAD, columns[:, head : head + 1], spreaded)
    return jnp.broadcast_to(spreaded, (columns.shape[0], width))


def two_parts(floats):
    high = floats.astype(jnp.bfloat16)
    return high, (floats - high.astype(jnp.float32)).astype(jnp.bfloat16)


def dot(a, b, dims=((1,), (0,))):
    return lax.dot_general(a, b, (dims, ((), ())), preferred_element_type=jnp.float32)


def near_first(place, count, rank):
    both = jnp.minimum(place, count - 1 - place)
    half = (rank + 1) // 2
    low = place < count - 1 - place
    below = jnp.where(low, rank % 2 == 1, rank % 2 == 0)
    alternating = jnp.where(below, place - half, place + half)
    one_sided = jnp.where(low, rank, count - 1 - rank)
    return jnp.where(rank <= 2 * both, alternating, one_sided)


def layer_kernel(
    size, depth, across, chunks, out_chunks,
    shard_ref, gain_ref, rate_ref, wq, wk, wv, wmq, wmk, wmv, wi, wf, bias_ref, shift_ref,
    lambda_ref, head_gain_ref, woa, wom,
    out_ref,
    weight_ref, soa, som, x_ref, scaled_ref, square_ref, sum_ref, cosine_ref, sine_ref,
    kv_out, q_out, kv_all, q_all, vt_ref, qn_ref, qt_ref, top_ref, acc_ref, att_out, attended_ref,
    mq_ref, mk_ref, mv_ref, pre_ref, states_ref, prefix_in, prefix_out, enter_ref,
    inner_ref, inner_den, inner_top, cumulative_ref, offset_ref, memory_ref,
    partial_ref, part_ref, pair_in, line_out, line_in,
    load_sems, line_send, line_recv, pair_send, pair_recv,
    kv_send, fwd_send, kv_recv, q_send, q_recv, att_send, att_recv,
    st_send, st_recv, px_send, px_recv,
    sp_send, sp_recv, sl_send, sl_recv,
):
    rows, columns = shard_ref.shape
    features = x_ref.shape[1]
    width = mq_ref.shape[1]
    heads = width // HEAD
    groups = width // 128
    lines = size // CORES
    spans = depth * across
    parts = spans // heads
    span = rows // chunks
    packed = span // 2

    tp = lax.axis_index("tp")
    core = lax.rem(tp, CORES)
    line = tp // CORES
    pair = line * CORES + (1 - core)
    me = lax.axis_index("sp")
    z = me // across
    x = lax.rem(me, across)
    my_head = me // parts
    my_part = lax.rem(me, parts)

    def owner_of(place):
        place_part = lax.rem(place, parts)
        return jnp.where((place // parts) % 2 == 0, place_part, parts - 1 - place_part)

    loads = []
    for index, source in enumerate((wk, wv, wq, wmk, wmv, wmq)):
        loads.append(
            pltpu.make_async_copy(
                source, weight_ref.at[:, pl.ds(index * width, width)], load_sems.at[index]
            )
        )
    loads.append(pltpu.make_async_copy(woa, soa, load_sems.at[6]))
    loads.append(pltpu.make_async_copy(wom, som, load_sems.at[7]))
    for copy in loads:
        copy.start()

    barrier = pltpu.get_barrier_semaphore()
    signal(barrier, "tp", pair)
    for step in range(1, lines):
        signal(barrier, "tp", lax.rem(line + step, lines) * CORES + core)
    for step in range(1, spans):
        signal(barrier, "sp", lax.rem(me + step, spans))

    position = (me * rows + lax.broadcasted_iota(jnp.int32, (1, rows), 1)).astype(jnp.float32)
    angles = rate_ref[...] * position
    cosines = jnp.cos(angles)
    sines = jnp.sin(angles)
    cosine_ref[...] = jnp.concatenate([cosines] * (128 * 2 // DD), axis=0).T
    sine_ref[...] = jnp.concatenate([-sines, sines] * (128 // DD), axis=0).T
    lanes = lax.broadcasted_iota(jnp.int32, (1, 128), 1)
    former = lax.rem(lanes, DD) < DD // 2
    low_lanes = lanes < HEAD

    def columns_of(owner):
        return pl.ds(pl.multiple_of(owner * columns, 128), columns)

    def rows_of(chunk):
        return pl.ds(chunk * span, span)

    def place(owner, chunk):
        return x_ref.at[rows_of(chunk), columns_of(owner)]

    pl.semaphore_wait(barrier, lines + spans - 1)

    sends = []
    pairs = {}
    for chunk in range(chunks):
        for step in range(1, lines):
            copy = remote(
                shard_ref.at[rows_of(chunk)], place(tp, chunk), line_send.at[step, chunk],
                line_recv.at[step, chunk], "tp", lax.rem(line + step, lines) * CORES + core,
            )
            copy.start()
            sends.append(copy)
    for chunk in range(chunks):
        copy = remote(
            shard_ref.at[rows_of(chunk)], place(tp, chunk), pair_send.at[0, chunk],
            pair_recv.at[0, chunk], "tp", pair,
        )
        copy.start()
        pairs[0, chunk] = copy

    def take(values, at_rows, owner):
        floats = values.astype(jnp.float32)
        scaled_ref[at_rows, columns_of(owner)] = (floats * gain_ref[:, columns_of(owner)]).astype(
            jnp.bfloat16
        )
        return jnp.sum(floats * floats, axis=1, keepdims=True)

    everywhere = pl.ds(0, rows)
    squares = take(shard_ref[...], everywhere, tp)
    for chunk in range(chunks):
        pairs[0, chunk].wait_recv()
    square_ref[...] = squares + take(x_ref[:, columns_of(pair)], everywhere, pair)

    def line_columns(owner_line):
        return pl.ds(pl.multiple_of(owner_line * CORES * columns, 128), CORES * columns)

    couples = [slice(index * width, (index + 2) * width) for index in (0, 2, 4)]
    for index, couple in enumerate(couples):
        loads[2 * index].wait()
        loads[2 * index + 1].wait()
        sum_ref[:, couple] = dot(
            scaled_ref[:, line_columns(line)], weight_ref[line_columns(line), couple]
        )

    gate_weights = jnp.concatenate([wi[...], wf[...]], axis=0)
    factor = (DD**-0.5) * LOG2E

    def rotated(wide, cosine, sine):
        partner = jnp.where(former, pltpu.roll(wide, 128 - DD // 2, 1), pltpu.roll(wide, DD // 2, 1))
        return wide * cosine + partner * sine

    def kv_sends(chunk):
        for rank in range(1, heads):
            head = near_first(my_head, heads, rank)
            yield remote(
                kv_out.at[head, rows_of(chunk)], kv_all.at[me, rows_of(chunk)],
                kv_send.at[rank, chunk], kv_recv.at[me, chunk], "sp", head * parts + my_part,
            )

    def forwards(source, origin, index, chunk):
        for step in range(1, parts):
            yield remote(
                source, kv_all.at[origin, rows_of(chunk)], fwd_send.at[index, step, chunk],
                kv_recv.at[origin, chunk], "sp",
                my_head * parts + lax.rem(my_part + step, parts),
            )

    points = {
        (1, 0): "chunk1", (1, 1): "chunk2", (1, 2): "projected", (2, 0): "projected",
        (1, 3): "state", (3, 0): "state", (2, 1): "first", (3, 1): "first",
        (2, 2): "inner", (3, 2): "second", (2, 3): "second", (3, 3): "seconded",
    }

    def landed(rank):
        return near_first(my_head, heads, rank) * parts + my_part

    def forward(point, index=""):
        for chunk in range(chunks):
            for rank in range(1, heads):
                if points.get((rank, chunk), "inner") == f"{point}{index}":
                    origin = landed(rank)
                    at = kv_all.at[origin, rows_of(chunk)]
                    remote(
                        at, at, kv_send.at[0, chunk], kv_recv.at[origin, chunk], "sp", me
                    ).wait_recv()
                    for copy in forwards(at, origin, origin // parts, chunk):
                        copy.start()

    packed_of = lambda chunk: pl.ds(chunk * packed, packed)
    my_slot = me // parts
    my_owner = owner_of(me)

    def q_sends(chunk):
        for rank in range(1, heads):
            head = near_first(my_head, heads, rank)
            yield remote(
                q_out.at[head, packed_of(chunk)], q_all.at[my_slot, packed_of(chunk)],
                q_send.at[rank, chunk], q_recv.at[my_slot, chunk], "sp", head * parts + my_owner,
            )

    def q_aside(chunk):
        return remote(
            q_out.at[my_head, packed_of(chunk)], q_all.at[my_slot, packed_of(chunk)],
            q_send.at[0, chunk], q_recv.at[my_slot, chunk], "sp", my_head * parts + my_owner,
        )

    def pull(chunk):
        for step in range(1, lines):
            source = lax.rem(line + lines - step, lines) * CORES + core
            at = place(source, chunk)
            remote(
                at, at, line_send.at[step, chunk], line_recv.at[step, chunk], "tp", pair
            ).wait_recv()
            copy = remote(
                at, at, pair_send.at[step, chunk], pair_recv.at[step, chunk], "tp", pair
            )
            copy.start()
            pairs[step, chunk] = copy

    pull(0)
    for chunk in range(chunks):
        at = rows_of(chunk)
        squares = square_ref[at]
        for step in range(1, lines):
            source = lax.rem(line + lines - step, lines) * CORES + core
            squares = squares + take(x_ref[at, columns_of(source)], at, source)
        for step in range(1, lines):
            source = lax.rem(line + lines - step, lines) * CORES + 1 - core
            pairs[step, chunk].wait_recv()
            squares = squares + take(x_ref[at, columns_of(source)], at, source)
        inverse = lax.rsqrt(squares / features + EPSILON)

        def products(index):
            total = sum_ref[at, couples[index]]
            for step in range(1, lines):
                other = line_columns(lax.rem(line + step, lines))
                total = total + dot(scaled_ref[at, other], weight_ref[other, couples[index]])
            total = (total * inverse).astype(jnp.bfloat16).astype(jnp.float32)
            return total[:, :width], total[:, width:]

        cosine = cosine_ref[at]
        sine = sine_ref[at]
        keys, values = products(0)
        for group in range(groups):
            lane_group = slice(group * 128, group * 128 + 128)
            key = rotated(keys[:, lane_group], cosine, sine)
            value = values[:, lane_group]
            kv_out[2 * group, at] = jnp.where(low_lanes, key, pltpu.roll(value, HEAD, 1)).astype(
                jnp.bfloat16
            )
            kv_out[2 * group + 1, at] = jnp.where(
                low_lanes, pltpu.roll(key, HEAD, 1), value
            ).astype(jnp.bfloat16)
        for copy in kv_sends(chunk):
            copy.start()
        for copy in forwards(kv_out.at[my_head, at], me, my_head, chunk):
            copy.start()
        kv_all[me, at] = kv_out[my_head, at]

        queries, memory_keys = products(1)
        for group in range(groups):
            query = rotated(queries[:, group * 128 : group * 128 + 128], cosine, sine) * factor
            top, bottom = query[:packed], query[packed:]
            q_out[2 * group, packed_of(chunk)] = jnp.where(
                low_lanes, top, pltpu.roll(bottom, HEAD, 1)
            ).astype(jnp.bfloat16)
            q_out[2 * group + 1, packed_of(chunk)] = jnp.where(
                low_lanes, pltpu.roll(top, HEAD, 1), bottom
            ).astype(jnp.bfloat16)
        for copy in q_sends(chunk):
            copy.start()

        @pl.when(my_owner == my_part)
        def _():
            q_all[my_slot, packed_of(chunk)] = q_out[my_head, packed_of(chunk)]

        @pl.when(my_owner != my_part)
        def _():
            q_aside(chunk).start()

        mk_ref[at] = memory_keys.astype(jnp.bfloat16)
        if chunk + 1 < chunks:
            pull(chunk + 1)
        memory_values, memory_queries = products(2)
        mv_ref[at] = memory_values.astype(jnp.bfloat16)
        mq_ref[at] = memory_queries.astype(jnp.bfloat16)
        pre_ref[at, : 2 * heads] = dot(scaled_ref[at, :], gate_weights, ((1,), (1,))) * inverse
        if chunk < chunks - 1:
            forward("chunk", chunk)

    forward("projected")

    gate = pre_ref[:, :heads]
    pre = pre_ref[:, heads : 2 * heads] + bias_ref[...]
    shift = shift_ref[...]
    shift = jnp.concatenate(
        [shift, jnp.zeros((128 - shift.shape[0], rows), jnp.float32)], axis=0
    ).T[:, : shift.shape[0]]
    forget = jnp.minimum(pre, 0.0) - jnp.log1p(jnp.exp(-jnp.abs(pre))) + shift
    row_index = lax.broadcasted_iota(jnp.int32, (rows, rows), 0)
    column_index = lax.broadcasted_iota(jnp.int32, (rows, rows), 1)
    lower = column_index <= row_index
    lower_ones = lower.astype(jnp.bfloat16)
    first, rest = two_parts(forget)
    second = (forget - first.astype(jnp.float32) - rest.astype(jnp.float32)).astype(jnp.bfloat16)
    sums = dot(lower_ones, jnp.concatenate([first, rest, second], axis=1))
    cumulative = sums[:, :heads] + (sums[:, heads : 2 * heads] + sums[:, 2 * heads :])
    cumulative_ref[:, :heads] = cumulative
    offsets = jnp.concatenate(
        [gate - cumulative, jnp.zeros((rows, 128 - heads), jnp.float32)], axis=1
    )
    offset_ref[...] = offsets.T[:8, :]
    end = cumulative[rows - 1 : rows, :]
    toward = end - cumulative + gate
    top = jnp.max(toward, axis=0, keepdims=True)
    end_weights = spread(jnp.exp(toward - top), width)
    keyed = mk_ref[...].astype(jnp.float32) * (HEAD**-0.5) * end_weights
    high, low = two_parts(keyed)
    whole = dot(high, mv_ref[...], ((0,), (0,))) + dot(low, mv_ref[...], ((0,), (0,)))
    memory = jnp.zeros((HEAD, width), jnp.float32)
    for head in range(heads):
        memory = jnp.where(
            head_mask(width, head), whole[head * HEAD : (head + 1) * HEAD, :], memory
        )
    states_ref[x, :HEAD, :] = memory
    states_ref[x, HEAD : HEAD + 1, :] = jnp.sum(keyed, axis=0, keepdims=True)
    states_ref[x, HEAD + 1 : HEAD + 2, :] = spread(top, width)
    states_ref[x, HEAD + 2 : HEAD + 3, :] = spread(end, width)
    states_ref[x, HEAD + 3 :, :] = jnp.zeros((STATE_ROWS - HEAD - 3, width), jnp.float32)

    def state_sends():
        for step in range(1, across):
            yield remote(
                states_ref.at[x], states_ref.at[x], st_send.at[step], st_recv.at[x], "sp",
                z * across + lax.rem(x + step, across),
            )

    forward("state")
    for copy in state_sends():
        copy.start()

    def inner():
        step_rows = 128
        for group in range(groups):
            lane_group = slice(group * 128, (group + 1) * 128)
            for start in range(0, rows, step_rows):
                stop = start + step_rows
                block_rows = slice(start, stop)
                keys = mk_ref[:stop, lane_group]
                values = mv_ref[:stop, lane_group]
                group_queries = mq_ref[block_rows, lane_group]
                row_index = lax.broadcasted_iota(jnp.int32, (step_rows, stop), 0)
                column_index = lax.broadcasted_iota(jnp.int32, (step_rows, stop), 1)
                lower = column_index <= row_index + start
                result = None
                for side in range(2):
                    head = group * 2 + side
                    chosen = (lanes // HEAD) == side
                    column = cumulative_ref[block_rows, head : head + 1]
                    gaps = jnp.where(lower, column + offset_ref[head : head + 1, :stop], NEGATIVE)
                    row_top = jnp.max(gaps, axis=1, keepdims=True)
                    within = jnp.exp(gaps - row_top)
                    scores = dot(jnp.where(chosen, group_queries, 0), keys, ((1,), (1,)))
                    scores = jnp.where(lower, within * (scores * (HEAD**-0.5)), 0.0)
                    inner_den[block_rows, head : head + 1] = jnp.sum(scores, axis=1, keepdims=True)
                    inner_top[block_rows, head : head + 1] = row_top
                    score_high, score_low = two_parts(scores)
                    numerator = dot(score_high, values) + dot(score_low, values)
                    result = numerator if result is None else jnp.where(chosen, numerator, result)
                inner_ref[block_rows, lane_group] = result

    def advance(body, stable, later):
        later_top = later[HEAD + 1 : HEAD + 2, :]
        decay = later[HEAD + 2 : HEAD + 3, :]
        new = jnp.maximum(decay + stable, later_top)
        return jnp.exp(decay + stable - new) * body + jnp.exp(later_top - new) * later, new

    def prefix_send():
        return remote(
            prefix_out, prefix_in, px_send, px_recv, "sp", jnp.minimum(me + across, spans - 1)
        )

    def level(body, stable):
        for other in range(across):

            @pl.when(x == other)
            def _():
                enter_ref[...] = body
                enter_ref[HEAD + 1 : HEAD + 2, :] = stable

            if other < across - 1:
                body, stable = advance(body, stable, states_ref[other])
        body, stable = advance(body, stable, states_ref[across - 1])

        @pl.when(z < depth - 1)
        def _():
            prefix_out[...] = body
            prefix_out[HEAD + 1 : HEAD + 2, :] = stable
            prefix_send().start()

    def chain():
        for step in range(1, across):
            other = lax.rem(x + step, across)
            at = states_ref.at[other]
            remote(at, at, st_send.at[step], st_recv.at[other], "sp", me).wait_recv()

        @pl.when(z == 0)
        def _():
            prefix_in[...] = jnp.zeros((STATE_ROWS, width), jnp.float32)

        pl.when(z > 0)(lambda: prefix_send().wait_recv())
        body = prefix_in[...]
        level(body, body[HEAD + 1 : HEAD + 2, :])

    top_ref[...] = jnp.full(top_ref.shape, NEGATIVE, jnp.float32)
    acc_ref[...] = jnp.zeros(acc_ref.shape, jnp.float32)
    units = spans // 2
    half_rows = rows // 2

    def run(steps):
        def score(step):
            slot, wave, place, diagonal = step
            if not diagonal:
                return dot(kv_all[place], qt_ref[slot, wave])
            visible = (wave + 1) * half_rows
            scores = dot(kv_all[place, :visible], qt_ref[slot, wave])
            key_index = lax.broadcasted_iota(jnp.int32, scores.shape, 0)
            query_index = lax.broadcasted_iota(jnp.int32, scores.shape, 1)
            query_index = jnp.where(query_index >= half_rows, query_index - half_rows, query_index)
            return jnp.where(key_index <= query_index + wave * half_rows, scores, NEGATIVE)

        def soften(step, scores):
            slot, wave, place, diagonal = step
            old_top = top_ref[slot, wave]
            top = jnp.maximum(jnp.max(scores, axis=0, keepdims=True), old_top)
            top_ref[slot, wave] = top
            return jnp.exp2(old_top - top), jnp.exp2(scores - top).astype(jnp.bfloat16)

        def gather_up(step, shrink, weights):
            slot, wave, place, diagonal = step
            sums = dot(vt_ref[place, :, : weights.shape[0]], weights)
            acc_ref[slot, wave] = acc_ref[slot, wave] * shrink + sums

        count = len(steps)
        scores = [score(step) for step in steps[:2]]
        held = None
        for index, step in enumerate(steps):
            if index + 2 < count:
                scores.append(score(steps[index + 2]))
            if held is not None:
                gather_up(steps[index - 1], *held)
            held = soften(step, scores[index])
        gather_up(steps[-1], *held)

    def visit_unit(rank):
        return near_first(me // 2, units, rank)

    def arrive(origin):
        @pl.when((origin != me) & (lax.rem(origin, parts) != my_part))
        def _():
            for chunk in range(chunks):
                at = kv_all.at[origin, rows_of(chunk)]
                remote(at, at, kv_send.at[0, chunk], kv_recv.at[origin, chunk], "sp", me).wait_recv()

        turned = kv_all[origin].T
        vt_ref[origin, :HEAD, :] = turned[HEAD:, :]
        vt_ref[origin, HEAD:, :] = jnp.ones((VALUE_ROWS - HEAD, rows), jnp.bfloat16)

        @pl.when(owner_of(origin) == my_part)
        def _():
            slot = origin // parts

            @pl.when(origin != me)
            def _():
                for chunk in range(chunks):
                    at = q_all.at[slot, packed_of(chunk)]
                    remote(
                        at, at, q_send.at[0, chunk], q_recv.at[slot, chunk], "sp", me
                    ).wait_recv()

            for chunk in range(chunks):
                wave = chunk * span // half_rows
                start = chunk * span - wave * half_rows
                low_rows = q_all[slot, packed_of(chunk)].astype(jnp.float32)
                high_rows = pltpu.roll(low_rows, HEAD, 1)
                for half in range(2):
                    chosen = (lanes // DD) == half
                    for side, values in enumerate((low_rows, high_rows)):
                        qn_ref[
                            wave, pl.ds(half * half_rows + start + side * packed, packed)
                        ] = jnp.where(chosen, values, 0.0).astype(jnp.bfloat16)
            for wave in range(2):
                qt_ref[slot, wave] = qn_ref[wave].T

    def mine(unit):
        return [owner_of(2 * unit + side) == my_part for side in range(2)]

    def within(unit, waves):
        chosen = mine(unit)

        @pl.when(chosen[0])
        def _():
            slot = 2 * unit // parts
            run([(slot, wave, 2 * unit, True) for wave in waves])

        @pl.when(chosen[1])
        def _():
            slot = (2 * unit + 1) // parts
            run(
                [(slot, wave, 2 * unit, False) for wave in waves]
                + [(slot, wave, 2 * unit + 1, True) for wave in waves]
            )

    def across_units(unit, other, waves):
        query = jnp.maximum(unit, other)
        key = jnp.minimum(unit, other)

        def both(slot):
            run([(slot, wave, 2 * key + side, False) for side in range(2) for wave in waves])

        if parts == 2:
            both(query)
        else:
            chosen = mine(query)
            for side in range(2):
                pl.when(chosen[side])(functools.partial(both, (2 * query + side) // parts))

    def settle(unit):
        for side in range(2):
            arrive(2 * unit + side)

    def visit(rank, unused):
        unit = visit_unit(rank)
        settle(unit)
        pl.when(rank == 1)(lambda: forward("second"))
        pl.when((z > 0) & (rank == z + 1))(chain)
        within(unit, (0, 1))

        def earlier(other_rank, unused):
            across_units(unit, visit_unit(other_rank), (0, 1))
            return unused

        lax.fori_loop(0, rank, earlier, 0)
        pl.when(rank == 1)(lambda: forward("seconded"))
        return unused

    eye = lax.broadcasted_iota(jnp.int32, (HEAD, HEAD), 0) == lax.broadcasted_iota(
        jnp.int32, (HEAD, HEAD), 1
    )
    head_gain = jnp.sum(jnp.where(eye, head_gain_ref[...], 0.0), axis=1, keepdims=True)
    head_lanes = lax.broadcasted_iota(jnp.int32, lambda_ref.shape, 1)
    factor_second = jnp.sum(
        jnp.where(head_lanes == my_head, lambda_ref[...], 0.0), axis=1, keepdims=True
    )

    def span_of(slot):
        return slot * parts + (my_part if slot % 2 == 0 else parts - 1 - my_part)

    def att_place(wave):
        return attended_ref.at[wave, pl.ds(pl.multiple_of(my_head * HEAD, HEAD), HEAD)]

    def att_copy(slot, wave):
        return remote(
            att_out.at[slot, wave], att_place(wave), att_send.at[slot, wave],
            att_recv.at[my_head, wave], "sp", span_of(slot),
        )

    def finish(wave):
        for slot in range(heads):
            sums = acc_ref[slot, wave]
            maps = sums[:HEAD] / sums[HEAD : HEAD + 1]
            second = pltpu.roll(maps, half_rows, 1)[:, :half_rows]
            difference = maps[:, :half_rows] - factor_second * second
            mean = jnp.mean(difference * difference, axis=0, keepdims=True)
            att_out[slot, wave] = (
                difference * lax.rsqrt(mean + EPSILON) * head_gain
            ).astype(jnp.bfloat16)

            @pl.when(span_of(slot) == me)
            def _():
                att_place(wave)[...] = att_out[slot, wave]

            @pl.when(span_of(slot) != me)
            def _():
                att_copy(slot, wave).start()

    def recall():
        stable = enter_ref[HEAD + 1 : HEAD + 2, :]
        memory_in = enter_ref[:HEAD, :]
        normal_in = enter_ref[HEAD : HEAD + 1, :]
        blocks = jnp.concatenate(
            [jnp.where(head_mask(width, head), memory_in, 0.0) for head in range(heads)], axis=0
        )
        high, low = two_parts(blocks)
        memory_queries = mq_ref[...]
        carried_part = dot(memory_queries, high) + dot(memory_queries, low)
        weighted = memory_queries.astype(jnp.float32) * normal_in
        for group in range(groups):
            lane_group = slice(group * 128, (group + 1) * 128)
            result = None
            for side in range(2):
                head = group * 2 + side
                chosen = (lanes // HEAD) == side
                column = slice(head, head + 1)
                carried_log = cumulative_ref[:, column] + stable[:, head * HEAD : head * HEAD + 1]
                own_top = inner_top[:, column]
                row_top = jnp.maximum(carried_log, own_top)
                inside = jnp.exp(own_top - row_top)
                outside = jnp.exp(carried_log - row_top)
                denominator = inside * inner_den[:, column] + outside * jnp.sum(
                    jnp.where(chosen, weighted[:, lane_group], 0.0), axis=1, keepdims=True
                )
                numerator = inside * inner_ref[:, lane_group] + outside * carried_part[:, lane_group]
                quotient = numerator / jnp.maximum(jnp.abs(denominator), 1.0)
                result = quotient if result is None else jnp.where(chosen, quotient, result)
            memory_ref[:, lane_group] = result.astype(jnp.bfloat16)

        loads[6].wait()
        loads[7].wait()
        partial_ref[...] = dot(memory_ref[...], som[...])

    settle(me // 2)
    within(me // 2, (0, 1))
    forward("first")
    inner()
    forward("inner")
    pl.when(z == 0)(chain)
    lax.fori_loop(1, units - 1, visit, 0)
    last = visit_unit(units - 1)
    settle(last)
    pl.when(z == units - 2)(chain)
    for wave in range(2):
        within(last, (wave,))
        if parts == 2:
            steps = []
            for rank in range(units - 1):
                other = visit_unit(rank)
                query = jnp.maximum(last, other)
                key = jnp.minimum(last, other)
                steps.append([(query, wave, 2 * key + side, False) for side in range(2)])
            run([step for side in zip(*steps) for step in side])
        else:

            def earlier(rank, unused):
                across_units(last, visit_unit(rank), (wave,))
                return unused

            lax.fori_loop(0, units - 1, earlier, 0)
        finish(wave)
        if wave == 0:
            pl.when(z < units - 1)(recall)
    @pl.when(z >= units - 1)
    def _():
        chain()
        recall()

    out_span = rows // out_chunks
    per_wave = out_chunks // 2

    def out_rows(chunk):
        return pl.ds(chunk * out_span, out_span)

    order = list(range(1, lines)) + [0]
    swaps = {}
    lined = {}

    def pair_sum(step, chunk):
        swaps[step, chunk].wait_recv()
        mine = part_ref[
            out_rows(chunk), columns_of(lax.rem(line + step, lines) * CORES + core)
        ]
        return mine.astype(jnp.float32) + pair_in[step, out_rows(chunk), :].astype(jnp.float32)

    def pass_on(chunk):
        for step in range(1, lines):
            line_out[step, out_rows(chunk), :] = pair_sum(step, chunk).astype(jnp.bfloat16)
            copy = remote(
                line_out.at[step, out_rows(chunk)], line_in.at[step, out_rows(chunk)],
                sl_send.at[step, chunk], sl_recv.at[step, chunk], "tp",
                lax.rem(line + step, lines) * CORES + core,
            )
            copy.start()
            lined[step, chunk] = copy

    for wave in range(2):
        for step in range(heads):

            @pl.when((my_owner != my_part) | (my_head != step))
            def _():
                at = attended_ref.at[wave, pl.ds(step * HEAD, HEAD)]
                remote(at, at, att_send.at[0, wave], att_recv.at[step, wave], "sp", me).wait_recv()

        at = slice(wave * half_rows, (wave + 1) * half_rows)
        part_ref[at, :] = (
            dot(attended_ref[wave], soa[...], ((0,), (0,))) + partial_ref[at, :]
        ).astype(jnp.bfloat16)
        for chunk in range(wave * per_wave, (wave + 1) * per_wave):
            for step in order:
                target = lax.rem(line + step, lines) * CORES + (1 - core)
                copy = remote(
                    part_ref.at[out_rows(chunk), columns_of(target)],
                    pair_in.at[step, out_rows(chunk)], sp_send.at[step, chunk],
                    sp_recv.at[step, chunk], "tp", pair,
                )
                copy.start()
                swaps[step, chunk] = copy
        for chunk in range(wave * per_wave, (wave + 1) * per_wave):
            pass_on(chunk)

    for copy in sends:
        copy.wait_send()
    for copy in pairs.values():
        copy.wait_send()
    for chunk in range(chunks):
        for copy in kv_sends(chunk):
            copy.wait_send()
        for copy in q_sends(chunk):
            copy.wait_send()
        for index in range(heads):
            for copy in forwards(kv_all.at[0, rows_of(chunk)], 0, index, chunk):
                copy.wait_send()

        @pl.when(my_owner != my_part)
        def _():
            q_aside(chunk).wait_send()

    for copy in state_sends():
        copy.wait_send()
    pl.when(z < depth - 1)(lambda: prefix_send().wait_send())
    for slot in range(heads):

        @pl.when(span_of(slot) != me)
        def _():
            for wave in range(2):
                att_copy(slot, wave).wait_send()

    for chunk in range(out_chunks):
        total = pair_sum(0, chunk)
        for step in range(1, lines):
            lined[step, chunk].wait_recv()
            total = total + line_in[step, out_rows(chunk), :].astype(jnp.float32)
        out_ref[out_rows(chunk), :] = total.astype(jnp.bfloat16)
    for copy in swaps.values():
        copy.wait_send()
    for copy in lined.values():
        copy.wait_send()


def per_device(tp_size, depth, across, inputs, norm_gain, query_weight, key_weight, value_weight,
               memory_query_weight, memory_key_weight, memory_value_weight, input_gate_weight,
               forget_gate_weight, forget_bias, decay_shift, lambdas, head_gain,
               out_weight_attention, out_weight_memory):
    rows, columns = inputs.shape
    features = norm_gain.shape[0]
    width = query_weight.shape[1]
    heads = width // HEAD
    lines = tp_size // CORES
    spans = depth * across
    parts = spans // heads
    chunks = 4
    out_chunks = 4
    dma = pltpu.SemaphoreType.DMA

    middle = DD // 2
    inverse = 1.0 / ROTARY_BASE ** (jnp.arange(middle, dtype=jnp.float32) / middle)

    hbm = pl.BlockSpec(memory_space=pl.ANY)
    bf16 = lambda *shape: pltpu.VMEM(shape, jnp.bfloat16)
    f32 = lambda *shape: pltpu.VMEM(shape, jnp.float32)
    return pl.pallas_call(
        functools.partial(layer_kernel, tp_size, depth, across, chunks, out_chunks),
        out_shape=jax.ShapeDtypeStruct((rows, columns), jnp.bfloat16),
        in_specs=[VMEM] * 3 + [hbm] * 6 + [VMEM] * 6 + [hbm] * 2,
        out_specs=VMEM,
        scratch_shapes=[bf16(features, 6 * width)]
        + [bf16(width, features)] * 2
        + [
            bf16(rows, features), bf16(rows, features), f32(rows, 1), f32(rows, 6 * width),
            f32(rows, 128), f32(rows, 128),
            bf16(heads, rows, 128), bf16(heads, rows // 2, 128), bf16(spans, rows, 128),
            bf16(heads, rows // 2, 128), bf16(spans, VALUE_ROWS, rows),
            bf16(2, rows, 128), bf16(heads, 2, 128, rows), f32(heads, 2, 1, rows),
            f32(heads, 2, VALUE_ROWS, rows), bf16(heads, 2, HEAD, rows // 2),
            bf16(2, width, rows // 2),
            bf16(rows, width), bf16(rows, width), bf16(rows, width), f32(rows, 128),
            f32(across, STATE_ROWS, width), f32(STATE_ROWS, width), f32(STATE_ROWS, width),
            f32(STATE_ROWS, width),
            f32(rows, width), f32(rows, 128), f32(rows, 128), f32(rows, 128), f32(8, rows),
            bf16(rows, width),
            f32(rows, features), bf16(rows, features), bf16(lines, rows, columns),
            bf16(lines, rows, columns),
            bf16(lines, rows, columns),
            dma((8,)), dma((lines, chunks)), dma((lines, chunks)), dma((lines, chunks)),
            dma((lines, chunks)),
            dma((heads, chunks)), dma((heads, parts, chunks)), dma((spans, chunks)),
            dma((heads, chunks)), dma((heads, chunks)), dma((heads, 2)), dma((heads, 2)),
            dma((across,)), dma((across,)), dma(()), dma(()),
            dma((lines, out_chunks)), dma((lines, out_chunks)), dma((lines, out_chunks)),
            dma((lines, out_chunks)),
        ],
        compiler_params=pltpu.CompilerParams(
            vmem_limit_bytes=VMEM_LIMIT, collective_id=0, has_side_effects=True
        ),
        name="layer",
    )(
        inputs, norm_gain[None, :], inverse[:, None], query_weight, key_weight, value_weight,
        memory_query_weight, memory_key_weight, memory_value_weight, input_gate_weight.T,
        forget_gate_weight.T, forget_bias[None, :], decay_shift.T, lambdas[None, :],
        head_gain[None, :], out_weight_attention, out_weight_memory,
    )


def columns_across(mesh):
    spans = mesh.shape["sp"]
    try:
        places = {device.coords[0] for device in mesh.devices.flat}
        across = len(places)
    except AttributeError:
        across = 2
    return across if spans % across == 0 else 1


def solution(mesh):
    across = columns_across(mesh)
    in_specs = (
        P("sp", "tp"),
        P(),
        P(None, "tp"),
        P(None, "tp"),
        P(None, "tp"),
        P(None, "tp"),
        P(None, "tp"),
        P(None, "tp"),
        P(None, "tp"),
        P(None, "tp"),
        P("tp"),
        P("sp", "tp"),
        P("tp"),
        P(),
        P("tp", None),
        P("tp", None),
    )
    return jax.shard_map(
        functools.partial(
            per_device, mesh.shape["tp"], mesh.shape["sp"] // across, across
        ),
        mesh=mesh,
        in_specs=in_specs,
        out_specs=P("sp", "tp"),
        check_vma=False,
    )
```

```python
import functools

import jax
import jax.numpy as jnp
from jax import lax
from jax.experimental import pallas as pl
from jax.experimental.pallas import tpu as pltpu
from jax.sharding import PartitionSpec as P

HEAD = 64
DD = 32
EPSILON = 1e-06
ROTARY_BASE = 10000.0
NEGATIVE = -1e30
LOG2E = 1.4426950408889634
CORES = 2
STATE_ROWS = HEAD + 8
VALUE_ROWS = HEAD + 16
VMEM = pl.BlockSpec(memory_space=pltpu.VMEM)
MESH = pl.DeviceIdType.MESH
VMEM_LIMIT = 60 * 1024 * 1024


def signal(semaphore, axis, place):
    pl.semaphore_signal(semaphore, inc=1, device_id={axis: place}, device_id_type=MESH)


def remote(source, target, send_sem, recv_sem, axis, place):
    return pltpu.make_async_remote_copy(
        src_ref=source,
        dst_ref=target,
        send_sem=send_sem,
        recv_sem=recv_sem,
        device_id={axis: place},
        device_id_type=MESH,
    )


def head_mask(width, head):
    lanes = lax.broadcasted_iota(jnp.int32, (1, width), 1)
    return (lanes // HEAD) == head


def two_parts(floats):
    high = floats.astype(jnp.bfloat16)
    return high, (floats - high.astype(jnp.float32)).astype(jnp.bfloat16)


def dot(a, b, dims=((1,), (0,))):
    return lax.dot_general(a, b, (dims, ((), ())), preferred_element_type=jnp.float32)


def near_first(place, count, rank):
    both = jnp.minimum(place, count - 1 - place)
    half = (rank + 1) // 2
    low = place < count - 1 - place
    below = jnp.where(low, rank % 2 == 1, rank % 2 == 0)
    alternating = jnp.where(below, place - half, place + half)
    one_sided = jnp.where(low, rank, count - 1 - rank)
    return jnp.where(rank <= 2 * both, alternating, one_sided)


def layer_kernel(
    size, depth, across, chunks, out_chunks,
    shard_ref, gain_ref, wq, wk, wv, wmq, wmk, wmv, wi, wf, bias_ref, shift_ref,
    lambda_ref, head_gain_ref, woa, wom,
    out_ref,
    weight_ref, soa, som, x_ref, scaled_ref, square_ref, sum_ref, cosine_ref, sine_ref,
    kv_out, q_out, kv_all, q_all, vt_ref, qn_ref, qt_ref, top_ref, acc_ref, att_out, attended_ref,
    mq_ref, mk_ref, mv_ref, mq_turned, mv_turned, pre_ref, states_ref, prefix_in, prefix_out, enter_ref,
    inner_ref, inner_den, inner_top, cumulative_ref, offset_ref, memory_ref,
    partial_ref, part_ref, pair_in, line_out, line_in, total_ref,
    out_sem, load_sems, line_send, line_recv, pair_send, pair_recv, own_recv,
    kv_send, fwd_send, land_recv, cross_recv, q_send, q_side, q_recv, att_send, att_recv,
    st_send, st_recv, px_send, px_recv, sp_send, sp_recv, sl_send, sl_recv,
):
    rows, columns = shard_ref.shape
    features = x_ref.shape[1]
    width = mq_ref.shape[1]
    heads = width // HEAD
    groups = width // 128
    lines = size // CORES
    spans = depth * across
    parts = spans // heads
    span = rows // chunks
    packed = span // 2

    tp = lax.axis_index("tp")
    core = lax.rem(tp, CORES)
    line = tp // CORES
    pair = line * CORES + (1 - core)
    me = lax.axis_index("sp")
    z = me // across
    x = lax.rem(me, across)
    my_head = me // parts
    my_part = lax.rem(me, parts)

    def owner_of(place):
        place_part = lax.rem(place, parts)
        return jnp.where((place // parts) % 2 == 0, place_part, parts - 1 - place_part)

    loads = []
    for index, source in enumerate((wk, wv, wq, wmk, wmv, wmq)):
        loads.append(
            pltpu.make_async_copy(
                source, weight_ref.at[:, pl.ds(index * width, width)], load_sems.at[index]
            )
        )
    loads.append(pltpu.make_async_copy(woa, soa, load_sems.at[6]))
    loads.append(pltpu.make_async_copy(wom, som, load_sems.at[7]))
    for copy in loads:
        copy.start()

    barrier = pltpu.get_barrier_semaphore()
    signal(barrier, "tp", pair)
    for step in range(1, lines):
        signal(barrier, "tp", lax.rem(line + step, lines) * CORES + core)
    for step in range(1, spans):
        signal(barrier, "sp", lax.rem(me + step, spans))

    position = (me * rows + lax.broadcasted_iota(jnp.int32, (1, rows), 1)).astype(jnp.float32)
    middle = DD // 2
    turn = lax.broadcasted_iota(jnp.int32, (middle, 1), 0)
    rates = jnp.zeros((middle, 1), jnp.float32)
    for index in range(middle):
        rates = jnp.where(turn == index, ROTARY_BASE ** (-index / middle), rates)
    angles = rates * position
    cosines = jnp.cos(angles)
    sines = jnp.sin(angles)
    cosine_ref[...] = jnp.concatenate([cosines] * (128 * 2 // DD), axis=0).T
    sine_ref[...] = jnp.concatenate([-sines, sines] * (128 // DD), axis=0).T
    lanes = lax.broadcasted_iota(jnp.int32, (1, 128), 1)
    former = lax.rem(lanes, DD) < DD // 2
    low_lanes = lanes < HEAD

    def columns_of(owner):
        return pl.ds(pl.multiple_of(owner * columns, 128), columns)

    def rows_of(chunk):
        return pl.ds(chunk * span, span)

    def place(owner, chunk):
        return x_ref.at[rows_of(chunk), columns_of(owner)]

    pl.semaphore_wait(barrier, lines + spans - 1)

    pairs = {}
    for chunk in range(chunks):
        for step in range(1, lines):
            copy = remote(
                shard_ref.at[rows_of(chunk)], place(tp, chunk), line_send,
                line_recv.at[step - 1, chunk], "tp", lax.rem(line + step, lines) * CORES + core,
            )
            copy.start()
    own_pair = remote(shard_ref, x_ref.at[:, columns_of(tp)], pair_send, own_recv, "tp", pair)
    own_pair.start()

    def take(values, at_rows, owner):
        floats = values.astype(jnp.float32)
        scaled_ref[at_rows, columns_of(owner)] = (floats * gain_ref[:, columns_of(owner)]).astype(
            jnp.bfloat16
        )
        return jnp.sum(floats * floats, axis=1, keepdims=True)

    everywhere = pl.ds(0, rows)
    squares = take(shard_ref[...], everywhere, tp)
    own_pair.wait_recv()
    square_ref[...] = squares + take(x_ref[:, columns_of(pair)], everywhere, pair)

    def line_columns(owner_line):
        return pl.ds(pl.multiple_of(owner_line * CORES * columns, 128), CORES * columns)

    couples = [slice(index * width, (index + 2) * width) for index in (0, 2, 4)]
    for index, couple in enumerate(couples):
        loads[2 * index].wait()
        loads[2 * index + 1].wait()
        sum_ref[:, couple] = dot(
            scaled_ref[:, line_columns(line)], weight_ref[line_columns(line), couple]
        )

    blank = jnp.zeros((8 - heads, features), jnp.float32)
    gate_weights = jnp.concatenate(
        [wi[...].astype(jnp.float32), blank, wf[...].astype(jnp.float32), blank], axis=0
    ).astype(jnp.bfloat16)
    gate_bias = jnp.concatenate(
        [jnp.zeros((1, 8), jnp.float32), bias_ref[...], jnp.zeros((1, 8 - heads), jnp.float32)],
        axis=1,
    )
    factor = (DD**-0.5) * LOG2E

    def rotated(wide, cosine, sine):
        partner = jnp.where(former, pltpu.roll(wide, 128 - DD // 2, 1), pltpu.roll(wide, DD // 2, 1))
        return wide * cosine + partner * sine

    def kv_sends(chunk):
        for rank in range(1, heads):
            head = near_first(my_head, heads, rank)
            yield remote(
                kv_out.at[head, rows_of(chunk)], kv_all.at[me, rows_of(chunk)],
                kv_send, land_recv.at[my_head, chunk], "sp", head * parts + my_part,
            )

    def forwards(source, origin, chunk):
        for step in range(1, parts):
            yield remote(
                source, kv_all.at[origin, rows_of(chunk)], fwd_send, cross_recv.at[origin], "sp",
                my_head * parts + lax.rem(my_part + step, parts),
            )

    points = {
        (1, 0): "chunk1", (1, 1): "chunk2", (1, 2): "projected", (2, 0): "projected",
        (1, 3): "state", (3, 0): "first", (2, 1): "first", (3, 1): "inner",
        (2, 2): "inner", (2, 3): "second", (3, 2): "seconded", (3, 3): "seconded",
    }

    def landed(rank):
        return near_first(my_head, heads, rank) * parts + my_part

    def forward(point, index=""):
        for rank in range(1, heads):
            for chunk in range(chunks):
                if points.get((rank, chunk), "inner") == f"{point}{index}":
                    origin = landed(rank)
                    at = kv_all.at[origin, rows_of(chunk)]
                    remote(
                        at, at, kv_send, land_recv.at[origin // parts, chunk], "sp", me
                    ).wait_recv()
                    for copy in forwards(at, origin, chunk):
                        copy.start()

    packed_of = lambda chunk: pl.ds(chunk * packed, packed)
    my_slot = me // parts
    my_owner = owner_of(me)

    def q_sends(chunk):
        for rank in range(1, heads):
            head = near_first(my_head, heads, rank)
            yield remote(
                q_out.at[head, packed_of(chunk)], q_all.at[my_slot, packed_of(chunk)],
                q_send, q_recv.at[my_slot], "sp", head * parts + my_owner,
            )

    def q_aside(chunk):
        return remote(
            q_out.at[my_head, packed_of(chunk)], q_all.at[my_slot, packed_of(chunk)],
            q_side, q_recv.at[my_slot], "sp", my_head * parts + my_owner,
        )

    def pull(chunk):
        for step in range(1, lines):
            source = lax.rem(line + lines - step, lines) * CORES + core
            at = place(source, chunk)
            remote(
                at, at, line_send, line_recv.at[step - 1, chunk], "tp", pair
            ).wait_recv()
            copy = remote(at, at, pair_send, pair_recv.at[step - 1, chunk], "tp", pair)
            copy.start()
            pairs[step, chunk] = copy

    pull(0)
    for chunk in range(chunks):
        at = rows_of(chunk)
        squares = square_ref[at]
        for step in range(1, lines):
            source = lax.rem(line + lines - step, lines) * CORES + core
            squares = squares + take(x_ref[at, columns_of(source)], at, source)
        for step in range(1, lines):
            source = lax.rem(line + lines - step, lines) * CORES + 1 - core
            pairs[step, chunk].wait_recv()
            squares = squares + take(x_ref[at, columns_of(source)], at, source)
        inverse = lax.rsqrt(squares / features + EPSILON)

        def products(index):
            total = sum_ref[at, couples[index]]
            for step in range(1, lines):
                other = line_columns(lax.rem(line + step, lines))
                total = total + dot(scaled_ref[at, other], weight_ref[other, couples[index]])
            total = (total * inverse).astype(jnp.bfloat16).astype(jnp.float32)
            return total[:, :width], total[:, width:]

        cosine = cosine_ref[at]
        sine = sine_ref[at]
        keys, values = products(0)
        for group in range(groups):
            lane_group = slice(group * 128, group * 128 + 128)
            key = rotated(keys[:, lane_group], cosine, sine)
            value = values[:, lane_group]
            kv_out[2 * group, at] = jnp.where(low_lanes, key, pltpu.roll(value, HEAD, 1)).astype(
                jnp.bfloat16
            )
            kv_out[2 * group + 1, at] = jnp.where(
                low_lanes, pltpu.roll(key, HEAD, 1), value
            ).astype(jnp.bfloat16)
        for copy in kv_sends(chunk):
            copy.start()
        for copy in forwards(kv_out.at[my_head, at], me, chunk):
            copy.start()
        kv_all[me, at] = kv_out[my_head, at]

        queries, memory_keys = products(1)
        for group in range(groups):
            query = rotated(queries[:, group * 128 : group * 128 + 128], cosine, sine) * factor
            top, bottom = query[:packed], query[packed:]
            q_out[2 * group, packed_of(chunk)] = jnp.where(
                low_lanes, top, pltpu.roll(bottom, HEAD, 1)
            ).astype(jnp.bfloat16)
            q_out[2 * group + 1, packed_of(chunk)] = jnp.where(
                low_lanes, pltpu.roll(top, HEAD, 1), bottom
            ).astype(jnp.bfloat16)
        for copy in q_sends(chunk):
            copy.start()

        @pl.when(my_owner == my_part)
        def _():
            q_all[my_slot, packed_of(chunk)] = q_out[my_head, packed_of(chunk)]

        @pl.when(my_owner != my_part)
        def _():
            q_aside(chunk).start()

        mk_ref[at] = memory_keys.astype(jnp.bfloat16)
        if chunk + 1 < chunks:
            pull(chunk + 1)
        memory_values, memory_queries = products(2)
        mv_ref[at] = memory_values.astype(jnp.bfloat16)
        mq_ref[at] = memory_queries.astype(jnp.bfloat16)
        pre_ref[at, :16] = dot(scaled_ref[at, :], gate_weights, ((1,), (1,))) * inverse + gate_bias
        if chunk < chunks - 1:
            forward("chunk", chunk)

    forward("projected")

    turned = pre_ref[...].T
    gate = turned[:8]
    pre = turned[8:16]
    shift = jnp.concatenate([shift_ref[...], jnp.zeros((8 - heads, rows), jnp.float32)], axis=0)
    forget = jnp.minimum(pre, 0.0) - jnp.log1p(jnp.exp(-jnp.abs(pre))) + shift
    first, rest = (part.astype(jnp.float32) for part in two_parts(forget))
    pieces = jnp.concatenate([first, rest, forget - first - rest], axis=0).astype(jnp.bfloat16)
    row_index = lax.broadcasted_iota(jnp.int32, (rows, rows), 0)
    column_index = lax.broadcasted_iota(jnp.int32, (rows, rows), 1)
    sums = dot(pieces, (row_index <= column_index).astype(jnp.bfloat16))
    cumulative = sums[:8] + (sums[8:16] + sums[16:24])
    cumulative_ref[...] = cumulative
    offset = gate - cumulative
    offset_ref[...] = jnp.concatenate([offset, jnp.zeros((120, rows), jnp.float32)], axis=0).T
    end = cumulative[:, rows - 1 : rows]
    toward = end + offset
    top = jnp.max(toward, axis=1, keepdims=True)
    end_weights = jnp.exp(toward - top) * (HEAD**-0.5)
    mv_turned[...] = mv_ref[...].T
    mq_turned[...] = mq_ref[...].T
    weighted = jnp.concatenate(
        [
            mv_turned[head * HEAD : (head + 1) * HEAD, :].astype(jnp.float32)
            * end_weights[head : head + 1, :]
            for head in range(heads)
        ]
        + [end_weights, end_weights],
        axis=0,
    )
    high, low = two_parts(weighted)
    whole = dot(high, mk_ref[...]) + dot(low, mk_ref[...])
    memory = jnp.zeros((HEAD, width), jnp.float32)
    normal = jnp.zeros((1, width), jnp.float32)
    top_row = jnp.zeros((1, width), jnp.float32)
    end_row = jnp.zeros((1, width), jnp.float32)
    for head in range(heads):
        chosen = head_mask(width, head)
        at_head = slice(head, head + 1)
        memory = jnp.where(chosen, whole[head * HEAD : (head + 1) * HEAD, :], memory)
        normal = jnp.where(chosen, whole[width + head : width + head + 1, :], normal)
        top_row = jnp.where(chosen, top[at_head], top_row)
        end_row = jnp.where(chosen, end[at_head], end_row)
    states_ref[x, :HEAD, :] = memory
    states_ref[x, HEAD : HEAD + 1, :] = normal
    states_ref[x, HEAD + 1 : HEAD + 2, :] = top_row
    states_ref[x, HEAD + 2 : HEAD + 3, :] = end_row
    states_ref[x, HEAD + 3 :, :] = jnp.zeros((STATE_ROWS - HEAD - 3, width), jnp.float32)

    def state_sends():
        for step in range(1, across):
            yield remote(
                states_ref.at[x], states_ref.at[x], st_send, st_recv.at[x], "sp",
                z * across + lax.rem(x + step, across),
            )

    forward("state")
    for copy in state_sends():
        copy.start()

    def inner():
        step_rows = 128
        for group in range(groups):
            lane_group = slice(group * 128, (group + 1) * 128)
            heads_here = (2 * group, 2 * group + 1)
            upper_half = lax.broadcasted_iota(jnp.int32, (128, step_rows), 0) < HEAD
            for start in range(0, rows, step_rows):
                stop = start + step_rows
                here = slice(start, stop)
                queries = mq_turned[lane_group, here].astype(jnp.float32)
                both = jnp.concatenate(
                    [jnp.where(upper_half, queries, 0.0), jnp.where(upper_half, 0.0, queries)], axis=1
                ).astype(jnp.bfloat16)
                scores = dot(mk_ref[:stop, lane_group], both)
                ahead = jnp.concatenate(
                    [cumulative_ref[head : head + 1, here] for head in heads_here], axis=1
                )
                behind = jnp.concatenate(
                    [
                        jnp.broadcast_to(offset_ref[:stop, head : head + 1], (stop, step_rows))
                        for head in heads_here
                    ],
                    axis=1,
                )
                key_index = lax.broadcasted_iota(jnp.int32, scores.shape, 0)
                query_index = lax.broadcasted_iota(jnp.int32, scores.shape, 1) % step_rows
                gaps = jnp.where(key_index <= query_index + start, ahead + behind, NEGATIVE)
                row_top = jnp.max(gaps, axis=0, keepdims=True)
                scores = jnp.exp(gaps - row_top) * (scores * (HEAD**-0.5))
                total = jnp.sum(scores, axis=0, keepdims=True)
                for side, head in enumerate(heads_here):
                    lanes_at = slice(side * step_rows, (side + 1) * step_rows)
                    inner_den[head : head + 1, here] = total[:, lanes_at]
                    inner_top[head : head + 1, here] = row_top[:, lanes_at]
                score_high, score_low = two_parts(scores)
                values = mv_turned[lane_group, :stop]
                numerator = dot(values, score_high) + dot(values, score_low)
                inner_ref[lane_group, here] = jnp.where(
                    upper_half, numerator[:, :step_rows], numerator[:, step_rows:]
                )

    def advance(body, stable, later):
        later_top = later[HEAD + 1 : HEAD + 2, :]
        decay = later[HEAD + 2 : HEAD + 3, :]
        new = jnp.maximum(decay + stable, later_top)
        return jnp.exp(decay + stable - new) * body + jnp.exp(later_top - new) * later, new

    def prefix_send():
        return remote(
            prefix_out, prefix_in, px_send, px_recv, "sp", jnp.minimum(me + across, spans - 1)
        )

    def level(body, stable):
        for other in range(across):

            @pl.when(x == other)
            def _():
                enter_ref[...] = body
                enter_ref[HEAD + 1 : HEAD + 2, :] = stable

            if other < across - 1:
                body, stable = advance(body, stable, states_ref[other])
        body, stable = advance(body, stable, states_ref[across - 1])

        @pl.when(z < depth - 1)
        def _():
            prefix_out[...] = body
            prefix_out[HEAD + 1 : HEAD + 2, :] = stable
            prefix_send().start()

    def chain():
        for step in range(1, across):
            other = lax.rem(x + step, across)
            at = states_ref.at[other]
            remote(at, at, st_send, st_recv.at[other], "sp", me).wait_recv()

        @pl.when(z == 0)
        def _():
            prefix_in[...] = jnp.zeros((STATE_ROWS, width), jnp.float32)

        pl.when(z > 0)(lambda: prefix_send().wait_recv())
        body = prefix_in[...]
        level(body, body[HEAD + 1 : HEAD + 2, :])

    top_ref[...] = jnp.full(top_ref.shape, NEGATIVE, jnp.float32)
    acc_ref[...] = jnp.zeros(acc_ref.shape, jnp.float32)
    units = spans // 2
    half_rows = rows // 2

    def run(steps):
        def score(step):
            slot, wave, place, diagonal = step
            if not diagonal:
                return dot(kv_all[place], qt_ref[slot, wave])
            visible = (wave + 1) * half_rows
            scores = dot(kv_all[place, :visible], qt_ref[slot, wave])
            key_index = lax.broadcasted_iota(jnp.int32, scores.shape, 0)
            query_index = lax.broadcasted_iota(jnp.int32, scores.shape, 1)
            query_index = jnp.where(query_index >= half_rows, query_index - half_rows, query_index)
            return jnp.where(key_index <= query_index + wave * half_rows, scores, NEGATIVE)

        def soften(step, scores):
            slot, wave, place, diagonal = step
            old_top = top_ref[slot, wave]
            top = jnp.maximum(jnp.max(scores, axis=0, keepdims=True), old_top)
            top_ref[slot, wave] = top
            return jnp.exp2(old_top - top), jnp.exp2(scores - top).astype(jnp.bfloat16)

        def gather_up(step, shrink, weights):
            slot, wave, place, diagonal = step
            sums = dot(vt_ref[place, :, : weights.shape[0]], weights)
            acc_ref[slot, wave] = acc_ref[slot, wave] * shrink + sums

        count = len(steps)
        scores = [score(step) for step in steps[:2]]
        held = None
        for index, step in enumerate(steps):
            if index + 2 < count:
                scores.append(score(steps[index + 2]))
            if held is not None:
                gather_up(steps[index - 1], *held)
            held = soften(step, scores[index])
        gather_up(steps[-1], *held)

    def visit_unit(rank):
        return near_first(me // 2, units, rank)

    def arrive(origin):
        @pl.when((origin != me) & (lax.rem(origin, parts) != my_part))
        def _():
            at = kv_all.at[origin]
            remote(at, at, fwd_send, cross_recv.at[origin], "sp", me).wait_recv()

        turned = kv_all[origin].T
        vt_ref[origin, :HEAD, :] = turned[HEAD:, :]
        vt_ref[origin, HEAD:, :] = jnp.ones((VALUE_ROWS - HEAD, rows), jnp.bfloat16)

        @pl.when(owner_of(origin) == my_part)
        def _():
            slot = origin // parts

            @pl.when(origin != me)
            def _():
                at = q_all.at[slot]
                remote(at, at, q_send, q_recv.at[slot], "sp", me).wait_recv()

            for chunk in range(chunks):
                wave = chunk * span // half_rows
                start = chunk * span - wave * half_rows
                low_rows = q_all[slot, packed_of(chunk)].astype(jnp.float32)
                high_rows = pltpu.roll(low_rows, HEAD, 1)
                for half in range(2):
                    chosen = (lanes // DD) == half
                    for side, values in enumerate((low_rows, high_rows)):
                        qn_ref[
                            wave, pl.ds(half * half_rows + start + side * packed, packed)
                        ] = jnp.where(chosen, values, 0.0).astype(jnp.bfloat16)
            for wave in range(2):
                qt_ref[slot, wave] = qn_ref[wave].T

    def mine(unit):
        return [owner_of(2 * unit + side) == my_part for side in range(2)]

    def within(unit, waves):
        chosen = mine(unit)

        @pl.when(chosen[0])
        def _():
            slot = 2 * unit // parts
            run([(slot, wave, 2 * unit, True) for wave in waves])

        @pl.when(chosen[1])
        def _():
            slot = (2 * unit + 1) // parts
            run(
                [(slot, wave, 2 * unit, False) for wave in waves]
                + [(slot, wave, 2 * unit + 1, True) for wave in waves]
            )

    def across_units(unit, other, waves):
        query = jnp.maximum(unit, other)
        key = jnp.minimum(unit, other)

        def both(slot):
            run([(slot, wave, 2 * key + side, False) for side in range(2) for wave in waves])

        if parts == 2:
            both(query)
        else:
            chosen = mine(query)
            for side in range(2):
                pl.when(chosen[side])(functools.partial(both, (2 * query + side) // parts))

    def settle(unit):
        for side in range(2):
            arrive(2 * unit + side)

    def visit(rank, unused):
        unit = visit_unit(rank)
        settle(unit)
        pl.when(rank == 1)(lambda: forward("second"))
        pl.when((z > 0) & (rank == z + 1))(chain)
        within(unit, (0, 1))

        def earlier(other_rank, unused):
            across_units(unit, visit_unit(other_rank), (0, 1))
            return unused

        lax.fori_loop(0, rank, earlier, 0)
        pl.when(rank == 1)(lambda: forward("seconded"))
        return unused

    eye = lax.broadcasted_iota(jnp.int32, (HEAD, HEAD), 0) == lax.broadcasted_iota(
        jnp.int32, (HEAD, HEAD), 1
    )
    head_gain = jnp.sum(jnp.where(eye, head_gain_ref[...], 0.0), axis=1, keepdims=True)
    head_lanes = lax.broadcasted_iota(jnp.int32, lambda_ref.shape, 1)
    factor_second = jnp.sum(
        jnp.where(head_lanes == my_head, lambda_ref[...], 0.0), axis=1, keepdims=True
    )

    def span_of(slot):
        return slot * parts + (my_part if slot % 2 == 0 else parts - 1 - my_part)

    def att_place(wave):
        return attended_ref.at[wave, pl.ds(pl.multiple_of(my_head * HEAD, HEAD), HEAD)]

    def att_copy(slot, wave):
        return remote(
            att_out.at[slot, wave], att_place(wave), att_send,
            att_recv.at[my_head, wave], "sp", span_of(slot),
        )

    def finish(wave):
        for slot in range(heads):
            sums = acc_ref[slot, wave]
            maps = sums[:HEAD] / sums[HEAD : HEAD + 1]
            second = pltpu.roll(maps, half_rows, 1)[:, :half_rows]
            difference = maps[:, :half_rows] - factor_second * second
            mean = jnp.mean(difference * difference, axis=0, keepdims=True)
            att_out[slot, wave] = (
                difference * lax.rsqrt(mean + EPSILON) * head_gain
            ).astype(jnp.bfloat16)

            @pl.when(span_of(slot) == me)
            def _():
                att_place(wave)[...] = att_out[slot, wave]

            @pl.when(span_of(slot) != me)
            def _():
                att_copy(slot, wave).start()

    def recall():
        memory_in = enter_ref[:HEAD, :]
        normal_in = enter_ref[HEAD : HEAD + 1, :]
        head_of_lane = lax.broadcasted_iota(jnp.int32, (16, width), 1) // HEAD
        head_of_row = lax.broadcasted_iota(jnp.int32, (16, width), 0)
        blocks = jnp.concatenate(
            [jnp.where(head_mask(width, head), memory_in, 0.0) for head in range(heads)]
            + [jnp.where(head_of_lane == head_of_row, normal_in, 0.0)],
            axis=0,
        )
        high, low = two_parts(blocks)
        carried = dot(high, mq_turned[...]) + dot(low, mq_turned[...])
        head_rows = lax.broadcasted_iota(jnp.int32, (heads, 1), 0)
        stable = jnp.zeros((heads, 1), jnp.float32)
        for head in range(heads):
            stable = jnp.where(
                head_rows == head,
                enter_ref[HEAD + 1 : HEAD + 2, head * HEAD : head * HEAD + 1],
                stable,
            )
        carried_log = cumulative_ref[:heads] + stable
        own_top = inner_top[:heads]
        row_top = jnp.maximum(carried_log, own_top)
        inside = jnp.exp(own_top - row_top)
        outside = jnp.exp(carried_log - row_top)
        denominator = inside * inner_den[:heads] + outside * carried[width : width + heads]
        denominator = jnp.maximum(jnp.abs(denominator), 1.0)
        inside = inside / denominator
        outside = outside / denominator
        for head in range(heads):
            at = slice(head * HEAD, (head + 1) * HEAD)
            one = slice(head, head + 1)
            memory_ref[at, :] = (inside[one] * inner_ref[at, :] + outside[one] * carried[at]).astype(
                jnp.bfloat16
            )
        loads[6].wait()
        loads[7].wait()
        partial_ref[...] = dot(memory_ref[...], som[...], ((0,), (0,)))

    settle(me // 2)
    within(me // 2, (0, 1))
    forward("first")
    inner()
    forward("inner")
    pl.when(z == 0)(chain)
    lax.fori_loop(1, units - 1, visit, 0)
    last = visit_unit(units - 1)
    settle(last)
    for wave in range(2):
        within(last, (wave,))
        if parts == 2:
            steps = []
            for rank in range(units - 1):
                other = visit_unit(rank)
                query = jnp.maximum(last, other)
                key = jnp.minimum(last, other)
                steps.append([(query, wave, 2 * key + side, False) for side in range(2)])
            run([step for side in zip(*steps) for step in side])
        else:

            def earlier(rank, unused):
                across_units(last, visit_unit(rank), (wave,))
                return unused

            lax.fori_loop(0, units - 1, earlier, 0)
        finish(wave)
        if wave == 0:
            pl.when(z == units - 2)(chain)
            pl.when(z < units - 1)(recall)
    @pl.when(z >= units - 1)
    def _():
        chain()
        recall()

    out_span = rows // out_chunks
    per_wave = out_chunks // 2

    def out_rows(chunk):
        return pl.ds(chunk * out_span, out_span)

    order = list(range(1, lines)) + [0]
    swaps = {}
    lined = {}

    def pair_sum(step, chunk):
        swaps[step, chunk].wait_recv()
        mine = part_ref[
            out_rows(chunk), columns_of(lax.rem(line + step, lines) * CORES + core)
        ]
        return mine.astype(jnp.float32) + pair_in[step, out_rows(chunk), :].astype(jnp.float32)

    def pass_on(chunk):
        for step in range(1, lines):
            line_out[step, out_rows(chunk), :] = pair_sum(step, chunk).astype(jnp.bfloat16)
            copy = remote(
                line_out.at[step, out_rows(chunk)], line_in.at[step, out_rows(chunk)],
                sl_send, sl_recv.at[step - 1, chunk], "tp",
                lax.rem(line + step, lines) * CORES + core,
            )
            copy.start()
            lined[step, chunk] = copy

    for wave in range(2):
        for step in range(heads):

            @pl.when((my_owner != my_part) | (my_head != step))
            def _():
                at = attended_ref.at[wave, pl.ds(step * HEAD, HEAD)]
                remote(at, at, att_send, att_recv.at[step, wave], "sp", me).wait_recv()

        at = slice(wave * half_rows, (wave + 1) * half_rows)
        part_ref[at, :] = (
            dot(attended_ref[wave], soa[...], ((0,), (0,))) + partial_ref[at, :]
        ).astype(jnp.bfloat16)
        for chunk in range(wave * per_wave, (wave + 1) * per_wave):
            for step in order:
                target = lax.rem(line + step, lines) * CORES + (1 - core)
                copy = remote(
                    part_ref.at[out_rows(chunk), columns_of(target)],
                    pair_in.at[step, out_rows(chunk)], sp_send,
                    sp_recv.at[step, chunk], "tp", pair,
                )
                copy.start()
                swaps[step, chunk] = copy
        for chunk in range(wave * per_wave, (wave + 1) * per_wave):
            pass_on(chunk)

    def sent(ref, semaphore):
        remote(ref, ref, semaphore, semaphore, "tp", pair).wait_send()

    others = line_in.at[pl.ds(1, lines - 1)]
    sent(others, line_send)
    sent(pair_in, pair_send)
    sent(kv_out.at[pl.ds(0, heads - 1)], kv_send)
    sent(kv_all.at[pl.ds(0, heads * (parts - 1))], fwd_send)
    sent(q_out.at[pl.ds(0, heads - 1)], q_send)
    pl.when(my_owner != my_part)(lambda: sent(q_out.at[0], q_side))
    sent(states_ref.at[pl.ds(0, across - 1)], st_send)
    pl.when(z < depth - 1)(lambda: prefix_send().wait_send())
    pl.when(my_owner == my_part)(lambda: sent(att_out.at[pl.ds(0, heads - 1)], att_send))
    pl.when(my_owner != my_part)(lambda: sent(att_out, att_send))
    for chunk in range(out_chunks):
        total = pair_sum(0, chunk)
        for step in range(1, lines):
            lined[step, chunk].wait_recv()
            total = total + line_in[step, out_rows(chunk), :].astype(jnp.float32)
        total_ref[out_rows(chunk), :] = total.astype(jnp.bfloat16)
        copy = pltpu.make_async_copy(
            total_ref.at[out_rows(chunk)], out_ref.at[out_rows(chunk)], out_sem
        )
        copy.start()
    pltpu.make_async_copy(total_ref, out_ref, out_sem).wait()
    sent(pair_in, sp_send)
    sent(others, sl_send)


def per_device(tp_size, depth, across, inputs, norm_gain, query_weight, key_weight, value_weight,
               memory_query_weight, memory_key_weight, memory_value_weight, input_gate_weight,
               forget_gate_weight, forget_bias, decay_shift, lambdas, head_gain,
               out_weight_attention, out_weight_memory):
    rows, columns = inputs.shape
    features = norm_gain.shape[0]
    width = query_weight.shape[1]
    heads = width // HEAD
    lines = tp_size // CORES
    spans = depth * across
    parts = spans // heads
    chunks = 4
    out_chunks = 4
    dma = pltpu.SemaphoreType.DMA


    hbm = pl.BlockSpec(memory_space=pl.ANY)
    bf16 = lambda *shape: pltpu.VMEM(shape, jnp.bfloat16)
    f32 = lambda *shape: pltpu.VMEM(shape, jnp.float32)
    return pl.pallas_call(
        functools.partial(layer_kernel, tp_size, depth, across, chunks, out_chunks),
        out_shape=jax.ShapeDtypeStruct((rows, columns), jnp.bfloat16),
        in_specs=[VMEM] * 2 + [hbm] * 6 + [VMEM] * 6 + [hbm] * 2,
        out_specs=hbm,
        scratch_shapes=[bf16(features, 6 * width)]
        + [bf16(width, features)] * 2
        + [
            bf16(rows, features), bf16(rows, features), f32(rows, 1), f32(rows, 6 * width),
            f32(rows, 128), f32(rows, 128),
            bf16(heads, rows, 128), bf16(heads, rows // 2, 128), bf16(spans, rows, 128),
            bf16(heads, rows // 2, 128), bf16(spans, VALUE_ROWS, rows),
            bf16(2, rows, 128), bf16(heads, 2, 128, rows), f32(heads, 2, 1, rows),
            f32(heads, 2, VALUE_ROWS, rows), bf16(heads, 2, HEAD, rows // 2),
            bf16(2, width, rows // 2),
            bf16(rows, width), bf16(rows, width), bf16(rows, width), bf16(width, rows),
            bf16(width, rows), f32(rows, 128),
            f32(across, STATE_ROWS, width), f32(STATE_ROWS, width), f32(STATE_ROWS, width),
            f32(STATE_ROWS, width),
            f32(width, rows), f32(8, rows), f32(8, rows), f32(8, rows), f32(rows, 128),
            bf16(width, rows),
            f32(rows, features), bf16(rows, features), bf16(lines, rows, columns),
            bf16(lines, rows, columns),
            bf16(lines, rows, columns), bf16(rows, columns),
            dma(()), dma((8,)), dma(()), dma((lines - 1, chunks)), dma(()),
            dma((lines - 1, chunks)), dma(()),
            dma(()), dma(()), dma((heads, chunks)), dma((spans,)), dma(()), dma(()),
            dma((heads,)), dma(()), dma((heads, 2)),
            dma(()), dma((across,)), dma(()), dma(()), dma(()), dma((lines, out_chunks)), dma(()),
            dma((lines - 1, out_chunks)),
        ],
        compiler_params=pltpu.CompilerParams(
            vmem_limit_bytes=VMEM_LIMIT, collective_id=0, has_side_effects=True
        ),
        name="layer",
    )(
        inputs, norm_gain[None, :], query_weight, key_weight, value_weight,
        memory_query_weight, memory_key_weight, memory_value_weight, input_gate_weight.T,
        forget_gate_weight.T, forget_bias[None, :], decay_shift.T, lambdas[None, :],
        head_gain[None, :], out_weight_attention, out_weight_memory,
    )


def columns_across(mesh):
    spans = mesh.shape["sp"]
    try:
        places = {device.coords[0] for device in mesh.devices.flat}
        across = len(places)
    except AttributeError:
        across = 2
    return across if spans % across == 0 else 1


def solution(mesh):
    across = columns_across(mesh)
    in_specs = (
        P("sp", "tp"),
        P(),
        P(None, "tp"),
        P(None, "tp"),
        P(None, "tp"),
        P(None, "tp"),
        P(None, "tp"),
        P(None, "tp"),
        P(None, "tp"),
        P(None, "tp"),
        P("tp"),
        P("sp", "tp"),
        P("tp"),
        P(),
        P("tp", None),
        P("tp", None),
    )
    return jax.shard_map(
        functools.partial(
            per_device, mesh.shape["tp"], mesh.shape["sp"] // across, across
        ),
        mesh=mesh,
        in_specs=in_specs,
        out_specs=P("sp", "tp"),
        check_vma=False,
    )
```

```python
import functools

import jax
import jax.numpy as jnp
from jax import lax
from jax.experimental import pallas as pl
from jax.experimental.pallas import tpu as pltpu
from jax.sharding import PartitionSpec as P

HEAD = 64
DD = 32
EPSILON = 1e-06
ROTARY_BASE = 10000.0
NEGATIVE = -1e30
LOG2E = 1.4426950408889634
CORES = 2
STATE_ROWS = HEAD + 8
VALUE_ROWS = HEAD + 16
VMEM = pl.BlockSpec(memory_space=pltpu.VMEM)
MESH = pl.DeviceIdType.MESH
VMEM_LIMIT = 60 * 1024 * 1024


def signal(semaphore, axis, place):
    pl.semaphore_signal(semaphore, inc=1, device_id={axis: place}, device_id_type=MESH)


def remote(source, target, send_sem, recv_sem, axis, place):
    return pltpu.make_async_remote_copy(
        src_ref=source,
        dst_ref=target,
        send_sem=send_sem,
        recv_sem=recv_sem,
        device_id={axis: place},
        device_id_type=MESH,
    )


def head_mask(width, head):
    lanes = lax.broadcasted_iota(jnp.int32, (1, width), 1)
    return (lanes // HEAD) == head


def two_parts(floats):
    high = floats.astype(jnp.bfloat16)
    return high, (floats - high.astype(jnp.float32)).astype(jnp.bfloat16)


def dot(a, b, dims=((1,), (0,))):
    return lax.dot_general(a, b, (dims, ((), ())), preferred_element_type=jnp.float32)


def near_first(place, count, rank):
    both = jnp.minimum(place, count - 1 - place)
    half = (rank + 1) // 2
    low = place < count - 1 - place
    below = jnp.where(low, rank % 2 == 1, rank % 2 == 0)
    alternating = jnp.where(below, place - half, place + half)
    one_sided = jnp.where(low, rank, count - 1 - rank)
    return jnp.where(rank <= 2 * both, alternating, one_sided)


def layer_kernel(
    size, depth, across, chunks, out_chunks,
    shard_ref, gain_ref, wq, wk, wv, wmq, wmk, wmv, wi, wf, bias_ref, shift_ref,
    lambda_ref, head_gain_ref, woa, wom,
    out_ref,
    weight_ref, soa, som, x_ref, scaled_ref, square_ref, sum_ref, cosine_ref, sine_ref,
    kv_out, q_out, kv_all, q_all, vt_ref, qn_ref, qt_ref, top_ref, acc_ref, att_out, attended_ref,
    mq_ref, mk_ref, mv_ref, mq_turned, mv_turned, pre_ref, states_ref, state_rows, prefix_in, row_in, prefix_out, row_out,
    enter_ref,
    inner_ref, inner_den, inner_top, cumulative_ref, offset_ref, memory_ref,
    partial_ref, part_ref, pair_in, line_out, line_in, total_ref,
    out_sem, load_sems, line_send, line_recv, pair_send, pair_recv, own_recv,
    kv_send, fwd_send, land_recv, cross_recv, q_send, q_side, q_recv, att_send, att_recv,
    st_send, st_recv, px_send, px_recv, sp_send, sp_recv, sl_send, sl_recv,
):
    rows, columns = shard_ref.shape
    features = x_ref.shape[1]
    width = mq_ref.shape[1]
    heads = width // HEAD
    groups = width // 128
    lines = size // CORES
    spans = depth * across
    parts = spans // heads
    span = rows // chunks
    packed = span // 2

    tp = lax.axis_index("tp")
    core = lax.rem(tp, CORES)
    line = tp // CORES
    pair = line * CORES + (1 - core)
    me = lax.axis_index("sp")
    z = me // across
    x = lax.rem(me, across)
    my_head = me // parts
    my_part = lax.rem(me, parts)

    def owner_of(place):
        place_part = lax.rem(place, parts)
        return jnp.where((place // parts) % 2 == 0, place_part, parts - 1 - place_part)

    loads = []
    for index, source in enumerate((wk, wv, wq, wmk, wmv, wmq)):
        loads.append(
            pltpu.make_async_copy(
                source, weight_ref.at[:, pl.ds(index * width, width)], load_sems.at[index]
            )
        )
    loads.append(pltpu.make_async_copy(woa, soa, load_sems.at[6]))
    loads.append(pltpu.make_async_copy(wom, som, load_sems.at[7]))
    for copy in loads:
        copy.start()

    barrier = pltpu.get_barrier_semaphore()
    signal(barrier, "tp", pair)
    for step in range(1, lines):
        signal(barrier, "tp", lax.rem(line + step, lines) * CORES + core)
    for step in range(1, spans):
        signal(barrier, "sp", lax.rem(me + step, spans))

    position = (me * rows + lax.broadcasted_iota(jnp.int32, (1, rows), 1)).astype(jnp.float32)
    middle = DD // 2
    turn = lax.broadcasted_iota(jnp.int32, (middle, 1), 0)
    rates = jnp.zeros((middle, 1), jnp.float32)
    for index in range(middle):
        rates = jnp.where(turn == index, ROTARY_BASE ** (-index / middle), rates)
    angles = rates * position
    cosines = jnp.cos(angles)
    sines = jnp.sin(angles)
    cosine_ref[...] = jnp.concatenate([cosines] * (128 * 2 // DD), axis=0).T
    sine_ref[...] = jnp.concatenate([-sines, sines] * (128 // DD), axis=0).T
    lanes = lax.broadcasted_iota(jnp.int32, (1, 128), 1)
    former = lax.rem(lanes, DD) < DD // 2
    low_lanes = lanes < HEAD

    def columns_of(owner):
        return pl.ds(pl.multiple_of(owner * columns, 128), columns)

    def rows_of(chunk):
        return pl.ds(chunk * span, span)

    def place(owner, chunk):
        return x_ref.at[rows_of(chunk), columns_of(owner)]

    pl.semaphore_wait(barrier, lines + spans - 1)

    pairs = {}
    for chunk in range(chunks):
        for step in range(1, lines):
            copy = remote(
                shard_ref.at[rows_of(chunk)], place(tp, chunk), line_send,
                line_recv.at[step - 1, chunk], "tp", lax.rem(line + step, lines) * CORES + core,
            )
            copy.start()
    own_pair = remote(shard_ref, x_ref.at[:, columns_of(tp)], pair_send, own_recv, "tp", pair)
    own_pair.start()

    def take(values, at_rows, owner):
        floats = values.astype(jnp.float32)
        scaled_ref[at_rows, columns_of(owner)] = (floats * gain_ref[:, columns_of(owner)]).astype(
            jnp.bfloat16
        )
        return jnp.sum(floats * floats, axis=1, keepdims=True)

    everywhere = pl.ds(0, rows)
    squares = take(shard_ref[...], everywhere, tp)
    own_pair.wait_recv()
    square_ref[...] = squares + take(x_ref[:, columns_of(pair)], everywhere, pair)

    def line_columns(owner_line):
        return pl.ds(pl.multiple_of(owner_line * CORES * columns, 128), CORES * columns)

    couples = [slice(index * width, (index + 2) * width) for index in (0, 2, 4)]
    for index, couple in enumerate(couples):
        loads[2 * index].wait()
        loads[2 * index + 1].wait()
        sum_ref[:, couple] = dot(
            scaled_ref[:, line_columns(line)], weight_ref[line_columns(line), couple]
        )

    blank = jnp.zeros((8 - heads, features), jnp.float32)
    gate_weights = jnp.concatenate(
        [wi[...].astype(jnp.float32), blank, wf[...].astype(jnp.float32), blank], axis=0
    ).astype(jnp.bfloat16)
    gate_bias = jnp.concatenate(
        [jnp.zeros((1, 8), jnp.float32), bias_ref[...], jnp.zeros((1, 8 - heads), jnp.float32)],
        axis=1,
    )
    factor = (DD**-0.5) * LOG2E

    def rotated(wide, cosine, sine):
        partner = jnp.where(former, pltpu.roll(wide, 128 - DD // 2, 1), pltpu.roll(wide, DD // 2, 1))
        return wide * cosine + partner * sine

    def kv_sends(chunk):
        for rank in range(1, heads):
            head = near_first(my_head, heads, rank)
            yield remote(
                kv_out.at[head, rows_of(chunk)], kv_all.at[me, rows_of(chunk)],
                kv_send, land_recv.at[my_head, chunk], "sp", head * parts + my_part,
            )

    def forwards(source, origin, chunk):
        for step in range(1, parts):
            yield remote(
                source, kv_all.at[origin, rows_of(chunk)], fwd_send, cross_recv.at[origin], "sp",
                my_head * parts + lax.rem(my_part + step, parts),
            )

    points = {
        (1, 0): "chunk1", (1, 1): "chunk2", (1, 2): "projected", (2, 0): "projected",
        (1, 3): "state", (3, 0): "first", (2, 1): "first", (3, 1): "inner",
        (2, 2): "inner", (2, 3): "second", (3, 2): "seconded", (3, 3): "seconded",
    }

    def landed(rank):
        return near_first(my_head, heads, rank) * parts + my_part

    def forward(point, index=""):
        for rank in range(1, heads):
            for chunk in range(chunks):
                if points.get((rank, chunk), "inner") == f"{point}{index}":
                    origin = landed(rank)
                    at = kv_all.at[origin, rows_of(chunk)]
                    remote(
                        at, at, kv_send, land_recv.at[origin // parts, chunk], "sp", me
                    ).wait_recv()
                    for copy in forwards(at, origin, chunk):
                        copy.start()

    packed_of = lambda chunk: pl.ds(chunk * packed, packed)
    my_slot = me // parts
    my_owner = owner_of(me)

    def q_sends(chunk):
        for rank in range(1, heads):
            head = near_first(my_head, heads, rank)
            yield remote(
                q_out.at[head, packed_of(chunk)], q_all.at[my_slot, packed_of(chunk)],
                q_send, q_recv.at[my_slot], "sp", head * parts + my_owner,
            )

    def q_aside(chunk):
        return remote(
            q_out.at[my_head, packed_of(chunk)], q_all.at[my_slot, packed_of(chunk)],
            q_side, q_recv.at[my_slot], "sp", my_head * parts + my_owner,
        )

    def pull(chunk):
        for step in range(1, lines):
            source = lax.rem(line + lines - step, lines) * CORES + core
            at = place(source, chunk)
            remote(
                at, at, line_send, line_recv.at[step - 1, chunk], "tp", pair
            ).wait_recv()
            copy = remote(at, at, pair_send, pair_recv.at[step - 1, chunk], "tp", pair)
            copy.start()
            pairs[step, chunk] = copy

    pull(0)
    for chunk in range(chunks):
        at = rows_of(chunk)
        squares = square_ref[at]
        for step in range(1, lines):
            source = lax.rem(line + lines - step, lines) * CORES + core
            squares = squares + take(x_ref[at, columns_of(source)], at, source)
        for step in range(1, lines):
            source = lax.rem(line + lines - step, lines) * CORES + 1 - core
            pairs[step, chunk].wait_recv()
            squares = squares + take(x_ref[at, columns_of(source)], at, source)
        inverse = lax.rsqrt(squares / features + EPSILON)

        def products(index):
            total = sum_ref[at, couples[index]]
            for step in range(1, lines):
                other = line_columns(lax.rem(line + step, lines))
                total = total + dot(scaled_ref[at, other], weight_ref[other, couples[index]])
            total = (total * inverse).astype(jnp.bfloat16).astype(jnp.float32)
            return total[:, :width], total[:, width:]

        cosine = cosine_ref[at]
        sine = sine_ref[at]
        keys, values = products(0)
        for group in range(groups):
            lane_group = slice(group * 128, group * 128 + 128)
            key = rotated(keys[:, lane_group], cosine, sine)
            value = values[:, lane_group]
            kv_out[2 * group, at] = jnp.where(low_lanes, key, pltpu.roll(value, HEAD, 1)).astype(
                jnp.bfloat16
            )
            kv_out[2 * group + 1, at] = jnp.where(
                low_lanes, pltpu.roll(key, HEAD, 1), value
            ).astype(jnp.bfloat16)
        for copy in kv_sends(chunk):
            copy.start()
        for copy in forwards(kv_out.at[my_head, at], me, chunk):
            copy.start()
        kv_all[me, at] = kv_out[my_head, at]

        queries, memory_keys = products(1)
        for group in range(groups):
            query = rotated(queries[:, group * 128 : group * 128 + 128], cosine, sine) * factor
            top, bottom = query[:packed], query[packed:]
            q_out[2 * group, packed_of(chunk)] = jnp.where(
                low_lanes, top, pltpu.roll(bottom, HEAD, 1)
            ).astype(jnp.bfloat16)
            q_out[2 * group + 1, packed_of(chunk)] = jnp.where(
                low_lanes, pltpu.roll(top, HEAD, 1), bottom
            ).astype(jnp.bfloat16)
        for copy in q_sends(chunk):
            copy.start()

        @pl.when(my_owner == my_part)
        def _():
            q_all[my_slot, packed_of(chunk)] = q_out[my_head, packed_of(chunk)]

        @pl.when(my_owner != my_part)
        def _():
            q_aside(chunk).start()

        mk_ref[at] = memory_keys.astype(jnp.bfloat16)
        if chunk + 1 < chunks:
            pull(chunk + 1)
        memory_values, memory_queries = products(2)
        mv_ref[at] = memory_values.astype(jnp.bfloat16)
        mq_ref[at] = memory_queries.astype(jnp.bfloat16)
        pre_ref[at, :16] = dot(scaled_ref[at, :], gate_weights, ((1,), (1,))) * inverse + gate_bias
        if chunk < chunks - 1:
            forward("chunk", chunk)

    forward("projected")

    turned = pre_ref[...].T
    gate = turned[:8]
    pre = turned[8:16]
    shift = jnp.concatenate([shift_ref[...], jnp.zeros((8 - heads, rows), jnp.float32)], axis=0)
    forget = jnp.minimum(pre, 0.0) - jnp.log1p(jnp.exp(-jnp.abs(pre))) + shift
    first, rest = (part.astype(jnp.float32) for part in two_parts(forget))
    pieces = jnp.concatenate([first, rest, forget - first - rest], axis=0).astype(jnp.bfloat16)
    row_index = lax.broadcasted_iota(jnp.int32, (rows, rows), 0)
    column_index = lax.broadcasted_iota(jnp.int32, (rows, rows), 1)
    sums = dot(pieces, (row_index <= column_index).astype(jnp.bfloat16))
    cumulative = sums[:8] + (sums[8:16] + sums[16:24])
    cumulative_ref[...] = cumulative
    offset = gate - cumulative
    offset_ref[...] = jnp.concatenate([offset, jnp.zeros((120, rows), jnp.float32)], axis=0).T
    end = cumulative[:, rows - 1 : rows]
    toward = end + offset
    top = jnp.max(toward, axis=1, keepdims=True)
    end_weights = jnp.exp(toward - top) * (HEAD**-0.5)
    mv_turned[...] = mv_ref[...].T
    mq_turned[...] = mq_ref[...].T
    weighted = jnp.concatenate(
        [
            mv_turned[head * HEAD : (head + 1) * HEAD, :].astype(jnp.float32)
            * end_weights[head : head + 1, :]
            for head in range(heads)
        ]
        + [end_weights, end_weights],
        axis=0,
    )
    high, low = two_parts(weighted)
    whole = dot(high, mk_ref[...]) + dot(low, mk_ref[...])
    memory = jnp.zeros((HEAD, width), jnp.float32)
    normal = jnp.zeros((1, width), jnp.float32)
    top_row = jnp.zeros((1, width), jnp.float32)
    end_row = jnp.zeros((1, width), jnp.float32)
    for head in range(heads):
        chosen = head_mask(width, head)
        at_head = slice(head, head + 1)
        memory = jnp.where(chosen, whole[head * HEAD : (head + 1) * HEAD, :], memory)
        normal = jnp.where(chosen, whole[width + head : width + head + 1, :], normal)
        top_row = jnp.where(chosen, top[at_head], top_row)
        end_row = jnp.where(chosen, end[at_head], end_row)
    states_ref[x] = memory.astype(jnp.bfloat16)
    state_rows[x] = jnp.concatenate(
        [normal, top_row, end_row, jnp.zeros((5, width), jnp.float32)], axis=0
    )

    def state_sends():
        for step in range(1, across):
            for index, ref in enumerate((states_ref, state_rows)):
                yield remote(
                    ref.at[x], ref.at[x], st_send.at[index], st_recv.at[index, x], "sp",
                    z * across + lax.rem(x + step, across),
                )

    forward("state")
    for copy in state_sends():
        copy.start()

    def inner():
        step_rows = 128
        for group in range(groups):
            lane_group = slice(group * 128, (group + 1) * 128)
            heads_here = (2 * group, 2 * group + 1)
            upper_half = lax.broadcasted_iota(jnp.int32, (128, step_rows), 0) < HEAD
            for start in range(0, rows, step_rows):
                stop = start + step_rows
                here = slice(start, stop)
                queries = mq_turned[lane_group, here].astype(jnp.float32)
                both = jnp.concatenate(
                    [jnp.where(upper_half, queries, 0.0), jnp.where(upper_half, 0.0, queries)], axis=1
                ).astype(jnp.bfloat16)
                scores = dot(mk_ref[:stop, lane_group], both)
                ahead = jnp.concatenate(
                    [cumulative_ref[head : head + 1, here] for head in heads_here], axis=1
                )
                behind = jnp.concatenate(
                    [
                        jnp.broadcast_to(offset_ref[:stop, head : head + 1], (stop, step_rows))
                        for head in heads_here
                    ],
                    axis=1,
                )
                key_index = lax.broadcasted_iota(jnp.int32, scores.shape, 0)
                query_index = lax.broadcasted_iota(jnp.int32, scores.shape, 1) % step_rows
                gaps = jnp.where(key_index <= query_index + start, ahead + behind, NEGATIVE)
                row_top = jnp.max(gaps, axis=0, keepdims=True)
                scores = jnp.exp(gaps - row_top) * (scores * (HEAD**-0.5))
                total = jnp.sum(scores, axis=0, keepdims=True)
                for side, head in enumerate(heads_here):
                    lanes_at = slice(side * step_rows, (side + 1) * step_rows)
                    inner_den[head : head + 1, here] = total[:, lanes_at]
                    inner_top[head : head + 1, here] = row_top[:, lanes_at]
                score_high, score_low = two_parts(scores)
                values = mv_turned[lane_group, :stop]
                numerator = dot(values, score_high) + dot(values, score_low)
                inner_ref[lane_group, here] = jnp.where(
                    upper_half, numerator[:, :step_rows], numerator[:, step_rows:]
                )

    def advance(memory, normal, stable, other):
        later_top = state_rows[other, 1:2, :]
        decay = state_rows[other, 2:3, :]
        new = jnp.maximum(decay + stable, later_top)
        former = jnp.exp(decay + stable - new)
        latter = jnp.exp(later_top - new)
        return (
            former * memory + latter * states_ref[other].astype(jnp.float32),
            former * normal + latter * state_rows[other, 0:1, :],
            new,
        )

    prefixes = ((prefix_out, prefix_in), (row_out, row_in))

    def prefix_sends():
        for index, (source, target) in enumerate(prefixes):
            yield remote(
                source, target, px_send.at[index], px_recv.at[index], "sp",
                jnp.minimum(me + across, spans - 1),
            )

    def chain():
        for step in range(1, across):
            other = lax.rem(x + step, across)
            for index, ref in enumerate((states_ref, state_rows)):
                at = ref.at[other]
                remote(
                    at, at, st_send.at[index], st_recv.at[index, other], "sp", me
                ).wait_recv()

        @pl.when(z == 0)
        def _():
            prefix_in[...] = jnp.zeros((HEAD, width), jnp.bfloat16)
            row_in[...] = jnp.zeros((8, width), jnp.float32)

        @pl.when(z > 0)
        def _():
            for copy in prefix_sends():
                copy.wait_recv()

        carry = (prefix_in[...].astype(jnp.float32), row_in[0:1, :], row_in[1:2, :])
        for other in range(across):

            @pl.when(x == other)
            def _():
                enter_ref[:HEAD, :] = carry[0]
                enter_ref[HEAD : HEAD + 1, :] = carry[1]
                enter_ref[HEAD + 1 : HEAD + 2, :] = carry[2]

            carry = advance(*carry, other)

        @pl.when(z < depth - 1)
        def _():
            prefix_out[...] = carry[0].astype(jnp.bfloat16)
            row_out[0:1, :] = carry[1]
            row_out[1:2, :] = carry[2]
            row_out[2:8, :] = jnp.zeros((6, width), jnp.float32)
            for copy in prefix_sends():
                copy.start()

    top_ref[...] = jnp.full(top_ref.shape, NEGATIVE, jnp.float32)
    acc_ref[...] = jnp.zeros(acc_ref.shape, jnp.float32)
    units = spans // 2
    half_rows = rows // 2

    def run(steps):
        def score(step):
            slot, wave, place, diagonal = step
            if not diagonal:
                return dot(kv_all[place], qt_ref[slot, wave])
            visible = (wave + 1) * half_rows
            scores = dot(kv_all[place, :visible], qt_ref[slot, wave])
            key_index = lax.broadcasted_iota(jnp.int32, scores.shape, 0)
            query_index = lax.broadcasted_iota(jnp.int32, scores.shape, 1)
            query_index = jnp.where(query_index >= half_rows, query_index - half_rows, query_index)
            return jnp.where(key_index <= query_index + wave * half_rows, scores, NEGATIVE)

        def soften(step, scores):
            slot, wave, place, diagonal = step
            old_top = top_ref[slot, wave]
            top = jnp.maximum(jnp.max(scores, axis=0, keepdims=True), old_top)
            top_ref[slot, wave] = top
            return jnp.exp2(old_top - top), jnp.exp2(scores - top).astype(jnp.bfloat16)

        def gather_up(step, shrink, weights):
            slot, wave, place, diagonal = step
            sums = dot(vt_ref[place, :, : weights.shape[0]], weights)
            acc_ref[slot, wave] = acc_ref[slot, wave] * shrink + sums

        count = len(steps)
        scores = [score(step) for step in steps[:2]]
        held = None
        for index, step in enumerate(steps):
            if index + 2 < count:
                scores.append(score(steps[index + 2]))
            if held is not None:
                gather_up(steps[index - 1], *held)
            held = soften(step, scores[index])
        gather_up(steps[-1], *held)

    def visit_unit(rank):
        return near_first(me // 2, units, rank)

    def arrive(origin):
        @pl.when((origin != me) & (lax.rem(origin, parts) != my_part))
        def _():
            at = kv_all.at[origin]
            remote(at, at, fwd_send, cross_recv.at[origin], "sp", me).wait_recv()

        turned = kv_all[origin].T
        vt_ref[origin, :HEAD, :] = turned[HEAD:, :]
        vt_ref[origin, HEAD:, :] = jnp.ones((VALUE_ROWS - HEAD, rows), jnp.bfloat16)

        @pl.when(owner_of(origin) == my_part)
        def _():
            slot = origin // parts

            @pl.when(origin != me)
            def _():
                at = q_all.at[slot]
                remote(at, at, q_send, q_recv.at[slot], "sp", me).wait_recv()

            for chunk in range(chunks):
                wave = chunk * span // half_rows
                start = chunk * span - wave * half_rows
                low_rows = q_all[slot, packed_of(chunk)].astype(jnp.float32)
                high_rows = pltpu.roll(low_rows, HEAD, 1)
                for half in range(2):
                    chosen = (lanes // DD) == half
                    for side, values in enumerate((low_rows, high_rows)):
                        qn_ref[
                            wave, pl.ds(half * half_rows + start + side * packed, packed)
                        ] = jnp.where(chosen, values, 0.0).astype(jnp.bfloat16)
            for wave in range(2):
                qt_ref[slot, wave] = qn_ref[wave].T

    def mine(unit):
        return [owner_of(2 * unit + side) == my_part for side in range(2)]

    def within(unit, waves):
        chosen = mine(unit)

        @pl.when(chosen[0])
        def _():
            slot = 2 * unit // parts
            run([(slot, wave, 2 * unit, True) for wave in waves])

        @pl.when(chosen[1])
        def _():
            slot = (2 * unit + 1) // parts
            run(
                [(slot, wave, 2 * unit, False) for wave in waves]
                + [(slot, wave, 2 * unit + 1, True) for wave in waves]
            )

    def across_units(unit, other, waves):
        query = jnp.maximum(unit, other)
        key = jnp.minimum(unit, other)

        def both(slot):
            run([(slot, wave, 2 * key + side, False) for side in range(2) for wave in waves])

        if parts == 2:
            both(query)
        else:
            chosen = mine(query)
            for side in range(2):
                pl.when(chosen[side])(functools.partial(both, (2 * query + side) // parts))

    def settle(unit):
        for side in range(2):
            arrive(2 * unit + side)

    def visit(rank, unused):
        unit = visit_unit(rank)
        settle(unit)
        pl.when(rank == 1)(lambda: forward("second"))
        pl.when((z > 0) & (rank == z + 1))(chain)
        within(unit, (0, 1))

        def earlier(other_rank, unused):
            across_units(unit, visit_unit(other_rank), (0, 1))
            return unused

        lax.fori_loop(0, rank, earlier, 0)
        pl.when(rank == 1)(lambda: forward("seconded"))
        return unused

    eye = lax.broadcasted_iota(jnp.int32, (HEAD, HEAD), 0) == lax.broadcasted_iota(
        jnp.int32, (HEAD, HEAD), 1
    )
    head_gain = jnp.sum(jnp.where(eye, head_gain_ref[...], 0.0), axis=1, keepdims=True)
    head_lanes = lax.broadcasted_iota(jnp.int32, lambda_ref.shape, 1)
    factor_second = jnp.sum(
        jnp.where(head_lanes == my_head, lambda_ref[...], 0.0), axis=1, keepdims=True
    )

    def span_of(slot):
        return slot * parts + (my_part if slot % 2 == 0 else parts - 1 - my_part)

    def att_place(wave):
        return attended_ref.at[wave, pl.ds(pl.multiple_of(my_head * HEAD, HEAD), HEAD)]

    def att_copy(slot, wave):
        return remote(
            att_out.at[slot, wave], att_place(wave), att_send,
            att_recv.at[my_head, wave], "sp", span_of(slot),
        )

    def finish(wave):
        for slot in range(heads):
            sums = acc_ref[slot, wave]
            maps = sums[:HEAD] / sums[HEAD : HEAD + 1]
            second = pltpu.roll(maps, half_rows, 1)[:, :half_rows]
            difference = maps[:, :half_rows] - factor_second * second
            mean = jnp.mean(difference * difference, axis=0, keepdims=True)
            att_out[slot, wave] = (
                difference * lax.rsqrt(mean + EPSILON) * head_gain
            ).astype(jnp.bfloat16)

            @pl.when(span_of(slot) == me)
            def _():
                att_place(wave)[...] = att_out[slot, wave]

            @pl.when(span_of(slot) != me)
            def _():
                att_copy(slot, wave).start()

    def recall():
        memory_in = enter_ref[:HEAD, :]
        normal_in = enter_ref[HEAD : HEAD + 1, :]
        head_of_lane = lax.broadcasted_iota(jnp.int32, (16, width), 1) // HEAD
        head_of_row = lax.broadcasted_iota(jnp.int32, (16, width), 0)
        blocks = jnp.concatenate(
            [jnp.where(head_mask(width, head), memory_in, 0.0) for head in range(heads)]
            + [jnp.where(head_of_lane == head_of_row, normal_in, 0.0)],
            axis=0,
        )
        high, low = two_parts(blocks)
        carried = dot(high, mq_turned[...]) + dot(low, mq_turned[...])
        head_rows = lax.broadcasted_iota(jnp.int32, (heads, 1), 0)
        stable = jnp.zeros((heads, 1), jnp.float32)
        for head in range(heads):
            stable = jnp.where(
                head_rows == head,
                enter_ref[HEAD + 1 : HEAD + 2, head * HEAD : head * HEAD + 1],
                stable,
            )
        carried_log = cumulative_ref[:heads] + stable
        own_top = inner_top[:heads]
        row_top = jnp.maximum(carried_log, own_top)
        inside = jnp.exp(own_top - row_top)
        outside = jnp.exp(carried_log - row_top)
        denominator = inside * inner_den[:heads] + outside * carried[width : width + heads]
        denominator = jnp.maximum(jnp.abs(denominator), 1.0)
        inside = inside / denominator
        outside = outside / denominator
        for head in range(heads):
            at = slice(head * HEAD, (head + 1) * HEAD)
            one = slice(head, head + 1)
            memory_ref[at, :] = (inside[one] * inner_ref[at, :] + outside[one] * carried[at]).astype(
                jnp.bfloat16
            )
        loads[6].wait()
        loads[7].wait()
        partial_ref[...] = dot(memory_ref[...], som[...], ((0,), (0,)))

    settle(me // 2)
    within(me // 2, (0, 1))
    forward("first")
    inner()
    forward("inner")
    pl.when(z == 0)(chain)
    lax.fori_loop(1, units - 1, visit, 0)
    last = visit_unit(units - 1)
    settle(last)
    for wave in range(2):
        within(last, (wave,))
        if parts == 2:
            steps = []
            for rank in range(units - 1):
                other = visit_unit(rank)
                query = jnp.maximum(last, other)
                key = jnp.minimum(last, other)
                steps.append([(query, wave, 2 * key + side, False) for side in range(2)])
            run([step for side in zip(*steps) for step in side])
        else:

            def earlier(rank, unused):
                across_units(last, visit_unit(rank), (wave,))
                return unused

            lax.fori_loop(0, units - 1, earlier, 0)
        finish(wave)
        if wave == 0:
            pl.when(z == units - 2)(chain)
            pl.when(z < units - 1)(recall)
    @pl.when(z >= units - 1)
    def _():
        chain()
        recall()

    out_span = rows // out_chunks
    per_wave = out_chunks // 2

    def out_rows(chunk):
        return pl.ds(chunk * out_span, out_span)

    order = list(range(1, lines)) + [0]
    swaps = {}
    lined = {}

    def pair_sum(step, chunk):
        swaps[step, chunk].wait_recv()
        mine = part_ref[
            out_rows(chunk), columns_of(lax.rem(line + step, lines) * CORES + core)
        ]
        return mine.astype(jnp.float32) + pair_in[step, out_rows(chunk), :].astype(jnp.float32)

    def pass_on(chunk):
        for step in range(1, lines):
            line_out[step, out_rows(chunk), :] = pair_sum(step, chunk).astype(jnp.bfloat16)
            copy = remote(
                line_out.at[step, out_rows(chunk)], line_in.at[step, out_rows(chunk)],
                sl_send, sl_recv.at[step - 1, chunk], "tp",
                lax.rem(line + step, lines) * CORES + core,
            )
            copy.start()
            lined[step, chunk] = copy

    for wave in range(2):
        for step in range(heads):

            @pl.when((my_owner != my_part) | (my_head != step))
            def _():
                at = attended_ref.at[wave, pl.ds(step * HEAD, HEAD)]
                remote(at, at, att_send, att_recv.at[step, wave], "sp", me).wait_recv()

        at = slice(wave * half_rows, (wave + 1) * half_rows)
        part_ref[at, :] = (
            dot(attended_ref[wave], soa[...], ((0,), (0,))) + partial_ref[at, :]
        ).astype(jnp.bfloat16)
        for chunk in range(wave * per_wave, (wave + 1) * per_wave):
            for step in order:
                target = lax.rem(line + step, lines) * CORES + (1 - core)
                copy = remote(
                    part_ref.at[out_rows(chunk), columns_of(target)],
                    pair_in.at[step, out_rows(chunk)], sp_send,
                    sp_recv.at[step, chunk], "tp", pair,
                )
                copy.start()
                swaps[step, chunk] = copy
        for chunk in range(wave * per_wave, (wave + 1) * per_wave):
            pass_on(chunk)

    def sent(ref, semaphore):
        remote(ref, ref, semaphore, semaphore, "tp", pair).wait_send()

    others = line_in.at[pl.ds(1, lines - 1)]
    sent(others, line_send)
    sent(pair_in, pair_send)
    sent(kv_out.at[pl.ds(0, heads - 1)], kv_send)
    sent(kv_all.at[pl.ds(0, heads * (parts - 1))], fwd_send)
    sent(q_out.at[pl.ds(0, heads - 1)], q_send)
    pl.when(my_owner != my_part)(lambda: sent(q_out.at[0], q_side))
    sent(states_ref.at[pl.ds(0, across - 1)], st_send.at[0])
    sent(state_rows.at[pl.ds(0, across - 1)], st_send.at[1])

    @pl.when(z < depth - 1)
    def _():
        for copy in prefix_sends():
            copy.wait_send()

    pl.when(my_owner == my_part)(lambda: sent(att_out.at[pl.ds(0, heads - 1)], att_send))
    pl.when(my_owner != my_part)(lambda: sent(att_out, att_send))
    for chunk in range(out_chunks):
        total = pair_sum(0, chunk)
        for step in range(1, lines):
            lined[step, chunk].wait_recv()
            total = total + line_in[step, out_rows(chunk), :].astype(jnp.float32)
        total_ref[out_rows(chunk), :] = total.astype(jnp.bfloat16)
        copy = pltpu.make_async_copy(
            total_ref.at[out_rows(chunk)], out_ref.at[out_rows(chunk)], out_sem
        )
        copy.start()
    pltpu.make_async_copy(total_ref, out_ref, out_sem).wait()
    sent(pair_in, sp_send)
    sent(others, sl_send)


def per_device(tp_size, depth, across, inputs, norm_gain, query_weight, key_weight, value_weight,
               memory_query_weight, memory_key_weight, memory_value_weight, input_gate_weight,
               forget_gate_weight, forget_bias, decay_shift, lambdas, head_gain,
               out_weight_attention, out_weight_memory):
    rows, columns = inputs.shape
    features = norm_gain.shape[0]
    width = query_weight.shape[1]
    heads = width // HEAD
    lines = tp_size // CORES
    spans = depth * across
    parts = spans // heads
    chunks = 4
    out_chunks = 4
    dma = pltpu.SemaphoreType.DMA


    hbm = pl.BlockSpec(memory_space=pl.ANY)
    bf16 = lambda *shape: pltpu.VMEM(shape, jnp.bfloat16)
    f32 = lambda *shape: pltpu.VMEM(shape, jnp.float32)
    return pl.pallas_call(
        functools.partial(layer_kernel, tp_size, depth, across, chunks, out_chunks),
        out_shape=jax.ShapeDtypeStruct((rows, columns), jnp.bfloat16),
        in_specs=[VMEM] * 2 + [hbm] * 6 + [VMEM] * 6 + [hbm] * 2,
        out_specs=hbm,
        scratch_shapes=[bf16(features, 6 * width)]
        + [bf16(width, features)] * 2
        + [
            bf16(rows, features), bf16(rows, features), f32(rows, 1), f32(rows, 6 * width),
            f32(rows, 128), f32(rows, 128),
            bf16(heads, rows, 128), bf16(heads, rows // 2, 128), bf16(spans, rows, 128),
            bf16(heads, rows // 2, 128), bf16(spans, VALUE_ROWS, rows),
            bf16(2, rows, 128), bf16(heads, 2, 128, rows), f32(heads, 2, 1, rows),
            f32(heads, 2, VALUE_ROWS, rows), bf16(heads, 2, HEAD, rows // 2),
            bf16(2, width, rows // 2),
            bf16(rows, width), bf16(rows, width), bf16(rows, width), bf16(width, rows),
            bf16(width, rows), f32(rows, 128),
            bf16(across, HEAD, width), f32(across, 8, width), bf16(HEAD, width), f32(8, width),
            bf16(HEAD, width), f32(8, width), f32(STATE_ROWS, width),
            f32(width, rows), f32(8, rows), f32(8, rows), f32(8, rows), f32(rows, 128),
            bf16(width, rows),
            f32(rows, features), bf16(rows, features), bf16(lines, rows, columns),
            bf16(lines, rows, columns),
            bf16(lines, rows, columns), bf16(rows, columns),
            dma(()), dma((8,)), dma(()), dma((lines - 1, chunks)), dma(()),
            dma((lines - 1, chunks)), dma(()),
            dma(()), dma(()), dma((heads, chunks)), dma((spans,)), dma(()), dma(()),
            dma((heads,)), dma(()), dma((heads, 2)),
            dma((2,)), dma((2, across)), dma((2,)), dma((2,)), dma(()), dma((lines, out_chunks)),
            dma(()),
            dma((lines - 1, out_chunks)),
        ],
        compiler_params=pltpu.CompilerParams(
            vmem_limit_bytes=VMEM_LIMIT, collective_id=0, has_side_effects=True
        ),
        name="layer",
    )(
        inputs, norm_gain[None, :], query_weight, key_weight, value_weight,
        memory_query_weight, memory_key_weight, memory_value_weight, input_gate_weight.T,
        forget_gate_weight.T, forget_bias[None, :], decay_shift.T, lambdas[None, :],
        head_gain[None, :], out_weight_attention, out_weight_memory,
    )


def columns_across(mesh):
    spans = mesh.shape["sp"]
    try:
        places = {device.coords[0] for device in mesh.devices.flat}
        across = len(places)
    except AttributeError:
        across = 2
    return across if spans % across == 0 else 1


def solution(mesh):
    across = columns_across(mesh)
    in_specs = (
        P("sp", "tp"),
        P(),
        P(None, "tp"),
        P(None, "tp"),
        P(None, "tp"),
        P(None, "tp"),
        P(None, "tp"),
        P(None, "tp"),
        P(None, "tp"),
        P(None, "tp"),
        P("tp"),
        P("sp", "tp"),
        P("tp"),
        P(),
        P("tp", None),
        P("tp", None),
    )
    return jax.shard_map(
        functools.partial(
            per_device, mesh.shape["tp"], mesh.shape["sp"] // across, across
        ),
        mesh=mesh,
        in_specs=in_specs,
        out_specs=P("sp", "tp"),
        check_vma=False,
    )
```

```python
import functools

import jax
import jax.numpy as jnp
from jax import lax
from jax.experimental import pallas as pl
from jax.experimental.pallas import tpu as pltpu
from jax.sharding import PartitionSpec as P

HEAD = 64
DD = 32
EPSILON = 1e-06
ROTARY_BASE = 10000.0
NEGATIVE = -1e30
LOG2E = 1.4426950408889634
CORES = 2
STATE_ROWS = HEAD + 8
VALUE_ROWS = HEAD + 16
VMEM = pl.BlockSpec(memory_space=pltpu.VMEM)
MESH = pl.DeviceIdType.MESH
VMEM_LIMIT = 60 * 1024 * 1024


def signal(semaphore, axis, place):
    pl.semaphore_signal(semaphore, inc=1, device_id={axis: place}, device_id_type=MESH)


def remote(source, target, send_sem, recv_sem, axis, place):
    return pltpu.make_async_remote_copy(
        src_ref=source,
        dst_ref=target,
        send_sem=send_sem,
        recv_sem=recv_sem,
        device_id={axis: place},
        device_id_type=MESH,
    )


def head_mask(width, head):
    lanes = lax.broadcasted_iota(jnp.int32, (1, width), 1)
    return (lanes // HEAD) == head


def two_parts(floats):
    high = floats.astype(jnp.bfloat16)
    return high, (floats - high.astype(jnp.float32)).astype(jnp.bfloat16)


def dot(a, b, dims=((1,), (0,))):
    return lax.dot_general(a, b, (dims, ((), ())), preferred_element_type=jnp.float32)


def near_first(place, count, rank):
    both = jnp.minimum(place, count - 1 - place)
    half = (rank + 1) // 2
    low = place < count - 1 - place
    below = jnp.where(low, rank % 2 == 1, rank % 2 == 0)
    alternating = jnp.where(below, place - half, place + half)
    one_sided = jnp.where(low, rank, count - 1 - rank)
    return jnp.where(rank <= 2 * both, alternating, one_sided)


def layer_kernel(
    size, depth, across, chunks, out_chunks,
    shard_ref, gain_ref, wq, wk, wv, wmq, wmk, wmv, wi, wf, bias_ref, shift_ref,
    lambda_ref, head_gain_ref, woa, wom,
    out_ref,
    weight_ref, soa, som, x_ref, scaled_ref, square_ref, sum_ref, cosine_ref, sine_ref,
    kv_out, q_out, kv_all, q_all, vt_ref, qn_ref, qt_ref, top_ref, acc_ref, att_out, attended_ref,
    mq_ref, mk_ref, mv_ref, mq_turned, mv_turned, pre_ref, states_ref, state_rows, prefix_in, row_in, prefix_out, row_out,
    enter_ref,
    inner_ref, inner_den, inner_top, cumulative_ref, offset_ref, memory_ref,
    partial_ref, part_ref, pair_in, line_out, line_in, total_ref,
    out_sem, load_sems, line_send, line_recv, pair_send, pair_recv, own_recv,
    kv_send, fwd_send, land_recv, cross_recv, q_send, q_side, q_recv, att_send, att_recv,
    st_send, st_recv, px_send, px_recv, sp_send, sp_recv, sl_send, sl_recv,
):
    rows, columns = shard_ref.shape
    features = x_ref.shape[1]
    width = mq_ref.shape[1]
    heads = width // HEAD
    groups = width // 128
    lines = size // CORES
    spans = depth * across
    parts = spans // heads
    span = rows // chunks
    packed = span // 2

    tp = lax.axis_index("tp")
    core = lax.rem(tp, CORES)
    line = tp // CORES
    pair = line * CORES + (1 - core)
    me = lax.axis_index("sp")
    z = me // across
    x = lax.rem(me, across)
    my_head = me // parts
    my_part = lax.rem(me, parts)

    def owner_of(place):
        place_part = lax.rem(place, parts)
        return jnp.where((place // parts) % 2 == 0, place_part, parts - 1 - place_part)

    loads = []
    for index, source in enumerate((wk, wv, wq, wmk, wmv, wmq)):
        loads.append(
            pltpu.make_async_copy(
                source, weight_ref.at[:, pl.ds(index * width, width)], load_sems.at[index]
            )
        )
    loads.append(pltpu.make_async_copy(woa, soa, load_sems.at[6]))
    loads.append(pltpu.make_async_copy(wom, som, load_sems.at[7]))
    for copy in loads:
        copy.start()

    barrier = pltpu.get_barrier_semaphore()
    signal(barrier, "tp", pair)
    for step in range(1, lines):
        signal(barrier, "tp", lax.rem(line + step, lines) * CORES + core)
    for step in range(1, spans):
        signal(barrier, "sp", lax.rem(me + step, spans))

    position = (me * rows + lax.broadcasted_iota(jnp.int32, (1, rows), 1)).astype(jnp.float32)
    middle = DD // 2
    turn = lax.broadcasted_iota(jnp.int32, (middle, 1), 0)
    rates = jnp.zeros((middle, 1), jnp.float32)
    for index in range(middle):
        rates = jnp.where(turn == index, ROTARY_BASE ** (-index / middle), rates)
    angles = rates * position
    cosines = jnp.cos(angles)
    sines = jnp.sin(angles)
    cosine_ref[...] = jnp.concatenate([cosines] * (128 * 2 // DD), axis=0).T
    sine_ref[...] = jnp.concatenate([-sines, sines] * (128 // DD), axis=0).T
    lanes = lax.broadcasted_iota(jnp.int32, (1, 128), 1)
    former = lax.rem(lanes, DD) < DD // 2
    low_lanes = lanes < HEAD

    def columns_of(owner):
        return pl.ds(pl.multiple_of(owner * columns, 128), columns)

    def rows_of(chunk):
        return pl.ds(chunk * span, span)

    def place(owner, chunk):
        return x_ref.at[rows_of(chunk), columns_of(owner)]

    pl.semaphore_wait(barrier, lines + spans - 1)

    pairs = {}
    for chunk in range(chunks):
        for step in range(1, lines):
            copy = remote(
                shard_ref.at[rows_of(chunk)], place(tp, chunk), line_send,
                line_recv.at[step - 1, chunk], "tp", lax.rem(line + step, lines) * CORES + core,
            )
            copy.start()
    own_pair = remote(shard_ref, x_ref.at[:, columns_of(tp)], pair_send, own_recv, "tp", pair)
    own_pair.start()

    def take(values, at_rows, owner):
        floats = values.astype(jnp.float32)
        scaled_ref[at_rows, columns_of(owner)] = (floats * gain_ref[:, columns_of(owner)]).astype(
            jnp.bfloat16
        )
        return jnp.sum(floats * floats, axis=1, keepdims=True)

    everywhere = pl.ds(0, rows)
    squares = take(shard_ref[...], everywhere, tp)
    own_pair.wait_recv()
    square_ref[...] = squares + take(x_ref[:, columns_of(pair)], everywhere, pair)

    def line_columns(owner_line):
        return pl.ds(pl.multiple_of(owner_line * CORES * columns, 128), CORES * columns)

    couples = [slice(index * width, (index + 2) * width) for index in (0, 2, 4)]
    for index, couple in enumerate(couples):
        loads[2 * index].wait()
        loads[2 * index + 1].wait()
        sum_ref[:, couple] = dot(
            scaled_ref[:, line_columns(line)], weight_ref[line_columns(line), couple]
        )

    blank = jnp.zeros((8 - heads, features), jnp.float32)
    gate_weights = jnp.concatenate(
        [wi[...].astype(jnp.float32), blank, wf[...].astype(jnp.float32), blank], axis=0
    ).astype(jnp.bfloat16)
    gate_bias = jnp.concatenate(
        [jnp.zeros((1, 8), jnp.float32), bias_ref[...], jnp.zeros((1, 8 - heads), jnp.float32)],
        axis=1,
    )
    factor = (DD**-0.5) * LOG2E

    def rotated(wide, cosine, sine):
        partner = jnp.where(former, pltpu.roll(wide, 128 - DD // 2, 1), pltpu.roll(wide, DD // 2, 1))
        return wide * cosine + partner * sine

    def kv_sends(chunk):
        for rank in range(1, heads):
            head = near_first(my_head, heads, rank)
            yield remote(
                kv_out.at[head, rows_of(chunk)], kv_all.at[me, rows_of(chunk)],
                kv_send, land_recv.at[my_head, chunk], "sp", head * parts + my_part,
            )

    def forwards(source, origin, chunk):
        for step in range(1, parts):
            yield remote(
                source, kv_all.at[origin, rows_of(chunk)], fwd_send, cross_recv.at[origin], "sp",
                my_head * parts + lax.rem(my_part + step, parts),
            )

    points = {
        (1, 0): "chunk1", (1, 1): "chunk2", (1, 2): "projected", (2, 0): "projected",
        (1, 3): "state", (3, 0): "first", (2, 1): "first", (3, 1): "inner",
        (2, 2): "inner", (2, 3): "second", (3, 2): "seconded", (3, 3): "seconded",
    }

    def landed(rank):
        return near_first(my_head, heads, rank) * parts + my_part

    def forward(point, index=""):
        for rank in range(1, heads):
            for chunk in range(chunks):
                if points.get((rank, chunk), "inner") == f"{point}{index}":
                    origin = landed(rank)
                    at = kv_all.at[origin, rows_of(chunk)]
                    remote(
                        at, at, kv_send, land_recv.at[origin // parts, chunk], "sp", me
                    ).wait_recv()
                    for copy in forwards(at, origin, chunk):
                        copy.start()

    packed_of = lambda chunk: pl.ds(chunk * packed, packed)
    my_slot = me // parts
    my_owner = owner_of(me)

    def q_sends(chunk):
        for rank in range(1, heads):
            head = near_first(my_head, heads, rank)
            yield remote(
                q_out.at[head, packed_of(chunk)], q_all.at[my_slot, packed_of(chunk)],
                q_send, q_recv.at[my_slot], "sp", head * parts + my_owner,
            )

    def q_aside(chunk):
        return remote(
            q_out.at[my_head, packed_of(chunk)], q_all.at[my_slot, packed_of(chunk)],
            q_side, q_recv.at[my_slot], "sp", my_head * parts + my_owner,
        )

    def pull(chunk):
        for step in range(1, lines):
            source = lax.rem(line + lines - step, lines) * CORES + core
            at = place(source, chunk)
            remote(
                at, at, line_send, line_recv.at[step - 1, chunk], "tp", pair
            ).wait_recv()
            copy = remote(at, at, pair_send, pair_recv.at[step - 1, chunk], "tp", pair)
            copy.start()
            pairs[step, chunk] = copy

    pull(0)
    for chunk in range(chunks):
        at = rows_of(chunk)
        squares = square_ref[at]
        for step in range(1, lines):
            source = lax.rem(line + lines - step, lines) * CORES + core
            squares = squares + take(x_ref[at, columns_of(source)], at, source)
        for step in range(1, lines):
            source = lax.rem(line + lines - step, lines) * CORES + 1 - core
            pairs[step, chunk].wait_recv()
            squares = squares + take(x_ref[at, columns_of(source)], at, source)
        inverse = lax.rsqrt(squares / features + EPSILON)

        def products(index):
            total = sum_ref[at, couples[index]]
            for step in range(1, lines):
                other = line_columns(lax.rem(line + step, lines))
                total = total + dot(scaled_ref[at, other], weight_ref[other, couples[index]])
            total = (total * inverse).astype(jnp.bfloat16).astype(jnp.float32)
            return total[:, :width], total[:, width:]

        cosine = cosine_ref[at]
        sine = sine_ref[at]
        keys, values = products(0)
        for group in range(groups):
            lane_group = slice(group * 128, group * 128 + 128)
            key = rotated(keys[:, lane_group], cosine, sine)
            value = values[:, lane_group]
            kv_out[2 * group, at] = jnp.where(low_lanes, key, pltpu.roll(value, HEAD, 1)).astype(
                jnp.bfloat16
            )
            kv_out[2 * group + 1, at] = jnp.where(
                low_lanes, pltpu.roll(key, HEAD, 1), value
            ).astype(jnp.bfloat16)
        for copy in kv_sends(chunk):
            copy.start()
        for copy in forwards(kv_out.at[my_head, at], me, chunk):
            copy.start()
        kv_all[me, at] = kv_out[my_head, at]

        queries, memory_keys = products(1)
        for group in range(groups):
            query = rotated(queries[:, group * 128 : group * 128 + 128], cosine, sine) * factor
            top, bottom = query[:packed], query[packed:]
            q_out[2 * group, packed_of(chunk)] = jnp.where(
                low_lanes, top, pltpu.roll(bottom, HEAD, 1)
            ).astype(jnp.bfloat16)
            q_out[2 * group + 1, packed_of(chunk)] = jnp.where(
                low_lanes, pltpu.roll(top, HEAD, 1), bottom
            ).astype(jnp.bfloat16)
        for copy in q_sends(chunk):
            copy.start()

        @pl.when(my_owner == my_part)
        def _():
            q_all[my_slot, packed_of(chunk)] = q_out[my_head, packed_of(chunk)]

        @pl.when(my_owner != my_part)
        def _():
            q_aside(chunk).start()

        mk_ref[at] = memory_keys.astype(jnp.bfloat16)
        if chunk + 1 < chunks:
            pull(chunk + 1)
        memory_values, memory_queries = products(2)
        mv_ref[at] = memory_values.astype(jnp.bfloat16)
        mq_ref[at] = memory_queries.astype(jnp.bfloat16)
        pre_ref[at, :16] = dot(scaled_ref[at, :], gate_weights, ((1,), (1,))) * inverse + gate_bias
        if chunk < chunks - 1:
            forward("chunk", chunk)

    forward("projected")

    turned = pre_ref[...].T
    gate = turned[:8]
    pre = turned[8:16]
    shift = jnp.concatenate([shift_ref[...], jnp.zeros((8 - heads, rows), jnp.float32)], axis=0)
    forget = jnp.minimum(pre, 0.0) - jnp.log1p(jnp.exp(-jnp.abs(pre))) + shift
    first, rest = (part.astype(jnp.float32) for part in two_parts(forget))
    pieces = jnp.concatenate([first, rest, forget - first - rest], axis=0).astype(jnp.bfloat16)
    row_index = lax.broadcasted_iota(jnp.int32, (rows, rows), 0)
    column_index = lax.broadcasted_iota(jnp.int32, (rows, rows), 1)
    sums = dot(pieces, (row_index <= column_index).astype(jnp.bfloat16))
    cumulative = sums[:8] + (sums[8:16] + sums[16:24])
    cumulative_ref[...] = cumulative
    offset = gate - cumulative
    offset_ref[...] = jnp.concatenate([offset, jnp.zeros((120, rows), jnp.float32)], axis=0).T
    end = cumulative[:, rows - 1 : rows]
    toward = end + offset
    top = jnp.max(toward, axis=1, keepdims=True)
    end_weights = jnp.exp(toward - top) * (HEAD**-0.5)
    mv_turned[...] = mv_ref[...].T
    mq_turned[...] = mq_ref[...].T
    weighted = jnp.concatenate(
        [
            mv_turned[head * HEAD : (head + 1) * HEAD, :].astype(jnp.float32)
            * end_weights[head : head + 1, :]
            for head in range(heads)
        ]
        + [end_weights, end_weights],
        axis=0,
    )
    high, low = two_parts(weighted)
    whole = dot(high, mk_ref[...]) + dot(low, mk_ref[...])
    memory = jnp.zeros((HEAD, width), jnp.float32)
    normal = jnp.zeros((1, width), jnp.float32)
    top_row = jnp.zeros((1, width), jnp.float32)
    end_row = jnp.zeros((1, width), jnp.float32)
    for head in range(heads):
        chosen = head_mask(width, head)
        at_head = slice(head, head + 1)
        memory = jnp.where(chosen, whole[head * HEAD : (head + 1) * HEAD, :], memory)
        normal = jnp.where(chosen, whole[width + head : width + head + 1, :], normal)
        top_row = jnp.where(chosen, top[at_head], top_row)
        end_row = jnp.where(chosen, end[at_head], end_row)
    states_ref[x] = memory.astype(jnp.bfloat16)
    state_rows[x] = jnp.concatenate(
        [normal, top_row, end_row, jnp.zeros((5, width), jnp.float32)], axis=0
    )

    def state_sends():
        for step in range(1, across):
            for index, ref in enumerate((states_ref, state_rows)):
                yield remote(
                    ref.at[x], ref.at[x], st_send.at[index], st_recv.at[index, x], "sp",
                    z * across + lax.rem(x + step, across),
                )

    forward("state")
    for copy in state_sends():
        copy.start()

    def inner():
        step_rows = 128
        for group in range(groups):
            lane_group = slice(group * 128, (group + 1) * 128)
            heads_here = (2 * group, 2 * group + 1)
            upper_half = lax.broadcasted_iota(jnp.int32, (128, step_rows), 0) < HEAD
            for start in range(0, rows, step_rows):
                stop = start + step_rows
                here = slice(start, stop)
                queries = mq_turned[lane_group, here].astype(jnp.float32)
                both = jnp.concatenate(
                    [jnp.where(upper_half, queries, 0.0), jnp.where(upper_half, 0.0, queries)], axis=1
                ).astype(jnp.bfloat16)
                scores = dot(mk_ref[:stop, lane_group], both)
                ahead = jnp.concatenate(
                    [cumulative_ref[head : head + 1, here] for head in heads_here], axis=1
                )
                behind = jnp.concatenate(
                    [
                        jnp.broadcast_to(offset_ref[:stop, head : head + 1], (stop, step_rows))
                        for head in heads_here
                    ],
                    axis=1,
                )
                key_index = lax.broadcasted_iota(jnp.int32, scores.shape, 0)
                query_index = lax.broadcasted_iota(jnp.int32, scores.shape, 1) % step_rows
                gaps = jnp.where(key_index <= query_index + start, ahead + behind, NEGATIVE)
                row_top = jnp.max(gaps, axis=0, keepdims=True)
                scores = jnp.exp(gaps - row_top) * (scores * (HEAD**-0.5))
                total = jnp.sum(scores, axis=0, keepdims=True)
                for side, head in enumerate(heads_here):
                    lanes_at = slice(side * step_rows, (side + 1) * step_rows)
                    inner_den[head : head + 1, here] = total[:, lanes_at]
                    inner_top[head : head + 1, here] = row_top[:, lanes_at]
                score_high, score_low = two_parts(scores)
                values = mv_turned[lane_group, :stop]
                numerator = dot(values, score_high) + dot(values, score_low)
                inner_ref[lane_group, here] = jnp.where(
                    upper_half, numerator[:, :step_rows], numerator[:, step_rows:]
                )

    def advance(memory, normal, stable, other):
        later_top = state_rows[other, 1:2, :]
        decay = state_rows[other, 2:3, :]
        new = jnp.maximum(decay + stable, later_top)
        former = jnp.exp(decay + stable - new)
        latter = jnp.exp(later_top - new)
        return (
            former * memory + latter * states_ref[other].astype(jnp.float32),
            former * normal + latter * state_rows[other, 0:1, :],
            new,
        )

    prefixes = ((prefix_out, prefix_in), (row_out, row_in))

    def prefix_sends():
        for index, (source, target) in enumerate(prefixes):
            yield remote(
                source, target, px_send.at[index], px_recv.at[index], "sp",
                jnp.minimum(me + across, spans - 1),
            )

    def chain():
        for step in range(1, across):
            other = lax.rem(x + step, across)
            for index, ref in enumerate((states_ref, state_rows)):
                at = ref.at[other]
                remote(
                    at, at, st_send.at[index], st_recv.at[index, other], "sp", me
                ).wait_recv()

        @pl.when(z == 0)
        def _():
            prefix_in[...] = jnp.zeros((HEAD, width), jnp.bfloat16)
            row_in[...] = jnp.zeros((8, width), jnp.float32)

        @pl.when(z > 0)
        def _():
            for copy in prefix_sends():
                copy.wait_recv()

        carry = (prefix_in[...].astype(jnp.float32), row_in[0:1, :], row_in[1:2, :])
        for other in range(across):

            @pl.when(x == other)
            def _():
                enter_ref[:HEAD, :] = carry[0]
                enter_ref[HEAD : HEAD + 1, :] = carry[1]
                enter_ref[HEAD + 1 : HEAD + 2, :] = carry[2]

            carry = advance(*carry, other)

        @pl.when(z < depth - 1)
        def _():
            prefix_out[...] = carry[0].astype(jnp.bfloat16)
            row_out[0:1, :] = carry[1]
            row_out[1:2, :] = carry[2]
            row_out[2:8, :] = jnp.zeros((6, width), jnp.float32)
            for copy in prefix_sends():
                copy.start()

    top_ref[...] = jnp.full(top_ref.shape, NEGATIVE, jnp.float32)
    acc_ref[...] = jnp.zeros(acc_ref.shape, jnp.float32)
    units = spans // 2
    half_rows = rows // 2

    def run(steps):
        def score(step):
            slot, wave, place, diagonal = step
            if not diagonal:
                return dot(kv_all[place], qt_ref[slot, wave])
            visible = (wave + 1) * half_rows
            scores = dot(kv_all[place, :visible], qt_ref[slot, wave])
            key_index = lax.broadcasted_iota(jnp.int32, scores.shape, 0)
            query_index = lax.broadcasted_iota(jnp.int32, scores.shape, 1)
            query_index = jnp.where(query_index >= half_rows, query_index - half_rows, query_index)
            return jnp.where(key_index <= query_index + wave * half_rows, scores, NEGATIVE)

        def soften(step, scores):
            slot, wave, place, diagonal = step
            old_top = top_ref[slot, wave]
            top = jnp.maximum(jnp.max(scores, axis=0, keepdims=True), old_top)
            top_ref[slot, wave] = top
            return jnp.exp2(old_top - top), jnp.exp2(scores - top).astype(jnp.bfloat16)

        def gather_up(step, shrink, weights):
            slot, wave, place, diagonal = step
            sums = dot(vt_ref[place, :, : weights.shape[0]], weights)
            acc_ref[slot, wave] = acc_ref[slot, wave] * shrink + sums

        count = len(steps)
        scores = [score(step) for step in steps[:2]]
        held = None
        for index, step in enumerate(steps):
            if index + 2 < count:
                scores.append(score(steps[index + 2]))
            if held is not None:
                gather_up(steps[index - 1], *held)
            held = soften(step, scores[index])
        gather_up(steps[-1], *held)

    def visit_unit(rank):
        return near_first(me // 2, units, rank)

    def arrive(origin):
        @pl.when((origin != me) & (lax.rem(origin, parts) != my_part))
        def _():
            at = kv_all.at[origin]
            remote(at, at, fwd_send, cross_recv.at[origin], "sp", me).wait_recv()

        turned = kv_all[origin].T
        vt_ref[origin, :HEAD, :] = turned[HEAD:, :]
        vt_ref[origin, HEAD:, :] = jnp.ones((VALUE_ROWS - HEAD, rows), jnp.bfloat16)

        @pl.when(owner_of(origin) == my_part)
        def _():
            slot = origin // parts

            @pl.when(origin != me)
            def _():
                at = q_all.at[slot]
                remote(at, at, q_send, q_recv.at[slot], "sp", me).wait_recv()

            for chunk in range(chunks):
                wave = chunk * span // half_rows
                start = chunk * span - wave * half_rows
                low_rows = q_all[slot, packed_of(chunk)].astype(jnp.float32)
                high_rows = pltpu.roll(low_rows, HEAD, 1)
                for half in range(2):
                    chosen = (lanes // DD) == half
                    for side, values in enumerate((low_rows, high_rows)):
                        qn_ref[
                            wave, pl.ds(half * half_rows + start + side * packed, packed)
                        ] = jnp.where(chosen, values, 0.0).astype(jnp.bfloat16)
            for wave in range(2):
                qt_ref[slot, wave] = qn_ref[wave].T

    def mine(unit):
        return [owner_of(2 * unit + side) == my_part for side in range(2)]

    def within(unit, waves):
        chosen = mine(unit)

        @pl.when(chosen[0])
        def _():
            slot = 2 * unit // parts
            run([(slot, wave, 2 * unit, True) for wave in waves])

        @pl.when(chosen[1])
        def _():
            slot = (2 * unit + 1) // parts
            run(
                [(slot, wave, 2 * unit, False) for wave in waves]
                + [(slot, wave, 2 * unit + 1, True) for wave in waves]
            )

    def across_units(unit, other, waves):
        query = jnp.maximum(unit, other)
        key = jnp.minimum(unit, other)

        def both(slot):
            run([(slot, wave, 2 * key + side, False) for side in range(2) for wave in waves])

        if parts == 2:
            both(query)
        else:
            chosen = mine(query)
            for side in range(2):
                pl.when(chosen[side])(functools.partial(both, (2 * query + side) // parts))

    def settle(unit):
        for side in range(2):
            arrive(2 * unit + side)

    def visit(rank, unused):
        unit = visit_unit(rank)
        settle(unit)
        pl.when(rank == 1)(lambda: forward("second"))
        pl.when((z > 0) & (rank == z + 1))(chain)
        within(unit, (0, 1))

        def earlier(other_rank, unused):
            across_units(unit, visit_unit(other_rank), (0, 1))
            return unused

        lax.fori_loop(0, rank, earlier, 0)
        pl.when(rank == 1)(lambda: forward("seconded"))
        return unused

    eye = lax.broadcasted_iota(jnp.int32, (HEAD, HEAD), 0) == lax.broadcasted_iota(
        jnp.int32, (HEAD, HEAD), 1
    )
    head_gain = jnp.sum(jnp.where(eye, head_gain_ref[...], 0.0), axis=1, keepdims=True)
    head_lanes = lax.broadcasted_iota(jnp.int32, lambda_ref.shape, 1)
    factor_second = jnp.sum(
        jnp.where(head_lanes == my_head, lambda_ref[...], 0.0), axis=1, keepdims=True
    )

    def span_of(slot):
        return slot * parts + (my_part if slot % 2 == 0 else parts - 1 - my_part)

    def att_place(wave):
        return attended_ref.at[wave, pl.ds(pl.multiple_of(my_head * HEAD, HEAD), HEAD)]

    def att_copy(slot, wave):
        return remote(
            att_out.at[slot, wave], att_place(wave), att_send,
            att_recv.at[my_head, wave], "sp", span_of(slot),
        )

    def finish(wave, slots):
        for slot in slots:
            sums = acc_ref[slot, wave]
            maps = sums[:HEAD] / sums[HEAD : HEAD + 1]
            second = pltpu.roll(maps, half_rows, 1)[:, :half_rows]
            difference = maps[:, :half_rows] - factor_second * second
            mean = jnp.mean(difference * difference, axis=0, keepdims=True)
            att_out[slot, wave] = (
                difference * lax.rsqrt(mean + EPSILON) * head_gain
            ).astype(jnp.bfloat16)

            @pl.when(span_of(slot) == me)
            def _():
                att_place(wave)[...] = att_out[slot, wave]

            @pl.when(span_of(slot) != me)
            def _():
                att_copy(slot, wave).start()

    def recall():
        memory_in = enter_ref[:HEAD, :]
        normal_in = enter_ref[HEAD : HEAD + 1, :]
        head_of_lane = lax.broadcasted_iota(jnp.int32, (16, width), 1) // HEAD
        head_of_row = lax.broadcasted_iota(jnp.int32, (16, width), 0)
        blocks = jnp.concatenate(
            [jnp.where(head_mask(width, head), memory_in, 0.0) for head in range(heads)]
            + [jnp.where(head_of_lane == head_of_row, normal_in, 0.0)],
            axis=0,
        )
        high, low = two_parts(blocks)
        carried = dot(high, mq_turned[...]) + dot(low, mq_turned[...])
        head_rows = lax.broadcasted_iota(jnp.int32, (heads, 1), 0)
        stable = jnp.zeros((heads, 1), jnp.float32)
        for head in range(heads):
            stable = jnp.where(
                head_rows == head,
                enter_ref[HEAD + 1 : HEAD + 2, head * HEAD : head * HEAD + 1],
                stable,
            )
        carried_log = cumulative_ref[:heads] + stable
        own_top = inner_top[:heads]
        row_top = jnp.maximum(carried_log, own_top)
        inside = jnp.exp(own_top - row_top)
        outside = jnp.exp(carried_log - row_top)
        denominator = inside * inner_den[:heads] + outside * carried[width : width + heads]
        denominator = jnp.maximum(jnp.abs(denominator), 1.0)
        inside = inside / denominator
        outside = outside / denominator
        for head in range(heads):
            at = slice(head * HEAD, (head + 1) * HEAD)
            one = slice(head, head + 1)
            memory_ref[at, :] = (inside[one] * inner_ref[at, :] + outside[one] * carried[at]).astype(
                jnp.bfloat16
            )
        loads[6].wait()
        loads[7].wait()
        partial_ref[...] = dot(memory_ref[...], som[...], ((0,), (0,)))

    settle(me // 2)
    within(me // 2, (0, 1))
    forward("first")
    inner()
    forward("inner")
    pl.when(z == 0)(chain)
    lax.fori_loop(1, units - 1, visit, 0)
    last = visit_unit(units - 1)
    settle(last)
    pl.when(z == units - 2)(chain)
    within(last, (0, 1))
    for wave in range(2):
        finish(wave, (0,))
    for wave in range(2):
        if parts == 2:
            steps = []
            for rank in range(units - 1):
                other = visit_unit(rank)
                query = jnp.maximum(last, other)
                key = jnp.minimum(last, other)
                steps.append([(query, wave, 2 * key + side, False) for side in range(2)])
            run([step for side in zip(*steps) for step in side])
        else:

            def earlier(rank, unused):
                across_units(last, visit_unit(rank), (wave,))
                return unused

            lax.fori_loop(0, units - 1, earlier, 0)
        finish(wave, range(1, heads))
        if wave == 0:
            pl.when(z == units - 1)(chain)
            recall()

    out_span = rows // out_chunks
    per_wave = out_chunks // 2

    def out_rows(chunk):
        return pl.ds(chunk * out_span, out_span)

    order = list(range(1, lines)) + [0]
    swaps = {}
    lined = {}

    def pair_sum(step, chunk):
        swaps[step, chunk].wait_recv()
        mine = part_ref[
            out_rows(chunk), columns_of(lax.rem(line + step, lines) * CORES + core)
        ]
        return mine.astype(jnp.float32) + pair_in[step, out_rows(chunk), :].astype(jnp.float32)

    def pass_on(chunk):
        for step in range(1, lines):
            line_out[step, out_rows(chunk), :] = pair_sum(step, chunk).astype(jnp.bfloat16)
            copy = remote(
                line_out.at[step, out_rows(chunk)], line_in.at[step, out_rows(chunk)],
                sl_send, sl_recv.at[step - 1, chunk], "tp",
                lax.rem(line + step, lines) * CORES + core,
            )
            copy.start()
            lined[step, chunk] = copy

    for wave in range(2):
        for step in range(heads):

            @pl.when((my_owner != my_part) | (my_head != step))
            def _():
                at = attended_ref.at[wave, pl.ds(step * HEAD, HEAD)]
                remote(at, at, att_send, att_recv.at[step, wave], "sp", me).wait_recv()

        at = slice(wave * half_rows, (wave + 1) * half_rows)
        part_ref[at, :] = (
            dot(attended_ref[wave], soa[...], ((0,), (0,))) + partial_ref[at, :]
        ).astype(jnp.bfloat16)
        for chunk in range(wave * per_wave, (wave + 1) * per_wave):
            for step in order:
                target = lax.rem(line + step, lines) * CORES + (1 - core)
                copy = remote(
                    part_ref.at[out_rows(chunk), columns_of(target)],
                    pair_in.at[step, out_rows(chunk)], sp_send,
                    sp_recv.at[step, chunk], "tp", pair,
                )
                copy.start()
                swaps[step, chunk] = copy
        for chunk in range(wave * per_wave, (wave + 1) * per_wave):
            pass_on(chunk)

    def sent(ref, semaphore):
        remote(ref, ref, semaphore, semaphore, "tp", pair).wait_send()

    others = line_in.at[pl.ds(1, lines - 1)]
    sent(others, line_send)
    sent(pair_in, pair_send)
    sent(kv_out.at[pl.ds(0, heads - 1)], kv_send)
    sent(kv_all.at[pl.ds(0, heads * (parts - 1))], fwd_send)
    sent(q_out.at[pl.ds(0, heads - 1)], q_send)
    pl.when(my_owner != my_part)(lambda: sent(q_out.at[0], q_side))
    sent(states_ref.at[pl.ds(0, across - 1)], st_send.at[0])
    sent(state_rows.at[pl.ds(0, across - 1)], st_send.at[1])

    @pl.when(z < depth - 1)
    def _():
        for copy in prefix_sends():
            copy.wait_send()

    pl.when(my_owner == my_part)(lambda: sent(att_out.at[pl.ds(0, heads - 1)], att_send))
    pl.when(my_owner != my_part)(lambda: sent(att_out, att_send))
    for chunk in range(out_chunks):
        total = pair_sum(0, chunk)
        for step in range(1, lines):
            lined[step, chunk].wait_recv()
            total = total + line_in[step, out_rows(chunk), :].astype(jnp.float32)
        total_ref[out_rows(chunk), :] = total.astype(jnp.bfloat16)
        copy = pltpu.make_async_copy(
            total_ref.at[out_rows(chunk)], out_ref.at[out_rows(chunk)], out_sem
        )
        copy.start()
    pltpu.make_async_copy(total_ref, out_ref, out_sem).wait()
    sent(pair_in, sp_send)
    sent(others, sl_send)


def per_device(tp_size, depth, across, inputs, norm_gain, query_weight, key_weight, value_weight,
               memory_query_weight, memory_key_weight, memory_value_weight, input_gate_weight,
               forget_gate_weight, forget_bias, decay_shift, lambdas, head_gain,
               out_weight_attention, out_weight_memory):
    rows, columns = inputs.shape
    features = norm_gain.shape[0]
    width = query_weight.shape[1]
    heads = width // HEAD
    lines = tp_size // CORES
    spans = depth * across
    parts = spans // heads
    chunks = 4
    out_chunks = 4
    dma = pltpu.SemaphoreType.DMA


    hbm = pl.BlockSpec(memory_space=pl.ANY)
    bf16 = lambda *shape: pltpu.VMEM(shape, jnp.bfloat16)
    f32 = lambda *shape: pltpu.VMEM(shape, jnp.float32)
    return pl.pallas_call(
        functools.partial(layer_kernel, tp_size, depth, across, chunks, out_chunks),
        out_shape=jax.ShapeDtypeStruct((rows, columns), jnp.bfloat16),
        in_specs=[VMEM] * 2 + [hbm] * 6 + [VMEM] * 6 + [hbm] * 2,
        out_specs=hbm,
        scratch_shapes=[bf16(features, 6 * width)]
        + [bf16(width, features)] * 2
        + [
            bf16(rows, features), bf16(rows, features), f32(rows, 1), f32(rows, 6 * width),
            f32(rows, 128), f32(rows, 128),
            bf16(heads, rows, 128), bf16(heads, rows // 2, 128), bf16(spans, rows, 128),
            bf16(heads, rows // 2, 128), bf16(spans, VALUE_ROWS, rows),
            bf16(2, rows, 128), bf16(heads, 2, 128, rows), f32(heads, 2, 1, rows),
            f32(heads, 2, VALUE_ROWS, rows), bf16(heads, 2, HEAD, rows // 2),
            bf16(2, width, rows // 2),
            bf16(rows, width), bf16(rows, width), bf16(rows, width), bf16(width, rows),
            bf16(width, rows), f32(rows, 128),
            bf16(across, HEAD, width), f32(across, 8, width), bf16(HEAD, width), f32(8, width),
            bf16(HEAD, width), f32(8, width), f32(STATE_ROWS, width),
            f32(width, rows), f32(8, rows), f32(8, rows), f32(8, rows), f32(rows, 128),
            bf16(width, rows),
            f32(rows, features), bf16(rows, features), bf16(lines, rows, columns),
            bf16(lines, rows, columns),
            bf16(lines, rows, columns), bf16(rows, columns),
            dma(()), dma((8,)), dma(()), dma((lines - 1, chunks)), dma(()),
            dma((lines - 1, chunks)), dma(()),
            dma(()), dma(()), dma((heads, chunks)), dma((spans,)), dma(()), dma(()),
            dma((heads,)), dma(()), dma((heads, 2)),
            dma((2,)), dma((2, across)), dma((2,)), dma((2,)), dma(()), dma((lines, out_chunks)),
            dma(()),
            dma((lines - 1, out_chunks)),
        ],
        compiler_params=pltpu.CompilerParams(
            vmem_limit_bytes=VMEM_LIMIT, collective_id=0, has_side_effects=True
        ),
        name="layer",
    )(
        inputs, norm_gain[None, :], query_weight, key_weight, value_weight,
        memory_query_weight, memory_key_weight, memory_value_weight, input_gate_weight.T,
        forget_gate_weight.T, forget_bias[None, :], decay_shift.T, lambdas[None, :],
        head_gain[None, :], out_weight_attention, out_weight_memory,
    )


def columns_across(mesh):
    spans = mesh.shape["sp"]
    try:
        places = {device.coords[0] for device in mesh.devices.flat}
        across = len(places)
    except AttributeError:
        across = 2
    return across if spans % across == 0 else 1


def solution(mesh):
    across = columns_across(mesh)
    in_specs = (
        P("sp", "tp"),
        P(),
        P(None, "tp"),
        P(None, "tp"),
        P(None, "tp"),
        P(None, "tp"),
        P(None, "tp"),
        P(None, "tp"),
        P(None, "tp"),
        P(None, "tp"),
        P("tp"),
        P("sp", "tp"),
        P("tp"),
        P(),
        P("tp", None),
        P("tp", None),
    )
    return jax.shard_map(
        functools.partial(
            per_device, mesh.shape["tp"], mesh.shape["sp"] // across, across
        ),
        mesh=mesh,
        in_specs=in_specs,
        out_specs=P("sp", "tp"),
        check_vma=False,
    )
```
